32 devices in a mesh: ep: 8 (over z, x), tp: 4 (over y, core).
Axes of the slice: x: 2, y: 2, z: 4, core: 2. Of those that a mesh axis runs over, the one named last changes fastest.
Arguments:
- receptance: bfloat16 [4096, 1024], P('ep', 'tp'), may hold values from -6 to 6
- key_matrix: bfloat16 [4096, 1024], P('ep', 'tp'), may hold values from -6 to 6
- value_matrix: bfloat16 [4096, 1024], P('ep', 'tp'), may hold values from -6 to 6
- decay_data_term: bfloat16 [4096, 1024], P('ep', 'tp'), may hold values from -3.5 to 3.5
- correction_rate_data: bfloat16 [4096, 1024], P('ep', 'tp'), may hold values from -6 to 6
- output_gate_input: bfloat16 [4096, 1024], P('ep', 'tp'), may hold values from -6 to 6
- decay_channel_offset: float32 [1024], P('tp'), may hold values from -12 to -2
- correction_rate_offset: float32 [1024], P('tp'), may hold values from -12 to 1
- extra_head_log_decay: float32 [4096, 16], P('ep', 'tp'), may hold values from -2.1 to 0, as said below
- head_norm_gain: float32 [1024], P('tp'), may hold values from 0.1 to 1.9
- mixer_output_weight: bfloat16 [1024, 2048], P('tp'), may hold values from -0.1875 to 0.1875
- expert_layer_input: bfloat16 [1024, 2048], P('ep'), may hold values from -6 to 6
- feedforward_norm_gain: float32 [2048], replicated, may hold values from 0.1 to 1.9
- group_router_weight: bfloat16 [2048, 4], replicated, may hold values from -0.125 to 0.125
- expert_router_weight: bfloat16 [2048, 8], replicated, may hold values from -0.125 to 0.125
- routes: int32 [1024, 2], P('ep'), may hold values from 0 to 7, all different within a row; in each aligned block of 128 rows (0 to 127, 128 to 255, ...) at most 64 rows name the same one
- expert_gate_weight: bfloat16 [8, 2048, 4096], P('ep', None, 'tp'), may hold values from -0.125 to 0.125
- expert_up_weight: bfloat16 [8, 2048, 4096], P('ep', None, 'tp'), may hold values from -0.125 to 0.125
- expert_down_weight: bfloat16 [8, 4096, 2048], P('ep', 'tp'), may hold values from -0.09375 to 0.09375
Outputs:
- token_mixer_output: bfloat16 [4096, 2048], P(('ep', 'tp'))
- expert_out: bfloat16 [1024, 2048], P('ep', 'tp')
The draws below stay inside these ranges and needn't reach their ends.
Inputs may be any that keep to these rules, and one draw needn't show every extreme that they name: A token's routes are distinct. Within the rows of one index of ep, no expert is named by more than 64 rows, a bound that some block reaches. `extra_head_log_decay`: entries are zero or negative; each head has a few nonzero positions.
All inputs are finite; a program needn't handle non-finite values.
Results may differ from the reference program's by a relative error of at most 0.022.
Values may be sent and summed in bfloat16 or wider, within the bound.
A program may use at most 128 MiB of HBM per device.

```python
import math
import jax
import jax.numpy as jnp
import numpy as np
from jax import lax

D = 2048
HEAD_DIM = 64
HEADS = 16
MIX = 1024
FF = 4096
GROUPS = 4
EXPERTS = 8
TOP = 2
MIX_ROWS = 512
MIX_TOKENS = 4096
MOE_ROWS = 128
MOE_TOKENS = 1024
CAP = 64
N_EP = 8
N_TP = 4


def slow_heads(key):
    share = 0.5
    return jax.random.uniform(jax.random.fold_in(key, 101), (HEADS,)) < share


def draw_decay_channel_offset(key, part):
    slow = slow_heads(key)
    slow_level = math.log(0.5 / MIX_TOKENS) + 0.5
    fast_level = math.log(0.03) + 0.5
    level = jnp.where(slow, slow_level, fast_level)
    jitter = jax.random.uniform(jax.random.fold_in(key, 3), (HEADS, HEAD_DIM), jnp.float32, -0.3, 0.3)
    return (level[:, None] + jitter).reshape(MIX).astype(jnp.float32)


def draw_correction_rate_offset(key, part):
    slow = slow_heads(key)
    slow_level = math.log(6.0 / MIX_TOKENS)
    spread = jax.random.uniform(jax.random.fold_in(key, 5), (HEADS, HEAD_DIM), jnp.float32, -1.0, 1.0)
    level = jnp.where(slow[:, None], slow_level + 0.3 * spread, spread)
    return level.reshape(MIX).astype(jnp.float32)


def draw_decay_data_term(key, part):
    blocks = MIX_TOKENS // MIX_ROWS
    offset = jax.random.uniform(jax.random.fold_in(key, 7), (blocks, 1, HEADS, 1), jnp.float32, -0.4, 0.4)
    noise = 0.5 * jax.random.normal(jax.random.fold_in(key, 9), (blocks, MIX_ROWS, HEADS, HEAD_DIM), jnp.float32)
    return (offset + noise).reshape(MIX_TOKENS, MIX).astype(jnp.bfloat16)


def draw_extra_head_log_decay(key, part):
    where_at = jax.random.randint(jax.random.fold_in(key, 13), (3, HEADS), 0, MIX_TOKENS)
    depth = jnp.log(jax.random.uniform(jax.random.fold_in(key, 17), (3, HEADS), jnp.float32, 0.5, 0.8))
    positions = jnp.arange(MIX_TOKENS)[:, None, None]
    struck = positions == where_at[None, :, :]
    return jnp.sum(jnp.where(struck, depth[None, :, :], 0.0), axis=1).astype(jnp.float32)


def levels(rng, extent, shards, low, high):
    loudness, own = 1.0, jax.random.fold_in(rng, 6)
    for position, blocks in shards:
        draws = jnp.exp(jax.random.uniform(jax.random.fold_in(own, position), (blocks,), jnp.float32, low / len(shards), high / len(shards)))
        loudness = loudness * jnp.repeat(draws, extent[position] // blocks).reshape([-1 if axis == position else 1 for axis in range(len(extent))])
    return loudness


def routed_block(own_key, own, number, rows, count, top, reach, skew):
    sequence = jax.random.permutation(own_key, count)
    heavy_load, ordinary = shares(count, rows * top, reach, skew, True), shares(count, rows * top, reach, skew, False)
    places = jnp.arange(count)

    def named(tallies, offset_by):
        used = int((tallies > 0).sum())
        fixed = max(1, used // 4)
        shifted = fixed + (places - fixed + offset_by * (used - fixed)) % max(1, count - fixed)
        return jnp.zeros((count,), jnp.int32).at[sequence[jnp.where(places < fixed, places, shifted)]].set(jnp.asarray(tallies, jnp.int32))

    tallies = jnp.where(number % 4 == 0, named(heavy_load, number // 4), named(ordinary, number - number // 4 - 1))
    mixed = jax.random.permutation(jax.random.fold_in(own, 3), count)
    giver, sink = mixed[0:count // 2 * 2:2], mixed[1:count // 2 * 2:2]
    margin = jnp.minimum(tallies[giver] - 1, reach - tallies[sink]) // 2
    margin = jnp.where((giver == sequence[0]) | (sink == sequence[0]) | (tallies[sink] == 0), 0, jnp.maximum(margin, 0))
    shifted = jax.random.randint(jax.random.fold_in(own, 4), (count // 2,), 0, 1 << 20) % (margin + 1)
    tallies = tallies.at[giver].add(-shifted).at[sink].add(shifted)
    labels = jnp.searchsorted(jnp.cumsum(tallies), jnp.arange(rows * top), side="right").astype(jnp.int32)
    table = labels.reshape(top, rows).T
    table = table[jax.random.permutation(jax.random.fold_in(own, 1), rows)]
    offset_by = jax.random.randint(jax.random.fold_in(own, 2), (rows, 1), 0, top)
    return jnp.take_along_axis(table, (jnp.arange(top)[None, :] + offset_by) % top, axis=1)


def shares(amount, total, bound, lean, full):
    portions = [(1 << 20) // math.isqrt(standing ** lean) + 1 for standing in range(1, amount + 1)]
    largest = bound if full else min(bound, max(-(-total // amount), total * portions[0] // sum(portions)))
    least = 1 if total - largest >= amount - 1 else 0
    counts, surplus = [largest] + [least] * (amount - 1), total - largest - least * (amount - 1)
    while surplus > 0:
        movable = [i for i in range(1, amount) if counts[i] < largest] or [i for i in range(1, amount) if counts[i] < bound]
        pool, remaining = sum([portions[i] for i in movable]), surplus
        for i in movable:
            addition = min(bound - counts[i], max(1, remaining * portions[i] // pool), surplus)
            counts[i] = counts[i] + addition
            surplus = surplus - addition
    return np.array(counts)


def centred(key, shape, scale, reach, pieces=(), held_as=jnp.bfloat16):
    drawn = scale * jax.random.normal(key, shape, jnp.float32)
    if pieces:
        drawn = drawn * levels(key, shape, pieces, -0.22, 0.18)
    return jnp.clip(drawn, -reach, reach).astype(held_as)


def setup_inputs(seed: int = 0) -> dict:
    splits = jax.random.split(jax.random.key(seed), 20)
    receptance = centred(splits[0], (MIX_TOKENS, MIX), 1.0, 6.0, ((0, 8), (1, 4)))
    key_matrix = centred(splits[1], (MIX_TOKENS, MIX), 1.0, 6.0, ((0, 8), (1, 4)))
    value_matrix = centred(splits[2], (MIX_TOKENS, MIX), 1.0, 6.0, ((0, 8), (1, 4)))
    decay_data_term = draw_decay_data_term(jax.random.fold_in(splits[19], 71), 0)
    correction_rate_data = centred(splits[4], (MIX_TOKENS, MIX), 1.0, 6.0, ((0, 8), (1, 4)))
    output_gate_input = centred(splits[5], (MIX_TOKENS, MIX), 1.0, 6.0, ((0, 8), (1, 4)))
    decay_channel_offset = draw_decay_channel_offset(jax.random.fold_in(splits[19], 71), 0)
    correction_rate_offset = draw_correction_rate_offset(jax.random.fold_in(splits[19], 71), 0)
    extra_head_log_decay = draw_extra_head_log_decay(jax.random.fold_in(splits[19], 71), 0)
    head_norm_gain = jnp.clip(1.0 + 0.18 * jax.random.normal(splits[9], (MIX,), jnp.float32), 0.1, 1.9)
    mixer_output_weight = centred(splits[10], (MIX, D), MIX ** -0.5, 0.1875, ((0, 4),))
    expert_layer_input = centred(splits[11], (MOE_TOKENS, D), 1.0, 6.0, ((0, 8),))
    feedforward_norm_gain = jnp.clip(1.0 + 0.18 * jax.random.normal(splits[12], (D,), jnp.float32), 0.1, 1.9)
    group_router_weight = centred(splits[13], (D, GROUPS), D ** -0.5, 0.125)
    expert_router_weight = centred(splits[14], (D, EXPERTS), D ** -0.5, 0.125)
    routes_keys = jax.random.split(jax.random.fold_in(splits[15], 1), MOE_TOKENS // MOE_ROWS)
    routes_turns = jax.random.permutation(jax.random.fold_in(splits[15], 3), MOE_TOKENS // MOE_ROWS)
    routes = jax.vmap(lambda own, number: routed_block(jax.random.fold_in(splits[15], 2), own, number, MOE_ROWS, EXPERTS, TOP, CAP, 2))(routes_keys, routes_turns).reshape((MOE_TOKENS, TOP))
    expert_gate_weight = centred(splits[16], (EXPERTS, D, FF), D ** -0.5, 0.125, ((0, 8), (2, 4)))
    expert_up_weight = centred(splits[17], (EXPERTS, D, FF), D ** -0.5, 0.125, ((0, 8), (2, 4)))
    expert_down_weight = centred(splits[18], (EXPERTS, FF, D), FF ** -0.5, 0.09375, ((0, 8), (1, 4)))
    return {"receptance": receptance, "key_matrix": key_matrix, "value_matrix": value_matrix, "decay_data_term": decay_data_term, "correction_rate_data": correction_rate_data, "output_gate_input": output_gate_input, "decay_channel_offset": decay_channel_offset, "correction_rate_offset": correction_rate_offset, "extra_head_log_decay": extra_head_log_decay, "head_norm_gain": head_norm_gain, "mixer_output_weight": mixer_output_weight, "expert_layer_input": expert_layer_input, "feedforward_norm_gain": feedforward_norm_gain, "group_router_weight": group_router_weight, "expert_router_weight": expert_router_weight, "routes": routes, "expert_gate_weight": expert_gate_weight, "expert_up_weight": expert_up_weight, "expert_down_weight": expert_down_weight}


key_eps = 1e-06
group_eps = 0.00064
norm_eps = 1e-06
highest = lax.Precision.HIGHEST

def token_mixer_block(receptance, key_matrix, value_matrix, decay_data_term, correction_rate_data, output_gate_input, decay_channel_offset, correction_rate_offset, extra_head_log_decay, head_norm_gain, mixer_output_weight):
    positions = receptance.shape[0]

    def head_view(tensor_in):
        return tensor_in.astype(jnp.float32).reshape(positions, HEADS, HEAD_DIM)
    recept = head_view(receptance)
    keyed = head_view(key_matrix)
    valued = head_view(value_matrix)
    unit_keys = keyed * lax.rsqrt(lax.optimization_barrier(jnp.sum(keyed * keyed, axis=-1, keepdims=True)) + key_eps)
    learn_rate = jax.nn.sigmoid(head_view(correction_rate_data) + correction_rate_offset.reshape(HEADS, HEAD_DIM))
    decay_preactivation = head_view(decay_data_term) + decay_channel_offset.reshape(HEADS, HEAD_DIM)
    decay_factor = jnp.exp(-jnp.exp(-jax.nn.softplus(-decay_preactivation) - 0.5) + extra_head_log_decay[:, :, None])
    removal = unit_keys * learn_rate

    def advance(state, inputs):
        recept_now, decay_now, unit_now, removal_now, key_now, value_now = inputs
        along = jnp.einsum('hvk,hk->hv', state, unit_now, precision=highest)
        state = state * decay_now[:, None, :] - along[:, :, None] * removal_now[:, None, :] + value_now[:, :, None] * key_now[:, None, :]
        return (state, jnp.einsum('hvk,hk->hv', state, recept_now, precision=highest))
    start_state = jnp.zeros((HEADS, HEAD_DIM, HEAD_DIM), jnp.float32)
    _, head_out = lax.scan(advance, start_state, (recept, decay_factor, unit_keys, removal, keyed, valued))
    centre = lax.optimization_barrier(jnp.mean(head_out, axis=-1, keepdims=True))
    spread = lax.optimization_barrier(jnp.mean(jnp.square(head_out - centre), axis=-1, keepdims=True))
    normed = (head_out - centre) * lax.rsqrt(spread + group_eps)
    gated = normed * head_norm_gain.reshape(HEADS, HEAD_DIM) * jax.nn.sigmoid(head_view(output_gate_input))
    mixed_hidden = gated.reshape(positions, MIX).astype(jnp.bfloat16)
    hidden_groups = jnp.moveaxis(mixed_hidden.reshape(positions, N_TP, MIX // N_TP), 1, 0)
    weight_groups = mixer_output_weight.reshape(N_TP, MIX // N_TP, D)

    def add_group(total, pair):
        block_hidden, block_weight = pair
        part = jnp.dot(block_hidden, block_weight, preferred_element_type=jnp.float32).astype(jnp.bfloat16)
        part = lax.optimization_barrier(part)
        return (total + part.astype(jnp.float32), None)
    total, _ = lax.scan(add_group, jnp.zeros((positions, D), jnp.float32), (hidden_groups, weight_groups))
    return total.astype(jnp.bfloat16)

def expert_block(expert_layer_input, feedforward_norm_gain, group_router_weight, expert_router_weight, routes, expert_gate_weight, expert_up_weight, expert_down_weight):
    tokens = expert_layer_input.shape[0]
    widened = expert_layer_input.astype(jnp.float32)
    normed_input = (widened * lax.rsqrt(lax.optimization_barrier(jnp.mean(widened * widened, axis=-1, keepdims=True)) + norm_eps) * feedforward_norm_gain).astype(jnp.bfloat16)
    group_logit = jnp.dot(normed_input, group_router_weight, preferred_element_type=jnp.float32)
    group_exp = jnp.exp(group_logit)
    group_prob = group_exp / lax.optimization_barrier(jnp.sum(group_exp, axis=-1, keepdims=True))
    expert_logit = jnp.dot(normed_input, expert_router_weight, preferred_element_type=jnp.float32)
    per_group = EXPERTS // GROUPS
    chosen_logit = jnp.take_along_axis(expert_logit, routes, axis=1)
    chosen_group = jnp.take_along_axis(group_prob, routes // per_group, axis=1)
    route_weight = chosen_group * jax.nn.sigmoid(chosen_logit - chosen_logit[:, ::-1])
    flat_routes = routes.reshape(-1)
    onehot = (flat_routes[:, None] == jnp.arange(EXPERTS, dtype=jnp.int32)[None, :]).astype(jnp.int32)
    ranked = lax.optimization_barrier(jnp.sum((jnp.cumsum(onehot, axis=0) - onehot) * onehot, axis=1))
    room = N_EP * CAP
    destination = (flat_routes * room + ranked).astype(jnp.int32)
    source_rows = jnp.zeros((EXPERTS * room,), jnp.int32).at[destination].set((jnp.arange(flat_routes.shape[0], dtype=jnp.int32) // TOP).astype(jnp.int32))
    gathered = normed_input[source_rows].reshape(EXPERTS, room, D)

    def run_expert(pack):
        rows_in, gate_mat, up_mat, down_mat = pack
        gate_val = jnp.dot(rows_in, gate_mat, preferred_element_type=jnp.float32)
        up_val = jnp.dot(rows_in, up_mat, preferred_element_type=jnp.float32)
        expert_hidden = (jax.nn.silu(gate_val) * up_val).astype(jnp.bfloat16)
        hidden_groups = expert_hidden.reshape(room, N_TP, FF // N_TP)
        down_groups = down_mat.reshape(N_TP, FF // N_TP, D)
        total = jnp.zeros((room, D), jnp.float32)
        for member in range(N_TP):
            part = jnp.dot(hidden_groups[:, member], down_groups[member], preferred_element_type=jnp.float32).astype(jnp.bfloat16)
            part = lax.optimization_barrier(part)
            total = total + part.astype(jnp.float32)
        return total.astype(jnp.bfloat16)
    expert_rows = lax.map(run_expert, (gathered, expert_gate_weight, expert_up_weight, expert_down_weight)).reshape(EXPERTS * room, D)
    picked = expert_rows[destination].astype(jnp.float32).reshape(tokens, TOP, D)
    return lax.optimization_barrier(jnp.sum(picked * route_weight[:, :, None], axis=1)).astype(jnp.bfloat16)

def reference(receptance, key_matrix, value_matrix, decay_data_term, correction_rate_data, output_gate_input, decay_channel_offset, correction_rate_offset, extra_head_log_decay, head_norm_gain, mixer_output_weight, expert_layer_input, feedforward_norm_gain, group_router_weight, expert_router_weight, routes, expert_gate_weight, expert_up_weight, expert_down_weight):
    token_mixer_output = token_mixer_block(receptance, key_matrix, value_matrix, decay_data_term, correction_rate_data, output_gate_input, decay_channel_offset, correction_rate_offset, extra_head_log_decay, head_norm_gain, mixer_output_weight)
    expert_out = expert_block(expert_layer_input, feedforward_norm_gain, group_router_weight, expert_router_weight, routes, expert_gate_weight, expert_up_weight, expert_down_weight)
    return (token_mixer_output, expert_out)
```

```python
import functools
import math

import jax
import jax.numpy as jnp
from jax import lax
from jax.experimental import pallas as pl
from jax.experimental.pallas import tpu as pltpu
from jax.sharding import PartitionSpec as P

HEAD_DIM = 64
PAIR = 2 * HEAD_DIM
VMEM_LIMIT = 56 << 20
HALF_EXP = math.exp(-0.5)
GROUPS = 4


key_eps = 1e-06
group_eps = 0.00064
norm_eps = 1e-06
highest = lax.Precision.HIGHEST


def bf(x):
    return x.astype(jnp.bfloat16)


def mm(x, y):
    return lax.dot_general(x, y, (((1,), (0,)), ((), ())), preferred_element_type=jnp.float32)


def mm_nt(x, y):
    return lax.dot_general(x, y, (((1,), (1,)), ((), ())), preferred_element_type=jnp.float32)


def mm_tn(x, y):
    return lax.dot_general(x, y, (((0,), (0,)), ((), ())), preferred_element_type=jnp.float32)


def halves(x):
    high = bf(x)
    return high, bf(x - high.astype(jnp.float32))


def sum_right(x, ones):
    high, low = halves(x)
    return mm(high, ones) + mm(low, ones)


def logistic(x):
    return 1.0 / (1.0 + jnp.exp(-x))


def flag(cond):
    return jnp.where(cond, 1.0, 0.0)


def iota(shape, dim):
    return lax.broadcasted_iota(jnp.int32, shape, dim)


def pair_blocks():
    return flag((iota((PAIR, PAIR), 0) < HEAD_DIM) == (iota((PAIR, PAIR), 1) < HEAD_DIM))


def scan_kernel(
    group,
    pump,
    r_ref,
    k_ref,
    v_ref,
    d_ref,
    a_ref,
    d_off_ref,
    a_off_ref,
    extra_ref,
    out_ref,
    reach_ref,
    ends_ref,
    chain_ref,
):
    positions, width = r_ref.shape
    pairs = width // PAIR
    C = HEAD_DIM
    rows_per = group * C
    own_block = pair_blocks()
    own_bf = bf(own_block)
    row, col = iota((C, PAIR), 0), iota((C, PAIR), 1) & (HEAD_DIM - 1)
    strict, upto = row > col, row >= col
    eye = flag(row == col)
    first = iota((1, PAIR), 1) < HEAD_DIM
    tri = bf(flag(iota((C, C), 0) >= iota((C, C), 1)))
    level_masks = []
    for s in range(6):
        inside = (
            ((row >> (s + 1)) == (col >> (s + 1)))
            & (((row >> s) & 1) == 1)
            & (((col >> s) & 1) == 0)
        )
        level_masks.append(bf(flag(inside)))

    def spread(x):
        return jnp.concatenate([x, x], axis=0) * own_bf

    square = (iota((PAIR, PAIR), 0) == iota((PAIR, PAIR), 1)).astype(jnp.float32)
    for p in range(pairs):
        chain_ref[p, :PAIR] = jnp.zeros((PAIR, PAIR), jnp.float32)
        chain_ref[p, PAIR:] = square

    def step(g, carry):
        base = pl.multiple_of(g * rows_per, rows_per)
        rows = pl.ds(base, rows_per)
        items = []
        for p in range(pairs):
            lanes = slice(p * PAIR, (p + 1) * PAIR)
            k = k_ref[rows, lanes].astype(jnp.float32)
            u = k * lax.rsqrt(sum_right(k * k, own_bf) + key_eps)
            rem = u * logistic(a_ref[rows, lanes].astype(jnp.float32) + a_off_ref[:, lanes])
            e = extra_ref[rows, :]
            extra = jnp.where(first, e[:, 2 * p : 2 * p + 1], e[:, 2 * p + 1 : 2 * p + 2])
            lg = extra - HALF_EXP * logistic(
                d_ref[rows, lanes].astype(jnp.float32) + d_off_ref[:, lanes]
            )
            r = r_ref[rows, lanes].astype(jnp.float32)
            v = v_ref[rows, lanes]
            for c in range(group):
                cut = slice(c * C, (c + 1) * C)
                items.append((p, c, k[cut], u[cut], rem[cut], lg[cut], r[cut], v[cut]))
        stage = []
        for p, c, k, u, rem, lg, r, v in items:
            high, low = halves(lg)
            rest = bf(lg - high.astype(jnp.float32) - low.astype(jnp.float32))
            cumul = mm(tri, high) + mm(tri, low) + mm(tri, rest)
            stage.append(cumul)
        work = []
        for (p, c, k, u, rem, lg, r, v), cumul in zip(items, stage):
            mid = 0.5 * cumul[C - 1 : C]
            up_now, down = jnp.exp(cumul - mid), jnp.exp(mid - cumul)
            up_before = jnp.exp(cumul - lg - mid)
            half = jnp.exp(mid)
            cq, cu, dk, dr = r * up_now, u * up_before, k * down, rem * down
            left = bf(jnp.concatenate([cu, cq], axis=0))
            pair_r = mm_nt(left, spread(bf(dr)))
            pair_k = mm_nt(left, spread(bf(dk)))
            work.append((cq * half, bf(cu * half), bf(dk * half), bf(dr * half), half * half, pair_r, pair_k))
        pump(g, 0)
        solve = []
        for (p, c, k, u, rem, lg, r, v), (qe, ue, kt, rt, ed, pair_r, pair_k) in zip(items, work):
            rp = bf(jnp.where(strict, pair_r[:C], 0.0))
            rr = bf(jnp.where(upto, pair_r[C:], 0.0))
            kp = jnp.where(strict, pair_k[:C], 0.0)
            rk = jnp.where(upto, pair_k[C:], 0.0)
            kv = mm(bf(jnp.concatenate([kp, rk], axis=0)), spread(v))
            inv = eye - (rp * level_masks[0]).astype(jnp.float32)
            solve.append([rp, rr, kv, inv])
        for s in range(1, 6):
            mids = [bf(mm(bf(inv), spread(rp * level_masks[s]))) for rp, rr, kv, inv in solve]
            for item, y in zip(solve, mids):
                item[3] = item[3] - mm(y, spread(bf(item[3])))
            if s == 2:
                pump(g, 1)
        wvs = []
        for (rp, rr, kv, inv), w in zip(solve, work):
            wide = jnp.concatenate([spread(w[1]), spread(bf(kv[:C]))], axis=1)
            wvs.append(bf(mm(bf(inv), wide)))
        pump(g, 2)
        tails = []
        for (rp, rr, kv, inv), (qe, ue, kt, rt, ed, _, _), wv, item in zip(solve, work, wvs, items):
            wide = jnp.concatenate([spread(wv[:, :PAIR]), spread(wv[:, PAIR:])], axis=1)
            rw = mm(rr, wide)
            read = bf(qe - rw[:, :PAIR])
            local = kv[C:] - rw[:, PAIR:]
            v = item[7]
            x = jnp.concatenate(
                [jnp.concatenate([v, jnp.zeros_like(v)], axis=1),
                 jnp.concatenate([-wv[:, PAIR:], -wv[:, :PAIR]], axis=1)], axis=0)
            nb = mm_tn(x, jnp.concatenate([kt, rt], axis=0))
            tails.append((read, local, nb[:PAIR] * own_block, bf(nb[PAIR:] * own_block), ed))
        z = [chain_ref[p] for p in range(pairs)]
        for c in range(group):
            for p in range(pairs):
                read, local, add, neg, ed = tails[p * group + c]
                zb = bf(z[p])
                qz = mm_nt(read, zb)
                at = pl.ds(pl.multiple_of(base + c * C, C), C)
                lanes = slice(p * PAIR, (p + 1) * PAIR)
                out_ref[at, lanes] = local + qz[:, :PAIR]
                reach_ref[at, lanes] = bf(qz[:, PAIR:])
                moved = z[p] * ed + mm(zb, neg)
                z[p] = jnp.concatenate([moved[:PAIR] + add, moved[PAIR:]], axis=0)
        for p in range(pairs):
            chain_ref[p] = z[p]
        pump(g, 3)
        return carry

    lax.fori_loop(0, positions // rows_per, step, 0)
    for p in range(pairs):
        s, m = chain_ref[p, :PAIR], chain_ref[p, PAIR:]
        ends_ref[p * 2 * C : p * 2 * C + C] = bf(s[:C] + s[C:])
        ends_ref[p * 2 * C + C : (p + 1) * 2 * C] = bf(m[:C] + m[C:])


def join_kernel(axis, all_ref, out_ref, reach_ref, gate_ref, gain_ref, mixed_ref):
    devices, place = lax.axis_size(axis), lax.axis_index(axis)
    width = out_ref.shape[1]
    pairs = width // PAIR
    C = HEAD_DIM
    own_block = pair_blocks()
    own_bf = bf(own_block)
    mean_bf = bf(own_block * (1.0 / HEAD_DIM))
    states = [jnp.zeros((C, PAIR), jnp.float32) for _ in range(pairs)]

    def hop(j, states):
        new = []
        for p in range(pairs):
            s = all_ref[j, p * 2 * C : p * 2 * C + C].astype(jnp.float32)
            m = all_ref[j, p * 2 * C + C : (p + 1) * 2 * C]
            m = jnp.concatenate([m, m], axis=0) * own_bf
            new.append(sum_right(states[p], m) + s)
        return tuple(new)

    states = lax.fori_loop(0, place, hop, tuple(states))
    for p in range(pairs):
        lanes = slice(p * PAIR, (p + 1) * PAIR)
        s = bf(states[p])
        s = jnp.concatenate([s, s], axis=0) * own_bf
        head = out_ref[:, lanes] + mm_nt(reach_ref[:, lanes], s)
        centred = head - sum_right(head, mean_bf)
        spread = sum_right(centred * centred, mean_bf)
        normed = centred * lax.rsqrt(spread + group_eps)
        gate = logistic(gate_ref[:, lanes].astype(jnp.float32))
        mixed_ref[:, lanes] = bf(normed * gain_ref[:, lanes] * gate)


def place_of():
    n_ep, n_tp = lax.axis_size("ep"), lax.axis_size("tp")
    e, t = lax.axis_index("ep"), lax.axis_index("tp")
    core = lax.rem(t, 2)
    return n_ep, n_tp, n_tp // 2, e, t, lax.div(t, 2), core


def remote(src, dst, send, recv, e, t):
    return pltpu.make_async_remote_copy(
        src_ref=src,
        dst_ref=dst,
        send_sem=send,
        recv_sem=recv,
        device_id=(e, t),
        device_id_type=pl.DeviceIdType.MESH,
    )


def meet():
    n_ep, n_tp, n_y, e, t, y, core = place_of()
    barrier = pltpu.get_barrier_semaphore()

    def greet(pe, pt):
        pl.semaphore_signal(
            barrier, inc=1, device_id=(pe, pt), device_id_type=pl.DeviceIdType.MESH
        )

    for d in range(1, n_ep):
        greet(lax.rem(e + d, n_ep), t)
    greet(e, 2 * y + 1 - core)
    for d in range(1, n_y):
        greet(e, 2 * lax.rem(y + d, n_y) + core)
    return lambda: pl.semaphore_wait(barrier, n_ep - 1 + n_y)


def span(first, last, body):
    def run(d, carry):
        body(d)
        return carry

    lax.fori_loop(first, last, run, 0)


def wide(x):
    return x.astype(jnp.float32)


def whole_kernel(
    group,
    r_hbm,
    k_hbm,
    v_hbm,
    d_hbm,
    a_hbm,
    gate_in_hbm,
    d_off_ref,
    a_off_ref,
    extra_ref,
    gain_ref,
    out_weight_hbm,
    x_hbm,
    norm_gain_ref,
    group_router_ref,
    expert_router_ref,
    routes_ref,
    gate_hbm,
    up_hbm,
    down_hbm,
    mixer_ref,
    expert_ref,
    r_ref,
    k_ref,
    v_ref,
    d_ref,
    a_ref,
    gate_in_ref,
    out_weight_ref,
    x_ref,
    normed_ref,
    place_ref,
    cols_ref,
    piece_ref,
    out_ref,
    reach_ref,
    every_ref,
    chain_ref,
    mixed_ref,
    proj_ref,
    gate_ref,
    up_ref,
    down_ref,
    hidden_ref,
    part_ref,
    near_ref,
    stage_ref,
    far_ref,
    final_ref,
    home_ref,
    mnear_ref,
    mstage_ref,
    mfar_ref,
    in_sem,
    gate_sem,
    up_sem,
    down_sem,
    es,
    er,
    cs,
    cr,
    ys,
    yr,
    fs,
    fr,
    zs,
    zr,
    gs,
    gr,
    ns,
    nr,
    bs,
    br,
    hs,
    hr,
    mns,
    mnr,
    mys,
    myr,
):
    n_ep, n_tp, n_y, e, t, y, core = place_of()
    units = gate_ref.shape[1]
    model = x_ref.shape[1]
    tokens = x_ref.shape[0]
    share = model // n_tp
    slots = piece_ref.shape[0]
    capacity = slots // n_ep
    experts = expert_router_ref.shape[0]
    groups = group_router_ref.shape[0]
    rows = proj_ref.shape[0] // (2 * n_tp)
    other = 2 * y + 1 - core
    half = n_ep // 2
    half_rows = half * capacity
    wide_units, wide_model = min(256, units), min(512, model)

    inputs = [(x_hbm, x_ref)]
    inputs += [(k_hbm, k_ref), (a_hbm, a_ref), (d_hbm, d_ref), (r_hbm, r_ref), (v_hbm, v_ref)]
    inputs += [(gate_in_hbm, gate_in_ref), (out_weight_hbm, out_weight_ref)]
    loads = [pltpu.make_async_copy(s, d, in_sem.at[i]) for i, (s, d) in enumerate(inputs)]

    def gate_copy(i):
        at = pl.ds(pl.multiple_of(i * wide_units, wide_units), wide_units)
        return (
            pltpu.make_async_copy(gate_hbm.at[0, :, at], gate_ref.at[:, at], gate_sem.at[i]),
            pltpu.make_async_copy(up_hbm.at[0, :, at], up_ref.at[:, at], up_sem.at[i]),
        )

    def down_copy(i):
        at = pl.ds(pl.multiple_of(i * wide_model, wide_model), wide_model)
        return pltpu.make_async_copy(down_hbm.at[0, :, at], down_ref.at[:, at], down_sem.at[i])

    def columns(index):
        return pl.ds(pl.multiple_of(index * share, share), share)

    def block(d):
        return pl.ds(pl.multiple_of(d * capacity, capacity), capacity)

    def peer_y(h):
        return lax.rem(y + h, n_y)

    def ep_copy(d):
        peer = lax.rem(e + d, n_ep)
        return remote(
            cols_ref.at[block(peer), :], piece_ref.at[block(d), columns(t)], es.at[d], er.at[d], peer, t
        )

    def core_copy(d):
        ref = piece_ref.at[block(d), columns(t)]
        return remote(ref, ref, cs.at[d], cr.at[d], e, other)

    def y_copy(d, h):
        ref = piece_ref.at[block(d), columns(t)]
        return remote(ref, ref, ys.at[h, d], yr.at[h, d], e, 2 * peer_y(h) + core)

    def forward_copy(d, h):
        ref = piece_ref.at[block(d), columns(2 * lax.rem(y - h + n_y, n_y) + core)]
        return remote(ref, ref, fs.at[h, d], fr.at[h, d], e, other)

    def arrived(d):
        ep_copy(d).wait_recv()
        for h in range(1, n_y):
            y_copy(d, h).start()
        core_copy(d).start()

    def pass_on(d):
        for h in range(1, n_y):
            y_copy(d, h).wait_recv()
            forward_copy(d, h).start()

    def gathered(d):
        core_copy(d).wait_recv()
        for h in range(1, n_y):
            forward_copy(d, h).wait_recv()

    n_x = gs.shape[0]
    n_z = n_ep // n_x
    z, x = lax.div(e, n_x), lax.rem(e, n_x)

    def up_copy(zz):
        ref = every_ref.at[zz * n_x + x]
        return remote(ref, ref, zs.at[zz], zr.at[zz], e + n_x, t)

    def side_copy(zz, h):
        ref = every_ref.at[zz * n_x + x]
        peer = z * n_x + lax.rem(x + h, n_x)
        return remote(ref, ref, gs.at[h, zz], gr.at[h, zz], peer, t)

    def pass_ends(zz):
        @pl.when(z + 1 < n_z)
        def _():
            up_copy(zz).start()

        for h in range(1, n_x):
            side_copy(zz, h).start()

    def relay_ends(i):
        @pl.when(z >= i)
        def _():
            up_copy(z - i).wait_recv()
            pass_ends(z - i)

    def collect_ends(zz):
        @pl.when(z >= zz)
        def _():
            for h in range(1, n_x):
                side_copy(zz, h).wait_recv()

    def close_ends(zz):
        @pl.when(z >= zz)
        def _():
            @pl.when(z + 1 < n_z)
            def _():
                up_copy(zz).wait_send()

            for h in range(1, n_x):
                side_copy(zz, h).wait_send()

    def near_copy(b, h):
        at = pl.ds(b * half_rows, half_rows)
        src = part_ref.at[at, columns(2 * peer_y(h) + 1 - core)]
        return remote(src, near_ref.at[h, at, :], ns.at[b, h], nr.at[b, h], e, other)

    def back_copy(d, h):
        src = stage_ref.at[h, block(d), :]
        dst = far_ref.at[h, block(d), :]
        return remote(src, dst, bs.at[h, d], br.at[h, d], e, 2 * peer_y(h) + core)

    def home_copy(d):
        peer = lax.rem(e - d + n_ep, n_ep)
        return remote(
            final_ref.at[block(d), :], home_ref.at[block(e), :], hs.at[d], hr.at[d], peer, t
        )

    def pair_sum(d, h):
        return wide(part_ref[block(d), columns(2 * peer_y(h) + core)]) + wide(near_ref[h, block(d), :])

    def add_near(b):
        for h in range(n_y):
            near_copy(b, h).wait_recv()

        def one(d):
            for h in range(1, n_y):
                stage_ref[h, block(d), :] = bf(pair_sum(d, h))
                back_copy(d, h).start()

        span(b * half, (b + 1) * half, one)

    def add_far(d):
        total = pair_sum(d, 0)
        for h in range(1, n_y):
            back_copy(d, h).wait_recv()
            total = total + wide(far_ref[h, block(d), :])
        return bf(total)

    def go_home(d):
        final_ref[block(d), :] = add_far(d)
        home_copy(d).start()

    def row_block(index, q):
        return pl.ds(pl.multiple_of((2 * index + q) * rows, rows), rows)

    def mnear_copy(q, h):
        src = proj_ref.at[row_block(2 * peer_y(h) + 1 - core, q), :]
        return remote(src, mnear_ref.at[q, h], mns.at[q, h], mnr.at[q, h], e, other)

    def my_copy(q, h):
        target = 2 * peer_y(h) + core
        return remote(
            mstage_ref.at[q, h], mfar_ref.at[q, h], mys.at[q, h], myr.at[q, h], e, target
        )

    def mixer_sum(q, h):
        return wide(proj_ref[row_block(2 * peer_y(h) + core, q), :]) + wide(mnear_ref[q, h])

    def mixer_share(q):
        for h in range(1, n_y):
            mnear_copy(q, h).wait_recv()
            mstage_ref[q, h] = bf(mixer_sum(q, h))
            my_copy(q, h).start()

    def mixer_end(q):
        mnear_copy(q, 0).wait_recv()
        total = mixer_sum(q, 0)
        for h in range(1, n_y):
            my_copy(q, h).wait_recv()
            total = total + wide(mfar_ref[q, h])
        mixer_ref[q * rows : (q + 1) * rows] = bf(total)

    def project(i):
        at = pl.ds(pl.multiple_of(i * wide_model, wide_model), wide_model)
        proj_ref[:, at] = bf(mm(mixed_ref[...], out_weight_ref[:, at]))

    def widen(b):
        def unit_tile(i):
            at = pl.ds(pl.multiple_of(i * wide_units, wide_units), wide_units)
            rows_in = piece_ref[b * half_rows : (b + 1) * half_rows, :]
            gate_val = mm(rows_in, gate_ref[:, at])
            hidden_ref[:, at] = bf(gate_val * logistic(gate_val) * mm(rows_in, up_ref[:, at]))

        span(0, units // wide_units, unit_tile)

    def narrow(b):
        at = slice(b * half_rows, (b + 1) * half_rows)

        def tile(index):
            part_ref[at, columns(index)] = bf(mm(hidden_ref[...], down_ref[:, columns(index)]))

        def send(i):
            h = n_y - 1 - i
            tile(2 * peer_y(h) + 1 - core)
            near_copy(b, h).start()

        span(0, n_y, send)
        span(0, n_y, lambda i: tile(2 * i + core))

    for copy in loads:
        copy.start()
    for i in range(units // wide_units):
        for copy in gate_copy(i):
            copy.start()
    for i in range(model // wide_model):
        down_copy(i).start()
    everyone_here = meet()

    order = flag(iota((tokens, tokens), 0) < iota((tokens, tokens), 1))
    expert_rows = max(16, experts)
    own_routes = routes_ref[...]
    names = iota((expert_rows, tokens), 0)
    named = [own_routes[k : k + 1, :] == names for k in range(own_routes.shape[0])]
    match = functools.reduce(jnp.logical_or, named)
    rank = mm(bf(flag(match)), bf(order))
    rank = jnp.where(match, rank, -1.0)
    level = iota((capacity, tokens), 0).astype(jnp.float32)
    for j in range(experts):
        place_ref[j * capacity : (j + 1) * capacity] = bf(flag(level == rank[j : j + 1, :]))
    loads[0].wait()
    step_rows = 32
    for i in range(tokens // step_rows):
        at = slice(i * step_rows, (i + 1) * step_rows)
        xw = wide(x_ref[at])
        scale = lax.rsqrt(jnp.mean(xw * xw, axis=-1, keepdims=True) + norm_eps)
        normed_ref[at] = bf(xw * scale * norm_gain_ref[...])
    own = normed_ref[:, columns(t)]
    for i in range(2):
        at = slice(i * half_rows, (i + 1) * half_rows)
        cols_ref[at] = bf(mm(place_ref[at], own))
    everyone_here()
    span(1, n_ep, lambda d: ep_copy(d).start())
    for i in range(model // wide_model):
        at = slice(i * wide_model, (i + 1) * wide_model)
        piece_ref[:capacity, at] = bf(mm(place_ref[block(e), :], normed_ref[:, at]))

    for copy in loads[1:6]:
        copy.wait()
    events = 4 * (r_ref.shape[0] // (group * HEAD_DIM))
    per, lag = -(-n_ep // events), 3

    def pump(g, point):
        p = 4 * g + point
        span(jnp.maximum(p * per, 1), jnp.minimum((p + 1) * per, n_ep), arrived)
        q = p - lag
        span(jnp.maximum(q * per, 1), jnp.minimum((q + 1) * per, n_ep), pass_on)

    scan_kernel(
        group,
        pump,
        r_ref,
        k_ref,
        v_ref,
        d_ref,
        a_ref,
        d_off_ref,
        a_off_ref,
        extra_ref,
        out_ref,
        reach_ref,
        every_ref.at[e],
        chain_ref,
    )
    pass_ends(z)
    passed = max(1, min(n_ep, (events - lag) * per))
    early = max(passed, half)
    span(passed, early, pass_on)
    for i in range(units // wide_units):
        for copy in gate_copy(i):
            copy.wait()
    for i in range(model // wide_model):
        down_copy(i).wait()
    span(1, half, gathered)
    widen(0)
    span(early, n_ep, pass_on)
    span(1, min(2, n_z), relay_ends)
    narrow(0)
    span(min(2, n_z), min(3, n_z), relay_ends)
    span(half, n_ep, gathered)
    add_near(0)
    widen(1)
    span(min(3, n_z), n_z, relay_ends)
    narrow(1)
    span(0, n_z, collect_ends)
    loads[6].wait()
    loads[7].wait()
    add_near(1)
    join_kernel("ep", every_ref, out_ref, reach_ref, gate_in_ref, gain_ref, mixed_ref)
    span(0, model // wide_model, project)
    for q in range(2):
        for h in range(n_y):
            mnear_copy(q, h).start()
    span(1, half, go_home)
    mixer_share(0)
    mixer_share(1)
    span(half, n_ep, go_home)
    home_ref[block(e), :] = add_far(0)

    normed = normed_ref[...]
    group_logit = mm_nt(group_router_ref[...], normed)
    group_exp = jnp.exp(group_logit)
    group_prob = group_exp / jnp.sum(group_exp, axis=0, keepdims=True)
    expert_logit = mm_nt(expert_router_ref[...], normed)
    per_group = experts // groups
    first_of = iota((groups, tokens), 0) * per_group
    expert_names = iota((experts, tokens), 0)
    chosen, prob = [], []
    for k in range(2):
        route = own_routes[k : k + 1, :]
        chosen.append(
            jnp.sum(jnp.where(route == expert_names, expert_logit, 0.0), axis=0, keepdims=True)
        )
        inside = (route >= first_of) & (route < first_of + per_group)
        prob.append(jnp.sum(jnp.where(inside, group_prob, 0.0), axis=0, keepdims=True))
    weights = [prob[0] * logistic(chosen[0] - chosen[1]), prob[1] * logistic(chosen[1] - chosen[0])]
    weights = [jnp.transpose(jnp.broadcast_to(w, (128, tokens))) for w in weights]
    picks = []
    for k in range(2):
        parts = []
        for j in range(experts):
            at = slice(j * capacity, (j + 1) * capacity)
            parts.append(place_ref[at] * bf(flag(own_routes[k : k + 1, :] == j)))
        picks.append(jnp.concatenate(parts, axis=0))

    mixer_end(0)
    span(1, n_ep, lambda d: home_copy(d).wait_recv())
    back = home_ref[...]
    first, second = mm_tn(picks[0], back), mm_tn(picks[1], back)
    for i in range(share // 128):
        at = slice(i * 128, (i + 1) * 128)
        expert_ref[:, at] = bf(weights[0] * first[:, at] + weights[1] * second[:, at])
    mixer_end(1)

    def close(d):
        ep_copy(d).wait_send()
        core_copy(d).wait_send()
        home_copy(d).wait_send()
        for h in range(1, n_y):
            y_copy(d, h).wait_send()
            forward_copy(d, h).wait_send()

    span(1, n_ep, close)

    def close_back(d):
        for h in range(1, n_y):
            back_copy(d, h).wait_send()

    span(0, n_ep, close_back)
    for b in range(2):
        for h in range(n_y):
            near_copy(b, h).wait_send()
            mnear_copy(b, h).wait_send()
        for h in range(1, n_y):
            my_copy(b, h).wait_send()
    span(0, n_z, close_ends)


def local(
    receptance,
    key_matrix,
    value_matrix,
    decay_data_term,
    correction_rate_data,
    output_gate_input,
    decay_channel_offset,
    correction_rate_offset,
    extra_head_log_decay,
    head_norm_gain,
    mixer_output_weight,
    expert_layer_input,
    feedforward_norm_gain,
    group_router_weight,
    expert_router_weight,
    routes,
    expert_gate_weight,
    expert_up_weight,
    expert_down_weight,
):
    positions, own_width = receptance.shape
    pairs = -(-own_width // PAIR)
    width = pairs * PAIR

    def filled(x, columns=width):
        return x if x.shape[-1] == columns else jnp.pad(x, ((0, 0), (0, columns - x.shape[-1])))

    blocks = positions // HEAD_DIM
    group = 4 if blocks % 4 == 0 else 1
    n_ep, n_tp = lax.axis_size("ep"), lax.axis_size("tp")
    n_y = n_tp // 2
    n_x = 1
    while 4 * n_x * n_x <= n_ep:
        n_x = 2 * n_x
    tokens, model = expert_layer_input.shape
    capacity, share = 4 * tokens // n_ep, model // n_tp
    slots = n_ep * capacity
    units = expert_gate_weight.shape[2]
    rows = positions // n_tp
    out_weight = jnp.pad(mixer_output_weight, ((0, width - own_width), (0, 0)))

    def held(*shape):
        return pltpu.VMEM(shape, jnp.bfloat16)

    def sems(*shape):
        return pltpu.SemaphoreType.DMA(shape)

    in_vmem, in_hbm = pl.BlockSpec(memory_space=pltpu.VMEM), pl.BlockSpec(memory_space=pltpu.HBM)
    one, many = sems(n_ep), sems(n_y, n_ep)
    mixer_out, expert_out = pl.pallas_call(
        functools.partial(whole_kernel, group),
        out_shape=(
            jax.ShapeDtypeStruct((rows, model), jnp.bfloat16),
            jax.ShapeDtypeStruct((tokens, share), jnp.bfloat16),
        ),
        in_specs=[in_hbm] * 6
        + [in_vmem] * 4
        + [in_hbm] * 2
        + [in_vmem] * 4
        + [in_hbm] * 3,
        out_specs=[in_vmem] * 2,
        scratch_shapes=[held(positions, width)] * 6
        + [
            held(width, model),
            held(tokens, model),
            held(tokens, model),
            held(slots, tokens),
            held(slots, share),
            held(slots, model),
            pltpu.VMEM((positions, width), jnp.float32),
            held(positions, width),
            held(n_ep, pairs * 2 * HEAD_DIM, PAIR),
            pltpu.VMEM((pairs, 2 * PAIR, PAIR), jnp.float32),
            held(positions, width),
            held(positions, model),
            held(model, units),
            held(model, units),
            held(units, model),
            held(slots // 2, units),
            held(slots, model),
        ]
        + [held(n_y, slots, share)] * 3
        + [held(slots, share)] * 2
        + [held(2, n_y, rows // 2, model)] * 3
        + [sems(8)]
        + [sems(max(1, units // 256))] * 2
        + [sems(max(1, model // 512))]
        + [one] * 4
        + [many] * 4
        + [sems(n_ep // n_x)] * 2
        + [sems(n_x, n_ep // n_x)] * 2
        + [sems(2, n_y)] * 2
        + [many] * 2
        + [one] * 2
        + [sems(2, n_y)] * 4,
        compiler_params=pltpu.CompilerParams(
            collective_id=0, has_side_effects=True, vmem_limit_bytes=VMEM_LIMIT
        ),
    )(
        filled(receptance),
        filled(key_matrix),
        filled(value_matrix),
        filled(decay_data_term),
        filled(correction_rate_data),
        filled(output_gate_input),
        filled(decay_channel_offset[None]),
        filled(correction_rate_offset[None]),
        filled(extra_head_log_decay, 2 * pairs),
        filled(head_norm_gain[None]),
        out_weight,
        expert_layer_input,
        feedforward_norm_gain[None],
        group_router_weight.T,
        expert_router_weight.T,
        routes.T,
        expert_gate_weight,
        expert_up_weight,
        expert_down_weight,
    )
    return mixer_out, expert_out


def solution(mesh):
    in_specs = (
        P("ep", "tp"),
        P("ep", "tp"),
        P("ep", "tp"),
        P("ep", "tp"),
        P("ep", "tp"),
        P("ep", "tp"),
        P("tp"),
        P("tp"),
        P("ep", "tp"),
        P("tp"),
        P("tp", None),
        P("ep", None),
        P(),
        P(),
        P(),
        P("ep", None),
        P("ep", None, "tp"),
        P("ep", None, "tp"),
        P("ep", "tp", None),
    )
    out_specs = (P(("ep", "tp"), None), P("ep", "tp"))
    return jax.shard_map(local, mesh=mesh, in_specs=in_specs, out_specs=out_specs, check_vma=False)
```

```python
import functools
import math

import jax
import jax.numpy as jnp
from jax import lax
from jax.experimental import pallas as pl
from jax.experimental.pallas import tpu as pltpu
from jax.sharding import PartitionSpec as P

HEAD_DIM = 64
PAIR = 2 * HEAD_DIM
VMEM_LIMIT = 48 << 20
HALF_EXP = math.exp(-0.5)
GROUPS = 4


key_eps = 1e-06
group_eps = 0.00064
norm_eps = 1e-06
highest = lax.Precision.HIGHEST


def bf(x):
    return x.astype(jnp.bfloat16)


def mm(x, y):
    return lax.dot_general(x, y, (((1,), (0,)), ((), ())), preferred_element_type=jnp.float32)


def mm_nt(x, y):
    return lax.dot_general(x, y, (((1,), (1,)), ((), ())), preferred_element_type=jnp.float32)


def mm_tn(x, y):
    return lax.dot_general(x, y, (((0,), (0,)), ((), ())), preferred_element_type=jnp.float32)


def halves(x):
    high = bf(x)
    return high, bf(x - high.astype(jnp.float32))


def sum_right(x, ones):
    high, low = halves(x)
    return mm(high, ones) + mm(low, ones)


def logistic(x):
    return 1.0 / (1.0 + jnp.exp(-x))


def flag(cond):
    return jnp.where(cond, 1.0, 0.0)


def iota(shape, dim):
    return lax.broadcasted_iota(jnp.int32, shape, dim)


def pair_blocks():
    return flag((iota((PAIR, PAIR), 0) < HEAD_DIM) == (iota((PAIR, PAIR), 1) < HEAD_DIM))


def scan_kernel(
    group,
    pump,
    r_ref,
    k_ref,
    v_ref,
    d_ref,
    a_ref,
    d_off_ref,
    a_off_ref,
    extra_ref,
    out_ref,
    reach_ref,
    ends_ref,
    chain_ref,
):
    positions, width = r_ref.shape
    pairs = width // PAIR
    C = HEAD_DIM
    rows_per = group * C
    own_block = pair_blocks()
    own_bf = bf(own_block)
    row, col = iota((C, PAIR), 0), iota((C, PAIR), 1) & (HEAD_DIM - 1)
    strict, upto = row > col, row >= col
    eye = flag(row == col)
    tri = bf(flag(iota((C, C), 0) >= iota((C, C), 1)))
    level_masks = []
    for s in range(6):
        inside = (
            ((row >> (s + 1)) == (col >> (s + 1)))
            & (((row >> s) & 1) == 1)
            & (((col >> s) & 1) == 0)
        )
        level_masks.append(bf(flag(inside)))

    def spread(x):
        return jnp.concatenate([x, x], axis=0) * own_bf

    square = (iota((PAIR, PAIR), 0) == iota((PAIR, PAIR), 1)).astype(jnp.float32)
    for p in range(pairs):
        chain_ref[p, :PAIR] = jnp.zeros((PAIR, PAIR), jnp.float32)
        chain_ref[p, PAIR:] = square

    def step(g, carry):
        base = pl.multiple_of(g * rows_per, rows_per)
        rows = pl.ds(base, rows_per)
        items = []
        for p in range(pairs):
            lanes = slice(p * PAIR, (p + 1) * PAIR)
            k = k_ref[rows, lanes].astype(jnp.float32)
            u = k * lax.rsqrt(sum_right(k * k, own_bf) + key_eps)
            rem = u * logistic(a_ref[rows, lanes].astype(jnp.float32) + a_off_ref[:, lanes])
            lg = extra_ref[rows, lanes] - HALF_EXP * logistic(
                d_ref[rows, lanes].astype(jnp.float32) + d_off_ref[:, lanes]
            )
            r = r_ref[rows, lanes].astype(jnp.float32)
            v = v_ref[rows, lanes]
            for c in range(group):
                cut = slice(c * C, (c + 1) * C)
                items.append((p, c, k[cut], u[cut], rem[cut], lg[cut], r[cut], v[cut]))
        stage = []
        for p, c, k, u, rem, lg, r, v in items:
            high, low = halves(lg)
            rest = bf(lg - high.astype(jnp.float32) - low.astype(jnp.float32))
            cumul = mm(tri, high) + mm(tri, low) + mm(tri, rest)
            stage.append(cumul)
        work = []
        for (p, c, k, u, rem, lg, r, v), cumul in zip(items, stage):
            mid = 0.5 * cumul[C - 1 : C]
            up_now, down = jnp.exp(cumul - mid), jnp.exp(mid - cumul)
            up_before = jnp.exp(cumul - lg - mid)
            half = jnp.exp(mid)
            cq, cu, dk, dr = r * up_now, u * up_before, k * down, rem * down
            left = bf(jnp.concatenate([cu, cq], axis=0))
            pair_r = mm_nt(left, spread(bf(dr)))
            pair_k = mm_nt(left, spread(bf(dk)))
            work.append((cq * half, bf(cu * half), bf(dk * half), bf(dr * half), half * half, pair_r, pair_k))
        pump(g, 0)
        solve = []
        for (p, c, k, u, rem, lg, r, v), (qe, ue, kt, rt, ed, pair_r, pair_k) in zip(items, work):
            rp = bf(jnp.where(strict, pair_r[:C], 0.0))
            rr = bf(jnp.where(upto, pair_r[C:], 0.0))
            kp = jnp.where(strict, pair_k[:C], 0.0)
            rk = jnp.where(upto, pair_k[C:], 0.0)
            kv = mm(bf(jnp.concatenate([kp, rk], axis=0)), spread(v))
            inv = eye - (rp * level_masks[0]).astype(jnp.float32)
            solve.append([rp, rr, kv, inv])
        for s in range(1, 6):
            mids = [bf(mm(bf(inv), spread(rp * level_masks[s]))) for rp, rr, kv, inv in solve]
            for item, y in zip(solve, mids):
                item[3] = item[3] - mm(y, spread(bf(item[3])))
            if s == 2:
                pump(g, 1)
        wvs = []
        for (rp, rr, kv, inv), w in zip(solve, work):
            wide = jnp.concatenate([spread(w[1]), spread(bf(kv[:C]))], axis=1)
            wvs.append(bf(mm(bf(inv), wide)))
        pump(g, 2)
        tails = []
        for (rp, rr, kv, inv), (qe, ue, kt, rt, ed, _, _), wv, item in zip(solve, work, wvs, items):
            wide = jnp.concatenate([spread(wv[:, :PAIR]), spread(wv[:, PAIR:])], axis=1)
            rw = mm(rr, wide)
            read = bf(qe - rw[:, :PAIR])
            local = kv[C:] - rw[:, PAIR:]
            v = item[7]
            x = jnp.concatenate(
                [jnp.concatenate([v, jnp.zeros_like(v)], axis=1),
                 jnp.concatenate([-wv[:, PAIR:], -wv[:, :PAIR]], axis=1)], axis=0)
            nb = mm_tn(x, jnp.concatenate([kt, rt], axis=0))
            tails.append((read, local, nb[:PAIR] * own_block, bf(nb[PAIR:] * own_block), ed))
        z = [chain_ref[p] for p in range(pairs)]
        for c in range(group):
            for p in range(pairs):
                read, local, add, neg, ed = tails[p * group + c]
                zb = bf(z[p])
                qz = mm_nt(read, zb)
                at = pl.ds(pl.multiple_of(base + c * C, C), C)
                lanes = slice(p * PAIR, (p + 1) * PAIR)
                out_ref[at, lanes] = local + qz[:, :PAIR]
                reach_ref[at, lanes] = bf(qz[:, PAIR:])
                moved = z[p] * ed + mm(zb, neg)
                z[p] = jnp.concatenate([moved[:PAIR] + add, moved[PAIR:]], axis=0)
        for p in range(pairs):
            chain_ref[p] = z[p]
        pump(g, 3)
        return carry

    lax.fori_loop(0, positions // rows_per, step, 0)
    for p in range(pairs):
        s, m = chain_ref[p, :PAIR], chain_ref[p, PAIR:]
        ends_ref[p * 2 * C : p * 2 * C + C] = bf(s[:C] + s[C:])
        ends_ref[p * 2 * C + C : (p + 1) * 2 * C] = bf(m[:C] + m[C:])


def join_kernel(axis, all_ref, out_ref, reach_ref, gate_ref, gain_ref, mixed_ref):
    devices, place = lax.axis_size(axis), lax.axis_index(axis)
    width = out_ref.shape[1]
    pairs = width // PAIR
    C = HEAD_DIM
    own_block = pair_blocks()
    own_bf = bf(own_block)
    mean_bf = bf(own_block * (1.0 / HEAD_DIM))
    states = [jnp.zeros((C, PAIR), jnp.float32) for _ in range(pairs)]

    def hop(j, states):
        new = []
        for p in range(pairs):
            s = all_ref[j, p * 2 * C : p * 2 * C + C].astype(jnp.float32)
            m = all_ref[j, p * 2 * C + C : (p + 1) * 2 * C]
            m = jnp.concatenate([m, m], axis=0) * own_bf
            new.append(sum_right(states[p], m) + s)
        return tuple(new)

    states = lax.fori_loop(0, place, hop, tuple(states))
    for p in range(pairs):
        lanes = slice(p * PAIR, (p + 1) * PAIR)
        s = bf(states[p])
        s = jnp.concatenate([s, s], axis=0) * own_bf
        head = out_ref[:, lanes] + mm_nt(reach_ref[:, lanes], s)
        centred = head - sum_right(head, mean_bf)
        spread = sum_right(centred * centred, mean_bf)
        normed = centred * lax.rsqrt(spread + group_eps)
        gate = logistic(gate_ref[:, lanes].astype(jnp.float32))
        mixed_ref[:, lanes] = bf(normed * gain_ref[:, lanes] * gate)


def place_of():
    n_ep, n_tp = lax.axis_size("ep"), lax.axis_size("tp")
    e, t = lax.axis_index("ep"), lax.axis_index("tp")
    core = lax.rem(t, 2)
    return n_ep, n_tp, n_tp // 2, e, t, lax.div(t, 2), core


def remote(src, dst, send, recv, e, t):
    return pltpu.make_async_remote_copy(
        src_ref=src,
        dst_ref=dst,
        send_sem=send,
        recv_sem=recv,
        device_id=(e, t),
        device_id_type=pl.DeviceIdType.MESH,
    )


def meet():
    n_ep, n_tp, n_y, e, t, y, core = place_of()
    barrier = pltpu.get_barrier_semaphore()

    def greet(pe, pt):
        pl.semaphore_signal(
            barrier, inc=1, device_id=(pe, pt), device_id_type=pl.DeviceIdType.MESH
        )

    for d in range(1, n_ep):
        greet(lax.rem(e + d, n_ep), t)
    greet(e, 2 * y + 1 - core)
    for d in range(1, n_y):
        greet(e, 2 * lax.rem(y + d, n_y) + core)
    return lambda: pl.semaphore_wait(barrier, n_ep - 1 + n_y)


def span(first, last, body):
    def run(d, carry):
        body(d)
        return carry

    lax.fori_loop(first, last, run, 0)


def wide(x):
    return x.astype(jnp.float32)


def whole_kernel(
    group,
    r_hbm,
    k_hbm,
    v_hbm,
    d_hbm,
    a_hbm,
    gate_in_hbm,
    d_off_hbm,
    a_off_hbm,
    extra_hbm,
    gain_hbm,
    out_weight_hbm,
    x_hbm,
    norm_gain_hbm,
    group_router_hbm,
    expert_router_hbm,
    routes_hbm,
    gate_hbm,
    up_hbm,
    down_hbm,
    mixer_ref,
    expert_ref,
    r_ref,
    k_ref,
    v_ref,
    d_ref,
    a_ref,
    gate_in_ref,
    out_weight_ref,
    x_ref,
    d_off_ref,
    a_off_ref,
    extra_in_ref,
    gain_ref,
    norm_gain_ref,
    group_router_ref,
    expert_router_ref,
    routes_ref,
    extra_parts_ref,
    extra_ref,
    normed_ref,
    place_ref,
    cols_ref,
    piece_ref,
    out_ref,
    reach_ref,
    every_ref,
    chain_ref,
    mixed_ref,
    proj_ref,
    gate_ref,
    up_ref,
    down_ref,
    hidden_ref,
    part_ref,
    near_ref,
    stage_ref,
    far_ref,
    final_ref,
    home_ref,
    mnear_ref,
    mstage_ref,
    mfar_ref,
    in_sem,
    gate_sem,
    up_sem,
    down_sem,
    es,
    er,
    cs,
    cr,
    ys,
    yr,
    fs,
    fr,
    zs,
    zr,
    gs,
    gr,
    ns,
    nr,
    bs,
    br,
    hs,
    hr,
    mns,
    mnr,
    mys,
    myr,
):
    n_ep, n_tp, n_y, e, t, y, core = place_of()
    units = gate_ref.shape[1]
    model = x_ref.shape[1]
    tokens = x_ref.shape[0]
    share = model // n_tp
    slots = piece_ref.shape[0]
    capacity = slots // n_ep
    experts = expert_router_ref.shape[0]
    groups = group_router_ref.shape[0]
    positions = proj_ref.shape[0]
    rows = positions // n_tp
    other = 2 * y + 1 - core
    half = n_ep // 2
    half_rows = half * capacity
    wide_units, wide_model = min(256, units), min(512, model)

    inputs = [(routes_hbm, routes_ref), (norm_gain_hbm, norm_gain_ref), (x_hbm, x_ref)]
    inputs += [(extra_hbm, extra_in_ref), (d_off_hbm, d_off_ref), (a_off_hbm, a_off_ref)]
    inputs += [(k_hbm, k_ref), (a_hbm, a_ref), (d_hbm, d_ref), (r_hbm, r_ref), (v_hbm, v_ref)]
    inputs += [(gate_in_hbm, gate_in_ref), (out_weight_hbm, out_weight_ref), (gain_hbm, gain_ref)]
    inputs += [(group_router_hbm, group_router_ref), (expert_router_hbm, expert_router_ref)]
    loads = [pltpu.make_async_copy(s, d, in_sem.at[i]) for i, (s, d) in enumerate(inputs)]

    def gate_copy(i):
        at = pl.ds(pl.multiple_of(i * wide_units, wide_units), wide_units)
        return (
            pltpu.make_async_copy(gate_hbm.at[0, :, at], gate_ref.at[:, at], gate_sem.at[i]),
            pltpu.make_async_copy(up_hbm.at[0, :, at], up_ref.at[:, at], up_sem.at[i]),
        )

    def down_copy(i):
        at = pl.ds(pl.multiple_of(i * wide_model, wide_model), wide_model)
        return pltpu.make_async_copy(down_hbm.at[0, :, at], down_ref.at[:, at], down_sem.at[i])

    def partner(d):
        bit, total = 1, 0
        while bit < n_ep:
            total = total + lax.rem(lax.div(e, bit) + lax.div(d, bit), 2) * bit
            bit = 2 * bit
        return total

    def columns(index):
        return pl.ds(pl.multiple_of(index * share, share), share)

    def block(d):
        return pl.ds(pl.multiple_of(d * capacity, capacity), capacity)

    def peer_y(h):
        return lax.rem(y + h, n_y)

    def ep_copy(d):
        peer = partner(d)
        return remote(
            cols_ref.at[block(peer), :], piece_ref.at[block(d), columns(t)], es.at[d], er.at[d], peer, t
        )

    def core_copy(d):
        ref = piece_ref.at[block(d), columns(t)]
        return remote(ref, ref, cs.at[d], cr.at[d], e, other)

    def y_copy(d, h):
        ref = piece_ref.at[block(d), columns(t)]
        return remote(ref, ref, ys.at[h, d], yr.at[h, d], e, 2 * peer_y(h) + core)

    def forward_copy(d, h):
        ref = piece_ref.at[block(d), columns(2 * lax.rem(y - h + n_y, n_y) + core)]
        return remote(ref, ref, fs.at[h, d], fr.at[h, d], e, other)

    def arrived(d):
        ep_copy(d).wait_recv()
        for h in range(1, n_y):
            y_copy(d, h).start()
        core_copy(d).start()

    def pass_on(d):
        for h in range(1, n_y):
            y_copy(d, h).wait_recv()
            forward_copy(d, h).start()

    def gathered(d):
        core_copy(d).wait_recv()
        for h in range(1, n_y):
            forward_copy(d, h).wait_recv()

    n_x = gs.shape[0]
    n_z = n_ep // n_x
    z, x = lax.div(e, n_x), lax.rem(e, n_x)

    def up_copy(zz):
        ref = every_ref.at[zz * n_x + x]
        return remote(ref, ref, zs.at[zz], zr.at[zz], e + n_x, t)

    def side_copy(zz, h):
        ref = every_ref.at[zz * n_x + x]
        peer = z * n_x + lax.rem(x + h, n_x)
        return remote(ref, ref, gs.at[h, zz], gr.at[h, zz], peer, t)

    def pass_ends(zz):
        @pl.when(z + 1 < n_z)
        def _():
            up_copy(zz).start()

        for h in range(1, n_x):
            side_copy(zz, h).start()

    def relay_ends(i):
        @pl.when(z >= i)
        def _():
            up_copy(z - i).wait_recv()
            pass_ends(z - i)

    def collect_ends(zz):
        @pl.when(z >= zz)
        def _():
            for h in range(1, n_x):
                side_copy(zz, h).wait_recv()

    def close_ends(zz):
        @pl.when(z >= zz)
        def _():
            @pl.when(z + 1 < n_z)
            def _():
                up_copy(zz).wait_send()

            for h in range(1, n_x):
                side_copy(zz, h).wait_send()

    def near_copy(b, h):
        at = pl.ds(b * half_rows, half_rows)
        src = part_ref.at[at, columns(2 * peer_y(h) + 1 - core)]
        return remote(src, near_ref.at[h, at, :], ns.at[b, h], nr.at[b, h], e, other)

    def back_copy(d, h):
        src = stage_ref.at[h, block(d), :]
        dst = far_ref.at[h, block(d), :]
        return remote(src, dst, bs.at[h, d], br.at[h, d], e, 2 * peer_y(h) + core)

    def home_copy(d):
        peer = partner(d)
        return remote(
            final_ref.at[block(d), :], home_ref.at[block(e), :], hs.at[d], hr.at[d], peer, t
        )

    def pair_sum(d, h):
        return wide(part_ref[block(d), columns(2 * peer_y(h) + core)]) + wide(near_ref[h, block(d), :])

    def add_near(b):
        for h in range(n_y):
            near_copy(b, h).wait_recv()

        def one(d):
            for h in range(1, n_y):
                stage_ref[h, block(d), :] = bf(pair_sum(d, h))
                back_copy(d, h).start()

        span(b * half, (b + 1) * half, one)

    def add_far(d):
        total = pair_sum(d, 0)
        for h in range(1, n_y):
            back_copy(d, h).wait_recv()
            total = total + wide(far_ref[h, block(d), :])
        return bf(total)

    def go_home(d):
        final_ref[block(d), :] = add_far(d)
        home_copy(d).start()

    tile_count = model // wide_model

    def tile_of(i):
        return slice(i * wide_model, (i + 1) * wide_model)

    def row_block(index):
        return pl.ds(pl.multiple_of(index * rows, rows), rows)

    def mnear_copy(i, h):
        src = proj_ref.at[row_block(2 * peer_y(h) + 1 - core), tile_of(i)]
        return remote(src, mnear_ref.at[i, h], mns.at[i, h], mnr.at[i, h], e, other)

    def my_copy(i, h):
        target = 2 * peer_y(h) + core
        return remote(
            mstage_ref.at[i, h], mfar_ref.at[i, h], mys.at[i, h], myr.at[i, h], e, target
        )

    def mixer_sum(i, h):
        return wide(proj_ref[row_block(2 * peer_y(h) + core), tile_of(i)]) + wide(mnear_ref[i, h])

    def project(i):
        proj_ref[:, tile_of(i)] = bf(mm(mixed_ref[...], out_weight_ref[:, tile_of(i)]))
        for h in range(n_y):
            mnear_copy(i, h).start()

    def mixer_share(i):
        for h in range(1, n_y):
            mnear_copy(i, h).wait_recv()
            mstage_ref[i, h] = bf(mixer_sum(i, h))
            my_copy(i, h).start()

    def mixer_end(i):
        mnear_copy(i, 0).wait_recv()
        total = mixer_sum(i, 0)
        for h in range(1, n_y):
            my_copy(i, h).wait_recv()
            total = total + wide(mfar_ref[i, h])
        mixer_ref[:, tile_of(i)] = bf(total)

    def tiles(count, body, hooks):
        for i in range(count):
            body(i)
            for hook in hooks.get(i, ()):
                hook()
        for i in sorted(hooks):
            for hook in hooks[i] if i >= count else ():
                hook()

    def widen(b, hooks):
        def unit_tile(i):
            at = slice(i * wide_units, (i + 1) * wide_units)
            if b == 0:
                for copy in gate_copy(i):
                    copy.wait()
            rows_in = piece_ref[b * half_rows : (b + 1) * half_rows, :]
            gate_val = mm(rows_in, gate_ref[:, at])
            hidden_ref[:, at] = bf(gate_val * logistic(gate_val) * mm(rows_in, up_ref[:, at]))

        tiles(units // wide_units, unit_tile, hooks)

    def narrow(b, hooks):
        at = slice(b * half_rows, (b + 1) * half_rows)
        if b == 0:
            for i in range(tile_count):
                down_copy(i).wait()

        def tile(i):
            h = n_y - 1 - i % n_y
            index = 2 * peer_y(h) + (1 - core if i < n_y else core)
            part_ref[at, columns(index)] = bf(mm(hidden_ref[...], down_ref[:, columns(index)]))
            if i < n_y:
                near_copy(b, h).start()

        tiles(n_tp, tile, hooks)

    for copy in loads:
        copy.start()
    for i in range(units // wide_units):
        for copy in gate_copy(i):
            copy.start()
    for i in range(model // wide_model):
        down_copy(i).start()
    everyone_here = meet()

    order = flag(iota((tokens, tokens), 0) < iota((tokens, tokens), 1))
    expert_rows = max(16, experts)
    loads[0].wait()
    loads[1].wait()
    own_routes = routes_ref[...]
    names = iota((expert_rows, tokens), 0)
    named = [own_routes[k : k + 1, :] == names for k in range(own_routes.shape[0])]
    match = functools.reduce(jnp.logical_or, named)
    rank = mm(bf(flag(match)), bf(order))
    rank = jnp.where(match, rank, -1.0)
    level = iota((capacity, tokens), 0).astype(jnp.float32)
    for j in range(experts):
        place_ref[j * capacity : (j + 1) * capacity] = bf(flag(level == rank[j : j + 1, :]))
    loads[2].wait()
    step_rows = 32
    for i in range(tokens // step_rows):
        at = slice(i * step_rows, (i + 1) * step_rows)
        xw = wide(x_ref[at])
        scale = lax.rsqrt(jnp.mean(xw * xw, axis=-1, keepdims=True) + norm_eps)
        normed_ref[at] = bf(xw * scale * norm_gain_ref[...])
    own = normed_ref[:, columns(t)]
    for i in range(2):
        at = slice(i * half_rows, (i + 1) * half_rows)
        cols_ref[at] = bf(mm(place_ref[at], own))
    everyone_here()
    span(1, n_ep, lambda d: ep_copy(d).start())
    for i in range(model // wide_model):
        at = slice(i * wide_model, (i + 1) * wide_model)
        piece_ref[:capacity, at] = bf(mm(place_ref[block(e), :], normed_ref[:, at]))

    for copy in loads[3:11]:
        copy.wait()
    heads, pairs = extra_in_ref.shape[0], chain_ref.shape[0]
    exact = extra_in_ref[...]
    extra_parts_ref[...] = jnp.zeros(extra_parts_ref.shape, jnp.float32)
    for i in range(3):
        piece = wide(bf(exact))
        extra_parts_ref[i * heads : (i + 1) * heads, :] = piece
        exact = exact - piece
    extra_parts = bf(extra_parts_ref[...])
    extra_rows = extra_parts_ref.shape[0]
    for p in range(pairs):
        head = lax.rem(iota((extra_rows, PAIR), 0), heads)
        wanted = head == 2 * p + lax.div(iota((extra_rows, PAIR), 1), HEAD_DIM)
        extra_ref[:, p * PAIR : (p + 1) * PAIR] = mm_tn(extra_parts, bf(flag(wanted)))
    steps = positions // (group * HEAD_DIM)
    per = max(1, n_ep // 8)

    def unit(u, body):
        lo = max(1, min(n_ep, u * per))
        return lambda: span(lo, max(lo, min(n_ep, (u + 1) * per)), body)

    events = {
        1: [unit(0, arrived)],
        2: [unit(1, arrived)],
        3: [unit(2, arrived)],
        4: [unit(3, arrived), unit(0, pass_on)],
        5: [unit(1, pass_on)],
        6: [unit(4, arrived), unit(2, pass_on)],
        7: [unit(5, arrived), unit(3, pass_on)],
    }

    def pump(g, point):
        for step in range(steps):
            due = events.get(4 * step + point)
            if due:

                @pl.when(g == step)
                def _(due=due):
                    for act in due:
                        act()

    scan_kernel(
        group,
        pump,
        r_ref,
        k_ref,
        v_ref,
        d_ref,
        a_ref,
        d_off_ref,
        a_off_ref,
        extra_ref,
        out_ref,
        reach_ref,
        every_ref.at[e],
        chain_ref,
    )
    for i in sorted(events):
        for act in events[i] if i >= 4 * steps else ():
            act()
    pass_ends(z)
    span(1, half, gathered)
    widen(0, {0: [unit(6, arrived)], 1: [unit(4, pass_on)], 2: [unit(7, arrived), unit(5, pass_on)]})
    relay_ends(1) if n_z > 1 else None
    narrow(0, {1: [unit(6, pass_on)]})
    add_near(0)
    unit(7, pass_on)()
    span(half, n_ep, gathered)
    relays = [lambda i=i: relay_ends(i) for i in range(2, n_z)]
    widen(1, {1: relays[:1]})
    narrow(1, {})
    for relay in relays[1:]:
        relay()
    add_near(1)
    span(1, half, go_home)
    for copy in loads[11:]:
        copy.wait()
    span(0, n_z, collect_ends)
    join_kernel("ep", every_ref, out_ref, reach_ref, gate_in_ref, gain_ref, mixed_ref)
    homes = [unit(u, go_home) for u in range(4, 8)]
    homes[0]()
    for i in range(tile_count):
        project(i)
    homes[1]()
    for i in range(tile_count):
        mixer_share(i)
    homes[2]()
    homes[3]()
    home_ref[block(e), :] = add_far(0)

    normed = normed_ref[...]
    group_logit = mm_nt(group_router_ref[...], normed)
    group_exp = jnp.exp(group_logit)
    group_prob = group_exp / jnp.sum(group_exp, axis=0, keepdims=True)
    expert_logit = mm_nt(expert_router_ref[...], normed)
    per_group = experts // groups
    first_of = iota((groups, tokens), 0) * per_group
    expert_names = iota((experts, tokens), 0)
    chosen, prob = [], []
    for k in range(2):
        route = own_routes[k : k + 1, :]
        chosen.append(
            jnp.sum(jnp.where(route == expert_names, expert_logit, 0.0), axis=0, keepdims=True)
        )
        inside = (route >= first_of) & (route < first_of + per_group)
        prob.append(jnp.sum(jnp.where(inside, group_prob, 0.0), axis=0, keepdims=True))
    weights = [prob[0] * logistic(chosen[0] - chosen[1]), prob[1] * logistic(chosen[1] - chosen[0])]
    weights = [jnp.transpose(jnp.broadcast_to(w, (128, tokens))) for w in weights]
    picks = []
    for k in range(2):
        parts = []
        for j in range(experts):
            at = slice(j * capacity, (j + 1) * capacity)
            parts.append(place_ref[at] * bf(flag(own_routes[k : k + 1, :] == j)))
        picks.append(jnp.concatenate(parts, axis=0))

    for i in range(tile_count - 1):
        mixer_end(i)
    span(1, n_ep, lambda d: home_copy(d).wait_recv())
    back = home_ref[...]
    first, second = mm_tn(picks[0], back), mm_tn(picks[1], back)
    for i in range(share // 128):
        at = slice(i * 128, (i + 1) * 128)
        expert_ref[:, at] = bf(weights[0] * first[:, at] + weights[1] * second[:, at])
    mixer_end(tile_count - 1)

    def close(d):
        ep_copy(d).wait_send()
        core_copy(d).wait_send()
        home_copy(d).wait_send()
        for h in range(1, n_y):
            y_copy(d, h).wait_send()
            forward_copy(d, h).wait_send()

    span(1, n_ep, close)

    def close_back(d):
        for h in range(1, n_y):
            back_copy(d, h).wait_send()

    span(0, n_ep, close_back)
    for b in range(2):
        for h in range(n_y):
            near_copy(b, h).wait_send()
    for i in range(tile_count):
        for h in range(n_y):
            mnear_copy(i, h).wait_send()
        for h in range(1, n_y):
            my_copy(i, h).wait_send()
    span(0, n_z, close_ends)


def local(
    receptance,
    key_matrix,
    value_matrix,
    decay_data_term,
    correction_rate_data,
    output_gate_input,
    decay_channel_offset,
    correction_rate_offset,
    extra_head_log_decay,
    head_norm_gain,
    mixer_output_weight,
    expert_layer_input,
    feedforward_norm_gain,
    group_router_weight,
    expert_router_weight,
    routes,
    expert_gate_weight,
    expert_up_weight,
    expert_down_weight,
):
    positions, own_width = receptance.shape
    pairs = -(-own_width // PAIR)
    width = pairs * PAIR

    def filled(x, columns=width):
        return x if x.shape[-1] == columns else jnp.pad(x, ((0, 0), (0, columns - x.shape[-1])))

    blocks = positions // HEAD_DIM
    group = 4 if blocks % 4 == 0 else 1
    n_ep, n_tp = lax.axis_size("ep"), lax.axis_size("tp")
    n_y = n_tp // 2
    n_x = 1
    while 4 * n_x * n_x <= n_ep:
        n_x = 2 * n_x
    tokens, model = expert_layer_input.shape
    capacity, share = 4 * tokens // n_ep, model // n_tp
    slots = n_ep * capacity
    units = expert_gate_weight.shape[2]
    rows = positions // n_tp
    tile_count = max(1, model // 512)
    out_weight = jnp.pad(mixer_output_weight, ((0, width - own_width), (0, 0)))

    def held(*shape):
        return pltpu.VMEM(shape, jnp.bfloat16)

    def single(*shape):
        return pltpu.VMEM(shape, jnp.float32)

    def sems(*shape):
        return pltpu.SemaphoreType.DMA(shape)

    operands = (
        filled(receptance),
        filled(key_matrix),
        filled(value_matrix),
        filled(decay_data_term),
        filled(correction_rate_data),
        filled(output_gate_input),
        filled(decay_channel_offset[None]),
        filled(correction_rate_offset[None]),
        filled(extra_head_log_decay, 2 * pairs).T,
        filled(head_norm_gain[None]),
        out_weight,
        expert_layer_input,
        feedforward_norm_gain[None],
        group_router_weight.T,
        expert_router_weight.T,
        routes.T,
        expert_gate_weight,
        expert_up_weight,
        expert_down_weight,
    )
    in_vmem, in_hbm = pl.BlockSpec(memory_space=pltpu.VMEM), pl.BlockSpec(memory_space=pltpu.HBM)
    one, many = sems(n_ep), sems(n_y, n_ep)
    mixer_out, expert_out = pl.pallas_call(
        functools.partial(whole_kernel, group),
        out_shape=(held(rows, model), held(tokens, share)),
        in_specs=[in_hbm] * 19,
        out_specs=[in_vmem] * 2,
        scratch_shapes=[held(positions, width)] * 6
        + [
            held(width, model),
            held(tokens, model),
            single(1, width),
            single(1, width),
            single(2 * pairs, positions),
            single(1, width),
            single(1, model),
            held(*group_router_weight.shape[::-1]),
            held(*expert_router_weight.shape[::-1]),
            pltpu.VMEM(routes.shape[::-1], jnp.int32),
            single(16, positions),
            single(positions, width),
            held(tokens, model),
            held(slots, tokens),
            held(slots, share),
            held(slots, model),
            single(positions, width),
            held(positions, width),
            held(n_ep, pairs * 2 * HEAD_DIM, PAIR),
            single(pairs, 2 * PAIR, PAIR),
            held(positions, width),
            held(positions, model),
            held(model, units),
            held(model, units),
            held(units, model),
            held(slots // 2, units),
            held(slots, model),
        ]
        + [held(n_y, slots, share)] * 3
        + [held(slots, share)] * 2
        + [held(tile_count, n_y, rows, model // tile_count)] * 3
        + [sems(16)]
        + [sems(max(1, units // 256))] * 2
        + [sems(max(1, model // 512))]
        + [one] * 4
        + [many] * 4
        + [sems(n_ep // n_x)] * 2
        + [sems(n_x, n_ep // n_x)] * 2
        + [sems(2, n_y)] * 2
        + [many] * 2
        + [one] * 2
        + [sems(tile_count, n_y)] * 4,
        compiler_params=pltpu.CompilerParams(
            collective_id=0, has_side_effects=True, vmem_limit_bytes=VMEM_LIMIT
        ),
    )(
        *(pltpu.with_memory_space_constraint(x, pltpu.HBM) for x in operands)
    )
    return mixer_out, expert_out


def solution(mesh):
    in_specs = (
        P("ep", "tp"),
        P("ep", "tp"),
        P("ep", "tp"),
        P("ep", "tp"),
        P("ep", "tp"),
        P("ep", "tp"),
        P("tp"),
        P("tp"),
        P("ep", "tp"),
        P("tp"),
        P("tp", None),
        P("ep", None),
        P(),
        P(),
        P(),
        P("ep", None),
        P("ep", None, "tp"),
        P("ep", None, "tp"),
        P("ep", "tp", None),
    )
    out_specs = (P(("ep", "tp"), None), P("ep", "tp"))
    return jax.shard_map(local, mesh=mesh, in_specs=in_specs, out_specs=out_specs, check_vma=False)
```

```python
import functools
import math

import jax
import jax.numpy as jnp
from jax import lax
from jax.experimental import pallas as pl
from jax.experimental.pallas import tpu as pltpu
from jax.sharding import PartitionSpec as P

HEAD_DIM = 64
PAIR = 2 * HEAD_DIM
VMEM_LIMIT = 48 << 20
HALF_EXP = math.exp(-0.5)
GROUPS = 4


key_eps = 1e-06
group_eps = 0.00064
norm_eps = 1e-06
highest = lax.Precision.HIGHEST


def bf(x):
    return x.astype(jnp.bfloat16)


def mm(x, y):
    return lax.dot_general(x, y, (((1,), (0,)), ((), ())), preferred_element_type=jnp.float32)


def mm_nt(x, y):
    return lax.dot_general(x, y, (((1,), (1,)), ((), ())), preferred_element_type=jnp.float32)


def mm_tn(x, y):
    return lax.dot_general(x, y, (((0,), (0,)), ((), ())), preferred_element_type=jnp.float32)


def halves(x):
    high = bf(x)
    return high, bf(x - high.astype(jnp.float32))


def sum_right(x, ones):
    high, low = halves(x)
    return mm(high, ones) + mm(low, ones)


def logistic(x):
    return 1.0 / (1.0 + jnp.exp(-x))


def flag(cond):
    return jnp.where(cond, 1.0, 0.0)


def iota(shape, dim):
    return lax.broadcasted_iota(jnp.int32, shape, dim)


def pair_blocks():
    return flag((iota((PAIR, PAIR), 0) < HEAD_DIM) == (iota((PAIR, PAIR), 1) < HEAD_DIM))


def scan_kernel(
    group,
    pump,
    r_ref,
    k_ref,
    v_ref,
    d_ref,
    a_ref,
    d_off_ref,
    a_off_ref,
    extra_ref,
    out_ref,
    reach_ref,
    ends_ref,
    chain_ref,
):
    positions, width = r_ref.shape
    pairs = width // PAIR
    C = HEAD_DIM
    rows_per = group * C
    own_block = pair_blocks()
    own_bf = bf(own_block)
    row, col = iota((C, PAIR), 0), iota((C, PAIR), 1) & (HEAD_DIM - 1)
    strict, upto = row > col, row >= col
    eye = flag(row == col)
    tri = bf(flag(iota((C, C), 0) >= iota((C, C), 1)))
    level_masks = []
    for s in range(6):
        inside = (
            ((row >> (s + 1)) == (col >> (s + 1)))
            & (((row >> s) & 1) == 1)
            & (((col >> s) & 1) == 0)
        )
        level_masks.append(bf(flag(inside)))

    def spread(x):
        return jnp.concatenate([x, x], axis=0) * own_bf

    square = (iota((PAIR, PAIR), 0) == iota((PAIR, PAIR), 1)).astype(jnp.float32)
    for p in range(pairs):
        chain_ref[p, :PAIR] = jnp.zeros((PAIR, PAIR), jnp.float32)
        chain_ref[p, PAIR:] = square

    def step(g, carry):
        base = pl.multiple_of(g * rows_per, rows_per)
        rows = pl.ds(base, rows_per)
        items = []
        for p in range(pairs):
            lanes = slice(p * PAIR, (p + 1) * PAIR)
            k = k_ref[rows, lanes].astype(jnp.float32)
            u = k * lax.rsqrt(sum_right(k * k, own_bf) + key_eps)
            rem = u * logistic(a_ref[rows, lanes].astype(jnp.float32) + a_off_ref[:, lanes])
            lg = extra_ref[rows, lanes] - HALF_EXP * logistic(
                d_ref[rows, lanes].astype(jnp.float32) + d_off_ref[:, lanes]
            )
            r = r_ref[rows, lanes].astype(jnp.float32)
            v = v_ref[rows, lanes]
            for c in range(group):
                cut = slice(c * C, (c + 1) * C)
                items.append((p, c, k[cut], u[cut], rem[cut], lg[cut], r[cut], v[cut]))
        stage = []
        for p, c, k, u, rem, lg, r, v in items:
            high, low = halves(lg)
            rest = bf(lg - high.astype(jnp.float32) - low.astype(jnp.float32))
            cumul = mm(tri, high) + mm(tri, low) + mm(tri, rest)
            stage.append(cumul)
        work = []
        for (p, c, k, u, rem, lg, r, v), cumul in zip(items, stage):
            mid = 0.5 * cumul[C - 1 : C]
            up_now, down = jnp.exp(cumul - mid), jnp.exp(mid - cumul)
            up_before = jnp.exp(cumul - lg - mid)
            half = jnp.exp(mid)
            cq, cu, dk, dr = r * up_now, u * up_before, k * down, rem * down
            left = bf(jnp.concatenate([cu, cq], axis=0))
            pair_r = mm_nt(left, spread(bf(dr)))
            pair_k = mm_nt(left, spread(bf(dk)))
            work.append((cq * half, bf(cu * half), bf(dk * half), bf(dr * half), half * half, pair_r, pair_k))
        pump(g, 0)
        solve = []
        for (p, c, k, u, rem, lg, r, v), (qe, ue, kt, rt, ed, pair_r, pair_k) in zip(items, work):
            rp = bf(jnp.where(strict, pair_r[:C], 0.0))
            rr = bf(jnp.where(upto, pair_r[C:], 0.0))
            kp = jnp.where(strict, pair_k[:C], 0.0)
            rk = jnp.where(upto, pair_k[C:], 0.0)
            kv = mm(bf(jnp.concatenate([kp, rk], axis=0)), spread(v))
            inv = eye - (rp * level_masks[0]).astype(jnp.float32)
            solve.append([rp, rr, kv, inv])
        for s in range(1, 6):
            mids = [bf(mm(bf(inv), spread(rp * level_masks[s]))) for rp, rr, kv, inv in solve]
            for item, y in zip(solve, mids):
                item[3] = item[3] - mm(y, spread(bf(item[3])))
            if s == 2:
                pump(g, 1)
        wvs = []
        for (rp, rr, kv, inv), w in zip(solve, work):
            wide = jnp.concatenate([spread(w[1]), spread(bf(kv[:C]))], axis=1)
            wvs.append(bf(mm(bf(inv), wide)))
        pump(g, 2)
        tails = []
        for (rp, rr, kv, inv), (qe, ue, kt, rt, ed, _, _), wv, item in zip(solve, work, wvs, items):
            wide = jnp.concatenate([spread(wv[:, :PAIR]), spread(wv[:, PAIR:])], axis=1)
            rw = mm(rr, wide)
            read = bf(qe - rw[:, :PAIR])
            local = kv[C:] - rw[:, PAIR:]
            v = item[7]
            x = jnp.concatenate(
                [jnp.concatenate([v, jnp.zeros_like(v)], axis=1),
                 jnp.concatenate([-wv[:, PAIR:], -wv[:, :PAIR]], axis=1)], axis=0)
            nb = mm_tn(x, jnp.concatenate([kt, rt], axis=0))
            tails.append((read, local, nb[:PAIR] * own_block, bf(nb[PAIR:] * own_block), ed))
        z = [chain_ref[p] for p in range(pairs)]
        for c in range(group):
            for p in range(pairs):
                read, local, add, neg, ed = tails[p * group + c]
                zb = bf(z[p])
                qz = mm_nt(read, zb)
                at = pl.ds(pl.multiple_of(base + c * C, C), C)
                lanes = slice(p * PAIR, (p + 1) * PAIR)
                out_ref[at, lanes] = local + qz[:, :PAIR]
                reach_ref[at, lanes] = bf(qz[:, PAIR:])
                moved = z[p] * ed + mm(zb, neg)
                z[p] = jnp.concatenate([moved[:PAIR] + add, moved[PAIR:]], axis=0)
        for p in range(pairs):
            chain_ref[p] = z[p]
        pump(g, 3)
        return carry

    lax.fori_loop(0, positions // rows_per, step, 0)
    for p in range(pairs):
        s, m = chain_ref[p, :PAIR], chain_ref[p, PAIR:]
        ends_ref[p * 2 * C : p * 2 * C + C] = bf(s[:C] + s[C:])
        ends_ref[p * 2 * C + C : (p + 1) * 2 * C] = bf(m[:C] + m[C:])


def join_kernel(axis, all_ref, out_ref, reach_ref, gate_ref, gain_ref, mixed_ref):
    devices, place = lax.axis_size(axis), lax.axis_index(axis)
    width = out_ref.shape[1]
    pairs = width // PAIR
    C = HEAD_DIM
    own_block = pair_blocks()
    own_bf = bf(own_block)
    mean_bf = bf(own_block * (1.0 / HEAD_DIM))
    states = [jnp.zeros((C, PAIR), jnp.float32) for _ in range(pairs)]

    def hop(j, states):
        new = []
        for p in range(pairs):
            s = all_ref[j, p * 2 * C : p * 2 * C + C].astype(jnp.float32)
            m = all_ref[j, p * 2 * C + C : (p + 1) * 2 * C]
            m = jnp.concatenate([m, m], axis=0) * own_bf
            new.append(sum_right(states[p], m) + s)
        return tuple(new)

    states = lax.fori_loop(0, place, hop, tuple(states))
    for p in range(pairs):
        lanes = slice(p * PAIR, (p + 1) * PAIR)
        s = bf(states[p])
        s = jnp.concatenate([s, s], axis=0) * own_bf
        head = out_ref[:, lanes] + mm_nt(reach_ref[:, lanes], s)
        centred = head - sum_right(head, mean_bf)
        spread = sum_right(centred * centred, mean_bf)
        normed = centred * lax.rsqrt(spread + group_eps)
        gate = logistic(gate_ref[:, lanes].astype(jnp.float32))
        mixed_ref[:, lanes] = bf(normed * gain_ref[:, lanes] * gate)


def place_of():
    n_ep, n_tp = lax.axis_size("ep"), lax.axis_size("tp")
    e, t = lax.axis_index("ep"), lax.axis_index("tp")
    core = lax.rem(t, 2)
    return n_ep, n_tp, n_tp // 2, e, t, lax.div(t, 2), core


def remote(src, dst, send, recv, e, t):
    return pltpu.make_async_remote_copy(
        src_ref=src,
        dst_ref=dst,
        send_sem=send,
        recv_sem=recv,
        device_id=(e, t),
        device_id_type=pl.DeviceIdType.MESH,
    )


def meet():
    n_ep, n_tp, n_y, e, t, y, core = place_of()
    barrier = pltpu.get_barrier_semaphore()

    def greet(pe, pt):
        pl.semaphore_signal(
            barrier, inc=1, device_id=(pe, pt), device_id_type=pl.DeviceIdType.MESH
        )

    for d in range(1, n_ep):
        greet(lax.rem(e + d, n_ep), t)
    greet(e, 2 * y + 1 - core)
    for d in range(1, n_y):
        greet(e, 2 * lax.rem(y + d, n_y) + core)
        greet(e, 2 * lax.rem(y + d, n_y) + 1 - core)
    return lambda: pl.semaphore_wait(barrier, n_ep - 2 + 2 * n_y)


def span(first, last, body):
    def run(d, carry):
        body(d)
        return carry

    lax.fori_loop(first, last, run, 0)


def wide(x):
    return x.astype(jnp.float32)


def whole_kernel(
    group,
    r_hbm,
    k_hbm,
    v_hbm,
    d_hbm,
    a_hbm,
    gate_in_hbm,
    d_off_hbm,
    a_off_hbm,
    extra_hbm,
    gain_hbm,
    out_weight_hbm,
    x_hbm,
    norm_gain_hbm,
    group_router_hbm,
    expert_router_hbm,
    routes_hbm,
    gate_hbm,
    up_hbm,
    down_hbm,
    mixer_ref,
    expert_ref,
    r_ref,
    k_ref,
    v_ref,
    d_ref,
    a_ref,
    gate_in_ref,
    w_ref,
    x_ref,
    d_off_ref,
    a_off_ref,
    extra_in_ref,
    gain_ref,
    norm_gain_ref,
    group_router_ref,
    expert_router_ref,
    routes_ref,
    extra_parts_ref,
    extra_ref,
    normed_ref,
    place_ref,
    near_out_ref,
    far_out_ref,
    picks_ref,
    weight_ref,
    piece_ref,
    out_ref,
    reach_ref,
    every_ref,
    chain_ref,
    mixed_ref,
    mixed_all_ref,
    gate_ref,
    up_ref,
    down_ref,
    hidden_ref,
    gate_part_ref,
    up_part_ref,
    part_ref,
    near_ref,
    stage_ref,
    far_ref,
    final_ref,
    home_ref,
    in_sem,
    gate_sem,
    up_sem,
    down_sem,
    es,
    er,
    cs,
    cr,
    ys,
    yr,
    fs,
    fr,
    zs,
    zr,
    gs,
    gr,
    ns,
    nr,
    bs,
    br,
    hs,
    hr,
    wys,
    wyr,
    wgs,
    wgr,
    wcs,
    wcr,
    xs,
    xr,
):
    n_ep, n_tp, n_y, e, t, y, core = place_of()
    units = gate_ref.shape[1]
    model = x_ref.shape[1]
    tokens = x_ref.shape[0]
    share = model // n_tp
    slots = piece_ref.shape[0]
    capacity = slots // n_ep
    experts = expert_router_ref.shape[0]
    groups = group_router_ref.shape[0]
    positions, width = mixed_ref.shape
    rows = positions // n_tp
    other = 2 * y + 1 - core
    half = n_ep // 2
    half_rows = half * capacity
    wide_units, wide_model = min(256, units), min(512, model)

    def shard(index):
        return pl.ds(pl.multiple_of(index * width, width), width)

    inputs = [(routes_hbm, routes_ref), (norm_gain_hbm, norm_gain_ref), (x_hbm, x_ref)]
    inputs += [(extra_hbm, extra_in_ref), (d_off_hbm, d_off_ref), (a_off_hbm, a_off_ref)]
    inputs += [(k_hbm, k_ref), (a_hbm, a_ref), (d_hbm, d_ref), (r_hbm, r_ref), (v_hbm, v_ref)]
    inputs += [(gate_in_hbm, gate_in_ref), (out_weight_hbm, w_ref.at[shard(t), :]), (gain_hbm, gain_ref)]
    inputs += [(group_router_hbm, group_router_ref), (expert_router_hbm, expert_router_ref)]
    loads = [pltpu.make_async_copy(s, d, in_sem.at[i]) for i, (s, d) in enumerate(inputs)]

    def gate_copy(i):
        at = pl.ds(pl.multiple_of(i * wide_units, wide_units), wide_units)
        return (
            pltpu.make_async_copy(gate_hbm.at[0, :, at], gate_ref.at[:, at], gate_sem.at[0]),
            pltpu.make_async_copy(up_hbm.at[0, :, at], up_ref.at[:, at], up_sem.at[0]),
        )

    def down_copy(i):
        at = pl.ds(pl.multiple_of(i * wide_model, wide_model), wide_model)
        return pltpu.make_async_copy(down_hbm.at[0, :, at], down_ref.at[:, at], down_sem.at[0])

    def partner(d):
        bit, total = 1, 0
        while bit < n_ep:
            total = total + lax.rem(lax.div(e, bit) + lax.div(d, bit), 2) * bit
            bit = 2 * bit
        return total

    def columns(index):
        return pl.ds(pl.multiple_of(index * share, share), share)

    def block(d):
        return pl.ds(pl.multiple_of(d * capacity, capacity), capacity)

    def peer_y(h):
        return lax.rem(y + h, n_y)

    plane = pl.ds(pl.multiple_of(core * (model // 2), model // 2), model // 2)

    def near_ep(d):
        dst = piece_ref.at[block(d), plane]
        return remote(near_out_ref.at[block(d), :], dst, es.at[0], er.at[d], partner(d), t)

    def far_ep(d):
        src = far_out_ref.at[block(d - half), :]
        return remote(src, piece_ref.at[block(d), columns(t)], es.at[1], er.at[d], partner(d), t)

    near_rows, far_rows = slice(capacity, half_rows), slice(half_rows, slots)

    def near_core(at):
        ref = piece_ref.at[at, plane]
        return remote(ref, ref, cs.at[0], cr.at[0], e, other)

    def far_core(at):
        ref = piece_ref.at[at, columns(t)]
        return remote(ref, ref, cs.at[1], cr.at[1], e, other)

    def y_copy(d, h):
        ref = piece_ref.at[block(d), columns(t)]
        peer = 2 * peer_y(h) + core
        return remote(ref, ref, ys.at[h - 1], yr.at[h - 1, d - half], e, peer)

    def forward_copy(at, h):
        ref = piece_ref.at[at, columns(2 * lax.rem(y - h + n_y, n_y) + core)]
        return remote(ref, ref, fs.at[h - 1], fr.at[h - 1], e, other)

    def near_arrived(d):
        near_ep(d).wait_recv()
        near_core(block(d)).start()

    def far_arrived(d):
        far_ep(d).wait_recv()
        for h in range(1, n_y):
            y_copy(d, h).start()
        far_core(block(d)).start()

    def pass_on(d):
        for h in range(1, n_y):
            y_copy(d, h).wait_recv()
            forward_copy(block(d), h).start()

    def gathered():
        for h in range(1, n_y):
            forward_copy(far_rows, h).wait_recv()

    n_x = gs.shape[0] + 1
    n_z = n_ep // n_x
    z, x = lax.div(e, n_x), lax.rem(e, n_x)

    def up_copy(zz):
        ref = every_ref.at[zz * n_x + x]
        return remote(ref, ref, zs.at[zz], zr.at[zz], e + n_x, t)

    def side_copy(zz, h):
        ref = every_ref.at[zz * n_x + x]
        peer = z * n_x + lax.rem(x + h, n_x)
        return remote(ref, ref, gs.at[h - 1, zz], gr.at[h - 1, zz], peer, t)

    def pass_ends(zz):
        @pl.when(z + 1 < n_z)
        def _():
            up_copy(zz).start()

        for h in range(1, n_x):
            side_copy(zz, h).start()

    def relay_ends(i, wanted=True):
        @pl.when((z >= i) & wanted)
        def _():
            up_copy(z - i).wait_recv()
            pass_ends(z - i)

    def collect_ends(zz):
        @pl.when(z >= zz)
        def _():
            for h in range(1, n_x):
                side_copy(zz, h).wait_recv()

    def close_ends(zz):
        @pl.when(z >= zz)
        def _():
            @pl.when(z + 1 < n_z)
            def _():
                up_copy(zz).wait_send()

            for h in range(1, n_x):
                side_copy(zz, h).wait_send()

    def near_copy(b, h):
        at = pl.ds(b * half_rows, half_rows)
        src = part_ref.at[at, columns(2 * peer_y(h) + 1 - core)]
        return remote(src, near_ref.at[h, at, :], ns.at[0], nr.at[b, h], e, other)

    def back_copy(d, h):
        src = stage_ref.at[h, block(d), :]
        dst = far_ref.at[h, block(d), :]
        return remote(src, dst, bs.at[h - 1], br.at[h - 1, d], e, 2 * peer_y(h) + core)

    def home_copy(d):
        src, dst = final_ref.at[block(d), :], home_ref.at[block(e), :]
        return remote(src, dst, hs.at[0], hr.at[0], partner(d), t)

    def all_home():
        src, dst = final_ref.at[capacity:, :], home_ref.at[capacity:, :]
        return remote(src, dst, hs.at[0], hr.at[0], partner(1), t)

    def pair_sum(d, h):
        return wide(part_ref[block(d), columns(2 * peer_y(h) + core)]) + wide(near_ref[h, block(d), :])

    def add_near(b):
        for h in range(1, n_y):
            near_copy(b, h).wait_recv()

        def one(d):
            for h in range(1, n_y):
                stage_ref[h, block(d), :] = bf(pair_sum(d, h))
                back_copy(d, h).start()

        span(b * half, (b + 1) * half, one)

    def add_far(d):
        total = pair_sum(d, 0)
        for h in range(1, n_y):
            back_copy(d, h).wait_recv()
            total = total + wide(far_ref[h, block(d), :])
        return bf(total)

    def go_home(d):
        final_ref[block(d), :] = add_far(d)
        home_copy(d).start()

    tile_count = model // wide_model
    part_rows = width // half
    part_at = lax.rem(e, half)

    def source_of(h):
        return 2 * lax.rem(y - h + n_y, n_y) + core

    def shard_part(index):
        return pl.ds(pl.multiple_of(index * width + part_at * part_rows, part_rows), part_rows)

    def w_plane(h):
        ref = w_ref.at[shard_part(t), :]
        return remote(ref, ref, wys.at[h - 1], wyr.at[h - 1], e, 2 * peer_y(h) + core)

    def w_group(h, k):
        ref = w_ref.at[shard_part(source_of(h)), :]
        return remote(ref, ref, wgs.at[0], wgr.at[0], partner(k), t)

    def w_grouped():
        ref = w_ref.at[: (n_y - 1) * (half - 1) * part_rows, :]
        return remote(ref, ref, wgs.at[0], wgr.at[0], partner(1), t)

    def w_core(h):
        ref = w_ref.at[shard(source_of(h)), :]
        return remote(ref, ref, wcs.at[h], wcr.at[h], e, other)

    def share_w():
        for h in range(1, n_y):
            w_plane(h).wait_recv()
            span(1, half, lambda k: w_group(h, k).start())

    def mixed_copy(j):
        to = lax.rem(t + j, n_tp)
        src = mixed_ref.at[pl.ds(pl.multiple_of(to * rows, rows), rows), :]
        return remote(src, mixed_all_ref.at[t], xs.at[0], xr.at[0], e, to)

    def all_mixed():
        ref = mixed_all_ref.at[1:]
        return remote(ref, ref, xs.at[0], xr.at[0], e, other)

    def tiles(count, body, hooks):
        for i in range(count):
            body(i)
            for hook in hooks.get(i, ()):
                hook()
        for i in sorted(hooks):
            for hook in hooks[i] if i >= count else ():
                hook()

    def units_at(i):
        return slice(i * wide_units, (i + 1) * wide_units)

    def activate(i, gate_val, up_val):
        hidden_ref[:, units_at(i)] = bf(gate_val * logistic(gate_val) * up_val)

    def widen_near(hooks):
        pltpu.make_async_copy(gate_hbm.at[0], gate_ref, gate_sem.at[0]).wait()
        pltpu.make_async_copy(up_hbm.at[0], up_ref, up_sem.at[0]).wait()

        def unit_tile(i):
            rows_in = piece_ref[:half_rows, :]
            activate(i, mm(rows_in, gate_ref[:, units_at(i)]), mm(rows_in, up_ref[:, units_at(i)]))

        tiles(units // wide_units, unit_tile, hooks)

    def widen_part(i, h):
        model_at = pl.ds(pl.multiple_of(peer_y(h) * 2 * share, 2 * share), 2 * share)
        rows_in = piece_ref[far_rows, model_at]
        return mm(rows_in, gate_ref[model_at, units_at(i)]), mm(rows_in, up_ref[model_at, units_at(i)])

    def widen_far_begin():
        for i in range(units // wide_units):
            gate_part_ref[:, units_at(i)], up_part_ref[:, units_at(i)] = widen_part(i, 0)

    def widen_far_end(hooks):
        def unit_tile(i):
            gate_val, up_val = gate_part_ref[:, units_at(i)], up_part_ref[:, units_at(i)]
            for h in range(1, n_y):
                more = widen_part(i, h)
                gate_val, up_val = gate_val + more[0], up_val + more[1]
            activate(i, gate_val, up_val)

        tiles(units // wide_units, unit_tile, hooks)

    def narrow(b, hooks):
        at = slice(b * half_rows, (b + 1) * half_rows)
        if b == 0:
            pltpu.make_async_copy(down_hbm.at[0], down_ref, down_sem.at[0]).wait()

        def tile(i):
            h = n_y - 1 - i % n_y
            index = 2 * peer_y(h) + (1 - core if i < n_y else core)
            part_ref[at, columns(index)] = bf(mm(hidden_ref[...], down_ref[:, columns(index)]))
            if i < n_y:
                near_copy(b, h).start()

        tiles(n_tp, tile, hooks)

    for copy in loads:
        copy.start()
    for i in range(units // wide_units):
        for copy in gate_copy(i):
            copy.start()
    for i in range(model // wide_model):
        down_copy(i).start()
    everyone_here = meet()

    order = flag(iota((tokens, tokens), 0) < iota((tokens, tokens), 1))
    expert_rows = max(16, experts)
    loads[0].wait()
    loads[1].wait()
    own_routes = routes_ref[...]
    names = iota((expert_rows, tokens), 0)
    named = [own_routes[k : k + 1, :] == names for k in range(own_routes.shape[0])]
    match = functools.reduce(jnp.logical_or, named)
    rank = mm(bf(flag(match)), bf(order))
    rank = jnp.where(match, rank, -1.0)
    level = iota((capacity, tokens), 0).astype(jnp.float32)
    for j in range(experts):
        place_ref[j * capacity : (j + 1) * capacity] = bf(flag(level == rank[j : j + 1, :]))
    loads[2].wait()
    step_rows = 32
    for i in range(tokens // step_rows):
        at = slice(i * step_rows, (i + 1) * step_rows)
        xw = wide(x_ref[at])
        scale = lax.rsqrt(jnp.mean(xw * xw, axis=-1, keepdims=True) + norm_eps)
        normed_ref[at] = bf(xw * scale * norm_gain_ref[...])
    here = jnp.concatenate([place_ref[block(partner(d)), :] for d in range(1, half)], axis=0)
    near_out_ref[capacity:half_rows] = bf(mm(here, normed_ref[:, plane]))
    there = jnp.concatenate([place_ref[block(partner(d)), :] for d in range(half, n_ep)], axis=0)
    far_out_ref[...] = bf(mm(there, normed_ref[:, columns(t)]))
    per = max(1, n_ep // 8)

    def unit(u, body):
        lo = max(1, min(n_ep, u * per))
        return lambda: span(lo, max(lo, min(n_ep, (u + 1) * per)), body)

    inner = lax.rem(lax.div(z + 1, 2), 2)

    def far_unit(k, body):
        first = [4 + 2 * inner, 5 + 2 * inner, 6 - 2 * inner, 7 - 2 * inner][k] * per
        return lambda: span(first, first + per, body)

    everyone_here()
    span(1, half, lambda d: near_ep(d).start())
    for k in range(4):
        far_unit(k, lambda d: far_ep(d).start())()
    for i in range(model // wide_model):
        at = slice(i * wide_model, (i + 1) * wide_model)
        piece_ref[:capacity, at] = bf(mm(place_ref[block(e), :], normed_ref[:, at]))

    loads[12].wait()
    for h in range(1, n_y):
        w_plane(h).start()
    w_core(0).start()
    for copy in loads[3:11]:
        copy.wait()
    heads, pairs = extra_in_ref.shape[0], chain_ref.shape[0]
    exact = extra_in_ref[...]
    extra_parts_ref[...] = jnp.zeros(extra_parts_ref.shape, jnp.float32)
    for i in range(3):
        piece = wide(bf(exact))
        extra_parts_ref[i * heads : (i + 1) * heads, :] = piece
        exact = exact - piece
    extra_parts = bf(extra_parts_ref[...])
    extra_rows = extra_parts_ref.shape[0]
    for p in range(pairs):
        head = lax.rem(iota((extra_rows, PAIR), 0), heads)
        wanted = head == 2 * p + lax.div(iota((extra_rows, PAIR), 1), HEAD_DIM)
        extra_ref[:, p * PAIR : (p + 1) * PAIR] = mm_tn(extra_parts, bf(flag(wanted)))
    steps = positions // (group * HEAD_DIM)
    events = {}

    def pump(g, point):
        for step in range(steps):
            due = events.get(4 * step + point)
            if due:

                @pl.when(g == step)
                def _(due=due):
                    for act in due:
                        act()

    scan_kernel(
        group,
        pump,
        r_ref,
        k_ref,
        v_ref,
        d_ref,
        a_ref,
        d_off_ref,
        a_off_ref,
        extra_ref,
        out_ref,
        reach_ref,
        every_ref.at[e],
        chain_ref,
    )
    for i in sorted(events):
        for act in events[i] if i >= 4 * steps else ():
            act()
    pass_ends(z)
    span(1, half, near_arrived)
    far_unit(0, far_arrived)()
    far_unit(1, far_arrived)()
    share_w()
    near_core(near_rows).wait_recv()
    relays = [lambda i=i: relay_ends(i) for i in range(1, n_z)]
    widen_near({2: [far_unit(2, far_arrived)], 3: [far_unit(0, pass_on)]})
    narrow(0, {0: [far_unit(1, pass_on)], 1: [far_unit(3, far_arrived)], 3: [far_unit(2, pass_on)]})
    add_near(0)
    for copy in loads[11:12] + loads[13:]:
        copy.wait()

    normed = normed_ref[...]
    group_logit = mm_nt(group_router_ref[...], normed)
    group_exp = jnp.exp(group_logit)
    group_prob = group_exp / jnp.sum(group_exp, axis=0, keepdims=True)
    expert_logit = mm_nt(expert_router_ref[...], normed)
    per_group = experts // groups
    first_of = iota((groups, tokens), 0) * per_group
    expert_names = iota((experts, tokens), 0)
    chosen, prob = [], []
    for k in range(2):
        route = own_routes[k : k + 1, :]
        chosen.append(
            jnp.sum(jnp.where(route == expert_names, expert_logit, 0.0), axis=0, keepdims=True)
        )
        inside = (route >= first_of) & (route < first_of + per_group)
        prob.append(jnp.sum(jnp.where(inside, group_prob, 0.0), axis=0, keepdims=True))
    weights = [prob[0] * logistic(chosen[0] - chosen[1]), prob[1] * logistic(chosen[1] - chosen[0])]
    for k in range(2):
        weight_ref[k] = jnp.transpose(jnp.broadcast_to(weights[k], (128, tokens)))
        for j in range(experts):
            at = slice(j * capacity, (j + 1) * capacity)
            picks_ref[k, at] = place_ref[at] * bf(flag(own_routes[k : k + 1, :] == j))
    far_core(far_rows).wait_recv()
    widen_far_begin()
    for relay in relays[:1]:
        relay()
    with jax.named_scope("pass3"):
        far_unit(3, pass_on)()
    near_copy(0, 0).wait_recv()
    gathered()
    last = z == n_z - 1
    widen_far_end({1: [lambda i=i: relay_ends(i, ~last) for i in range(2, 3)]})
    narrow(1, {})
    add_near(1)
    span(1, half, go_home)
    near_copy(1, 0).wait_recv()
    unit(4, go_home)()
    for i in range(2, n_z):
        relay_ends(i, last if i < 3 else True)
    for u in range(5, 8):
        unit(u, go_home)()
    home_ref[block(e), :] = add_far(0)
    span(0, n_z, collect_ends)
    join_kernel("ep", every_ref, out_ref, reach_ref, gate_in_ref, gain_ref, mixed_ref)
    for j in range(1, n_tp):
        mixed_copy(j).start()
    mixed_all_ref[t] = mixed_ref[pl.ds(pl.multiple_of(t * rows, rows), rows), :]
    w_grouped().wait_recv()
    for h in range(1, n_y):
        w_core(h).start()
    all_mixed().wait_recv()
    for h in range(n_y):
        w_core(h).wait_recv()
    mixed = jnp.concatenate([mixed_all_ref[j] for j in range(n_tp)], axis=1)

    def project(i):
        at = pl.ds(pl.multiple_of(i * wide_model, wide_model), wide_model)
        mixer_ref[:, at] = bf(mm(mixed, w_ref[:, at]))

    for i in range(tile_count):
        project(i)

    near_src = near_out_ref.at[near_rows, :]
    remote(near_src, near_src, es.at[0], er.at[0], e, other).wait_send()
    remote(far_out_ref, far_out_ref, es.at[1], er.at[0], e, other).wait_send()
    near_core(near_rows).wait_send()
    far_core(far_rows).wait_send()
    remote(near_ref, near_ref, ns.at[0], nr.at[0, 0], e, other).wait_send()
    for h in range(1, n_y):
        ref = piece_ref.at[far_rows, columns(t)]
        remote(ref, ref, ys.at[h - 1], yr.at[h - 1, 0], e, other).wait_send()
        forward_copy(far_rows, h).wait_send()
        ref = stage_ref.at[h]
        remote(ref, ref, bs.at[h - 1], br.at[h - 1, 0], e, other).wait_send()
        w_plane(h).wait_send()
    for h in range(n_y):
        w_core(h).wait_send()
    w_grouped().wait_send()
    all_mixed().wait_send()
    span(0, n_z, close_ends)
    all_home().wait_recv()
    back = home_ref[...]
    first, second = mm_tn(picks_ref[0], back), mm_tn(picks_ref[1], back)
    for i in range(share // 128):
        at = slice(i * 128, (i + 1) * 128)
        expert_ref[:, at] = bf(weight_ref[0] * first[:, at] + weight_ref[1] * second[:, at])
    all_home().wait_send()


def local(
    receptance,
    key_matrix,
    value_matrix,
    decay_data_term,
    correction_rate_data,
    output_gate_input,
    decay_channel_offset,
    correction_rate_offset,
    extra_head_log_decay,
    head_norm_gain,
    mixer_output_weight,
    expert_layer_input,
    feedforward_norm_gain,
    group_router_weight,
    expert_router_weight,
    routes,
    expert_gate_weight,
    expert_up_weight,
    expert_down_weight,
):
    positions, own_width = receptance.shape
    pairs = -(-own_width // PAIR)
    width = pairs * PAIR

    def filled(x, columns=width):
        return x if x.shape[-1] == columns else jnp.pad(x, ((0, 0), (0, columns - x.shape[-1])))

    blocks = positions // HEAD_DIM
    group = 4 if blocks % 4 == 0 else 1
    n_ep, n_tp = lax.axis_size("ep"), lax.axis_size("tp")
    n_y = n_tp // 2
    n_x = 1
    while 4 * n_x * n_x <= n_ep:
        n_x = 2 * n_x
    tokens, model = expert_layer_input.shape
    capacity, share = 4 * tokens // n_ep, model // n_tp
    slots = n_ep * capacity
    units = expert_gate_weight.shape[2]
    rows = positions // n_tp
    out_weight = jnp.pad(mixer_output_weight, ((0, width - own_width), (0, 0)))

    def held(*shape):
        return pltpu.VMEM(shape, jnp.bfloat16)

    def single(*shape):
        return pltpu.VMEM(shape, jnp.float32)

    def sems(*shape):
        return pltpu.SemaphoreType.DMA(shape)

    operands = (
        filled(receptance),
        filled(key_matrix),
        filled(value_matrix),
        filled(decay_data_term),
        filled(correction_rate_data),
        filled(output_gate_input),
        filled(decay_channel_offset[None]),
        filled(correction_rate_offset[None]),
        filled(extra_head_log_decay, 2 * pairs).T,
        filled(head_norm_gain[None]),
        out_weight,
        expert_layer_input,
        feedforward_norm_gain[None],
        group_router_weight.T,
        expert_router_weight.T,
        routes.T,
        expert_gate_weight,
        expert_up_weight,
        expert_down_weight,
    )
    in_vmem, in_hbm = pl.BlockSpec(memory_space=pltpu.VMEM), pl.BlockSpec(memory_space=pltpu.HBM)
    one, hops = sems(n_ep), sems(n_y - 1)
    mixer_out, expert_out = pl.pallas_call(
        functools.partial(whole_kernel, group),
        out_shape=(held(rows, model), held(tokens, share)),
        in_specs=[in_hbm] * 19,
        out_specs=[in_vmem] * 2,
        scratch_shapes=[held(positions, width)] * 6
        + [
            held(n_tp * width, model),
            held(tokens, model),
            single(1, width),
            single(1, width),
            single(2 * pairs, positions),
            single(1, width),
            single(1, model),
            held(*group_router_weight.shape[::-1]),
            held(*expert_router_weight.shape[::-1]),
            pltpu.VMEM(routes.shape[::-1], jnp.int32),
            single(16, positions),
            single(positions, width),
            held(tokens, model),
            held(slots, tokens),
            held(slots // 2, model // 2),
            held(slots // 2, share),
            held(2, slots, tokens),
            single(2, tokens, 128),
            held(slots, model),
            single(positions, width),
            held(positions, width),
            held(n_ep, pairs * 2 * HEAD_DIM, PAIR),
            single(pairs, 2 * PAIR, PAIR),
            held(positions, width),
            held(n_tp, rows, width),
            held(model, units),
            held(model, units),
            held(units, model),
            held(slots // 2, units),
            single(slots // 2, units),
            single(slots // 2, units),
            held(slots, model),
        ]
        + [held(n_y, slots, share)] * 3
        + [held(slots, share)] * 2
        + [sems(16)]
        + [sems(1)] * 3
        + [sems(2), one, sems(2), sems(2)]
        + [hops, sems(n_y - 1, n_ep // 2), hops, hops]
        + [sems(n_ep // n_x)] * 2
        + [sems(n_x - 1, n_ep // n_x)] * 2
        + [sems(1), sems(2, n_y)]
        + [hops, sems(n_y - 1, n_ep)]
        + [sems(1)] * 2
        + [hops, hops, sems(1), sems(1), sems(n_y), sems(n_y), sems(1), sems(1)],
        compiler_params=pltpu.CompilerParams(
            collective_id=0, has_side_effects=True, vmem_limit_bytes=VMEM_LIMIT
        ),
    )(
        *(pltpu.with_memory_space_constraint(x, pltpu.HBM) for x in operands)
    )
    return mixer_out, expert_out


def solution(mesh):
    in_specs = (
        P("ep", "tp"),
        P("ep", "tp"),
        P("ep", "tp"),
        P("ep", "tp"),
        P("ep", "tp"),
        P("ep", "tp"),
        P("tp"),
        P("tp"),
        P("ep", "tp"),
        P("tp"),
        P("tp", None),
        P("ep", None),
        P(),
        P(),
        P(),
        P("ep", None),
        P("ep", None, "tp"),
        P("ep", None, "tp"),
        P("ep", "tp", None),
    )
    out_specs = (P(("ep", "tp"), None), P("ep", "tp"))
    return jax.shard_map(local, mesh=mesh, in_specs=in_specs, out_specs=out_specs, check_vma=False)
```

```python
import functools
import math

import jax
import jax.numpy as jnp
from jax import lax
from jax.experimental import pallas as pl
from jax.experimental.pallas import tpu as pltpu
from jax.sharding import PartitionSpec as P

HEAD_DIM = 64
PAIR = 2 * HEAD_DIM
VMEM_LIMIT = 48 << 20
HALF_EXP = math.exp(-0.5)
GROUPS = 4


key_eps = 1e-06
group_eps = 0.00064
norm_eps = 1e-06
highest = lax.Precision.HIGHEST


def bf(x):
    return x.astype(jnp.bfloat16)


def mm(x, y):
    return lax.dot_general(x, y, (((1,), (0,)), ((), ())), preferred_element_type=jnp.float32)


def mm_nt(x, y):
    return lax.dot_general(x, y, (((1,), (1,)), ((), ())), preferred_element_type=jnp.float32)


def mm_tn(x, y):
    return lax.dot_general(x, y, (((0,), (0,)), ((), ())), preferred_element_type=jnp.float32)


def halves(x):
    high = bf(x)
    return high, bf(x - high.astype(jnp.float32))


def sum_right(x, ones):
    high, low = halves(x)
    return mm(high, ones) + mm(low, ones)


def logistic(x):
    return 1.0 / (1.0 + jnp.exp(-x))


def flag(cond):
    return jnp.where(cond, 1.0, 0.0)


def iota(shape, dim):
    return lax.broadcasted_iota(jnp.int32, shape, dim)


def pair_blocks():
    return flag((iota((PAIR, PAIR), 0) < HEAD_DIM) == (iota((PAIR, PAIR), 1) < HEAD_DIM))


def scan_kernel(
    group,
    pump,
    r_ref,
    k_ref,
    v_ref,
    d_ref,
    a_ref,
    d_off_ref,
    a_off_ref,
    extra_ref,
    out_ref,
    reach_ref,
    ends_ref,
    chain_ref,
):
    positions, width = r_ref.shape
    pairs = width // PAIR
    C = HEAD_DIM
    rows_per = group * C
    own_block = pair_blocks()
    own_bf = bf(own_block)
    row, col = iota((C, PAIR), 0), iota((C, PAIR), 1) & (HEAD_DIM - 1)
    strict, upto = row > col, row >= col
    eye = flag(row == col)
    tri = bf(flag(iota((C, C), 0) >= iota((C, C), 1)))
    level_masks = []
    for s in range(6):
        inside = (
            ((row >> (s + 1)) == (col >> (s + 1)))
            & (((row >> s) & 1) == 1)
            & (((col >> s) & 1) == 0)
        )
        level_masks.append(bf(flag(inside)))

    def spread(x):
        return jnp.concatenate([x, x], axis=0) * own_bf

    square = (iota((PAIR, PAIR), 0) == iota((PAIR, PAIR), 1)).astype(jnp.float32)
    for p in range(pairs):
        chain_ref[p, :PAIR] = jnp.zeros((PAIR, PAIR), jnp.float32)
        chain_ref[p, PAIR:] = square

    def step(g, carry):
        base = pl.multiple_of(g * rows_per, rows_per)
        rows = pl.ds(base, rows_per)
        items = []
        for p in range(pairs):
            lanes = slice(p * PAIR, (p + 1) * PAIR)
            k = k_ref[rows, lanes].astype(jnp.float32)
            u = k * lax.rsqrt(sum_right(k * k, own_bf) + key_eps)
            rem = u * logistic(a_ref[rows, lanes].astype(jnp.float32) + a_off_ref[:, lanes])
            lg = extra_ref[rows, lanes] - HALF_EXP * logistic(
                d_ref[rows, lanes].astype(jnp.float32) + d_off_ref[:, lanes]
            )
            r = r_ref[rows, lanes].astype(jnp.float32)
            v = v_ref[rows, lanes]
            for c in range(group):
                cut = slice(c * C, (c + 1) * C)
                items.append((p, c, k[cut], u[cut], rem[cut], lg[cut], r[cut], v[cut]))
        stage = []
        for p, c, k, u, rem, lg, r, v in items:
            high, low = halves(lg)
            rest = bf(lg - high.astype(jnp.float32) - low.astype(jnp.float32))
            cumul = mm(tri, high) + mm(tri, low) + mm(tri, rest)
            stage.append(cumul)
        work = []
        for (p, c, k, u, rem, lg, r, v), cumul in zip(items, stage):
            mid = 0.5 * cumul[C - 1 : C]
            up_now, down = jnp.exp(cumul - mid), jnp.exp(mid - cumul)
            up_before = jnp.exp(cumul - lg - mid)
            half = jnp.exp(mid)
            cq, cu, dk, dr = r * up_now, u * up_before, k * down, rem * down
            left = bf(jnp.concatenate([cu, cq], axis=0))
            pair_r = mm_nt(left, spread(bf(dr)))
            pair_k = mm_nt(left, spread(bf(dk)))
            work.append((cq * half, bf(cu * half), bf(dk * half), bf(dr * half), half * half, pair_r, pair_k))
        pump(g, 0)
        solve = []
        for (p, c, k, u, rem, lg, r, v), (qe, ue, kt, rt, ed, pair_r, pair_k) in zip(items, work):
            rp = bf(jnp.where(strict, pair_r[:C], 0.0))
            rr = bf(jnp.where(upto, pair_r[C:], 0.0))
            kp = jnp.where(strict, pair_k[:C], 0.0)
            rk = jnp.where(upto, pair_k[C:], 0.0)
            kv = mm(bf(jnp.concatenate([kp, rk], axis=0)), spread(v))
            inv = eye - (rp * level_masks[0]).astype(jnp.float32)
            solve.append([rp, rr, kv, inv])
        for s in range(1, 6):
            mids = [bf(mm(bf(inv), spread(rp * level_masks[s]))) for rp, rr, kv, inv in solve]
            for item, y in zip(solve, mids):
                item[3] = item[3] - mm(y, spread(bf(item[3])))
            if s == 2:
                pump(g, 1)
        wvs = []
        for (rp, rr, kv, inv), w in zip(solve, work):
            wide = jnp.concatenate([spread(w[1]), spread(bf(kv[:C]))], axis=1)
            wvs.append(bf(mm(bf(inv), wide)))
        pump(g, 2)
        tails = []
        for (rp, rr, kv, inv), (qe, ue, kt, rt, ed, _, _), wv, item in zip(solve, work, wvs, items):
            wide = jnp.concatenate([spread(wv[:, :PAIR]), spread(wv[:, PAIR:])], axis=1)
            rw = mm(rr, wide)
            read = bf(qe - rw[:, :PAIR])
            local = kv[C:] - rw[:, PAIR:]
            v = item[7]
            x = jnp.concatenate(
                [jnp.concatenate([v, jnp.zeros_like(v)], axis=1),
                 jnp.concatenate([-wv[:, PAIR:], -wv[:, :PAIR]], axis=1)], axis=0)
            nb = mm_tn(x, jnp.concatenate([kt, rt], axis=0))
            tails.append((read, local, nb[:PAIR] * own_block, bf(nb[PAIR:] * own_block), ed))
        z = [chain_ref[p] for p in range(pairs)]
        for c in range(group):
            for p in range(pairs):
                read, local, add, neg, ed = tails[p * group + c]
                zb = bf(z[p])
                qz = mm_nt(read, zb)
                at = pl.ds(pl.multiple_of(base + c * C, C), C)
                lanes = slice(p * PAIR, (p + 1) * PAIR)
                out_ref[at, lanes] = local + qz[:, :PAIR]
                reach_ref[at, lanes] = bf(qz[:, PAIR:])
                moved = z[p] * ed + mm(zb, neg)
                z[p] = jnp.concatenate([moved[:PAIR] + add, moved[PAIR:]], axis=0)
        for p in range(pairs):
            chain_ref[p] = z[p]
        pump(g, 3)
        return carry

    lax.fori_loop(0, positions // rows_per, step, 0)
    for p in range(pairs):
        s, m = chain_ref[p, :PAIR], chain_ref[p, PAIR:]
        ends_ref[p * 2 * C : p * 2 * C + C] = bf(s[:C] + s[C:])
        ends_ref[p * 2 * C + C : (p + 1) * 2 * C] = bf(m[:C] + m[C:])


def join_kernel(axis, all_ref, out_ref, reach_ref, gate_ref, gain_ref, mixed_ref, owners, done):
    devices, place = lax.axis_size(axis), lax.axis_index(axis)
    width = out_ref.shape[1]
    pairs = width // PAIR
    C = HEAD_DIM
    own_block = pair_blocks()
    own_bf = bf(own_block)
    mean_bf = bf(own_block * (1.0 / HEAD_DIM))
    states = [jnp.zeros((C, PAIR), jnp.float32) for _ in range(pairs)]

    def hop(j, states):
        new = []
        for p in range(pairs):
            s = all_ref[j, p * 2 * C : p * 2 * C + C].astype(jnp.float32)
            m = all_ref[j, p * 2 * C + C : (p + 1) * 2 * C]
            m = jnp.concatenate([m, m], axis=0) * own_bf
            new.append(sum_right(states[p], m) + s)
        return tuple(new)

    states = lax.fori_loop(0, place, hop, tuple(states))
    rows = out_ref.shape[0] // len(owners)
    moves = []
    for p in range(pairs):
        s = bf(states[p])
        moves.append(jnp.concatenate([s, s], axis=0) * own_bf)
    for i, owner in enumerate(owners):
        at = pl.ds(pl.multiple_of(owner * rows, rows), rows)
        for p in range(pairs):
            lanes = slice(p * PAIR, (p + 1) * PAIR)
            head = out_ref[at, lanes] + mm_nt(reach_ref[at, lanes], moves[p])
            centred = head - sum_right(head, mean_bf)
            spread = sum_right(centred * centred, mean_bf)
            normed = centred * lax.rsqrt(spread + group_eps)
            gate = logistic(gate_ref[at, lanes].astype(jnp.float32))
            mixed_ref[at, lanes] = bf(normed * gain_ref[:, lanes] * gate)
        done(i)


def place_of():
    n_ep, n_tp = lax.axis_size("ep"), lax.axis_size("tp")
    e, t = lax.axis_index("ep"), lax.axis_index("tp")
    core = lax.rem(t, 2)
    return n_ep, n_tp, n_tp // 2, e, t, lax.div(t, 2), core


def remote(src, dst, send, recv, e, t):
    return pltpu.make_async_remote_copy(
        src_ref=src,
        dst_ref=dst,
        send_sem=send,
        recv_sem=recv,
        device_id=(e, t),
        device_id_type=pl.DeviceIdType.MESH,
    )


def meet():
    n_ep, n_tp, n_y, e, t, y, core = place_of()
    barrier = pltpu.get_barrier_semaphore()

    def greet(pe, pt):
        pl.semaphore_signal(
            barrier, inc=1, device_id=(pe, pt), device_id_type=pl.DeviceIdType.MESH
        )

    for d in range(1, n_ep):
        greet(lax.rem(e + d, n_ep), t)
    greet(e, 2 * y + 1 - core)
    for d in range(1, n_y):
        greet(e, 2 * lax.rem(y + d, n_y) + core)
        greet(e, 2 * lax.rem(y + d, n_y) + 1 - core)
    return lambda: pl.semaphore_wait(barrier, n_ep - 2 + 2 * n_y)


def span(first, last, body):
    def run(d, carry):
        body(d)
        return carry

    lax.fori_loop(first, last, run, 0)


def wide(x):
    return x.astype(jnp.float32)


def whole_kernel(
    group,
    r_hbm,
    k_hbm,
    v_hbm,
    d_hbm,
    a_hbm,
    gate_in_hbm,
    d_off_hbm,
    a_off_hbm,
    extra_hbm,
    gain_hbm,
    out_weight_hbm,
    x_hbm,
    norm_gain_hbm,
    group_router_hbm,
    expert_router_hbm,
    routes_hbm,
    gate_hbm,
    up_hbm,
    down_hbm,
    mixer_ref,
    expert_ref,
    r_ref,
    k_ref,
    v_ref,
    d_ref,
    a_ref,
    gate_in_ref,
    w_ref,
    x_ref,
    d_off_ref,
    a_off_ref,
    extra_in_ref,
    gain_ref,
    norm_gain_ref,
    group_router_ref,
    expert_router_ref,
    routes_ref,
    extra_parts_ref,
    extra_ref,
    normed_ref,
    place_ref,
    near_out_ref,
    far_out_ref,
    picks_ref,
    weight_ref,
    piece_ref,
    out_ref,
    reach_ref,
    every_ref,
    chain_ref,
    mixed_ref,
    mixed_all_ref,
    gate_ref,
    up_ref,
    down_ref,
    hidden_ref,
    gate_part_ref,
    up_part_ref,
    part_ref,
    near_ref,
    stage_ref,
    far_ref,
    final_ref,
    home_ref,
    in_sem,
    gate_sem,
    up_sem,
    down_sem,
    es,
    er,
    cs,
    cr,
    ys,
    yr,
    fs,
    fr,
    zs,
    zr,
    gs,
    gr,
    ns,
    nr,
    bs,
    br,
    hs,
    hr,
    wys,
    wyr,
    wgs,
    wgr,
    wzr,
    wcs,
    wcr,
    xs,
    xr,
):
    n_ep, n_tp, n_y, e, t, y, core = place_of()
    units = gate_ref.shape[1]
    model = x_ref.shape[1]
    tokens = x_ref.shape[0]
    share = model // n_tp
    slots = piece_ref.shape[0]
    capacity = slots // n_ep
    experts = expert_router_ref.shape[0]
    groups = group_router_ref.shape[0]
    positions, width = mixed_ref.shape
    rows = positions // n_tp
    other = 2 * y + 1 - core
    half = n_ep // 2
    half_rows = half * capacity
    wide_units, wide_model = min(256, units), min(512, model)

    def shard(index):
        return pl.ds(pl.multiple_of(index * width, width), width)

    inputs = [(routes_hbm, routes_ref), (norm_gain_hbm, norm_gain_ref), (x_hbm, x_ref)]
    inputs += [(extra_hbm, extra_in_ref), (d_off_hbm, d_off_ref), (a_off_hbm, a_off_ref)]
    inputs += [(k_hbm, k_ref), (a_hbm, a_ref), (d_hbm, d_ref), (r_hbm, r_ref), (v_hbm, v_ref)]
    inputs += [(gate_in_hbm, gate_in_ref), (out_weight_hbm, w_ref.at[shard(t), :]), (gain_hbm, gain_ref)]
    inputs += [(group_router_hbm, group_router_ref), (expert_router_hbm, expert_router_ref)]
    loads = [pltpu.make_async_copy(s, d, in_sem.at[i]) for i, (s, d) in enumerate(inputs)]

    def gate_copy(i):
        at = pl.ds(pl.multiple_of(i * wide_units, wide_units), wide_units)
        return (
            pltpu.make_async_copy(gate_hbm.at[0, :, at], gate_ref.at[:, at], gate_sem.at[0]),
            pltpu.make_async_copy(up_hbm.at[0, :, at], up_ref.at[:, at], up_sem.at[0]),
        )

    def down_copy(i):
        at = pl.ds(pl.multiple_of(i * wide_model, wide_model), wide_model)
        return pltpu.make_async_copy(down_hbm.at[0, :, at], down_ref.at[:, at], down_sem.at[0])

    def partner(d):
        bit, total = 1, 0
        while bit < n_ep:
            total = total + lax.rem(lax.div(e, bit) + lax.div(d, bit), 2) * bit
            bit = 2 * bit
        return total

    def columns(index):
        return pl.ds(pl.multiple_of(index * share, share), share)

    def block(d):
        return pl.ds(pl.multiple_of(d * capacity, capacity), capacity)

    def peer_y(h):
        return lax.rem(y + h, n_y)

    plane = pl.ds(pl.multiple_of(core * (model // 2), model // 2), model // 2)

    def near_ep(d):
        dst = piece_ref.at[block(d), plane]
        return remote(near_out_ref.at[block(d), :], dst, es.at[0], er.at[d], partner(d), t)

    def far_ep(d):
        src = far_out_ref.at[block(d - half), :]
        return remote(src, piece_ref.at[block(d), columns(t)], es.at[1], er.at[d], partner(d), t)

    near_rows, far_rows = slice(capacity, half_rows), slice(half_rows, slots)

    def near_core(at):
        ref = piece_ref.at[at, plane]
        return remote(ref, ref, cs.at[0], cr.at[0], e, other)

    def far_core(at):
        ref = piece_ref.at[at, columns(t)]
        return remote(ref, ref, cs.at[1], cr.at[1], e, other)

    def y_copy(d, h):
        ref = piece_ref.at[block(d), columns(t)]
        peer = 2 * peer_y(h) + core
        return remote(ref, ref, ys.at[h - 1], yr.at[h - 1, d - half], e, peer)

    def forward_copy(at, h):
        ref = piece_ref.at[at, columns(2 * lax.rem(y - h + n_y, n_y) + core)]
        return remote(ref, ref, fs.at[h - 1], fr.at[h - 1], e, other)

    def near_arrived(d):
        near_ep(d).wait_recv()
        near_core(block(d)).start()

    def far_arrived(d):
        far_ep(d).wait_recv()
        for h in range(1, n_y):
            y_copy(d, h).start()
        far_core(block(d)).start()

    def pass_on(d):
        for h in range(1, n_y):
            y_copy(d, h).wait_recv()
            forward_copy(block(d), h).start()

    def gathered():
        for h in range(1, n_y):
            forward_copy(far_rows, h).wait_recv()

    n_x = gs.shape[0] + 1
    n_z = n_ep // n_x
    z, x = lax.div(e, n_x), lax.rem(e, n_x)

    def up_copy(zz):
        ref = every_ref.at[zz * n_x + x]
        return remote(ref, ref, zs.at[zz], zr.at[zz], e + n_x, t)

    def side_copy(zz, h):
        ref = every_ref.at[zz * n_x + x]
        peer = z * n_x + lax.rem(x + h, n_x)
        return remote(ref, ref, gs.at[h - 1, zz], gr.at[h - 1, zz], peer, t)

    def pass_ends(zz):
        @pl.when(z + 1 < n_z)
        def _():
            up_copy(zz).start()

        for h in range(1, n_x):
            side_copy(zz, h).start()

    def relay_ends(i, wanted=True):
        @pl.when((z >= i) & wanted)
        def _():
            up_copy(z - i).wait_recv()
            pass_ends(z - i)

    def collect_ends(zz):
        @pl.when(z >= zz)
        def _():
            for h in range(1, n_x):
                side_copy(zz, h).wait_recv()

    def close_ends(zz):
        @pl.when(z >= zz)
        def _():
            @pl.when(z + 1 < n_z)
            def _():
                up_copy(zz).wait_send()

            for h in range(1, n_x):
                side_copy(zz, h).wait_send()

    def near_copy(b, h):
        at = pl.ds(b * half_rows, half_rows)
        src = part_ref.at[at, columns(2 * peer_y(h) + 1 - core)]
        return remote(src, near_ref.at[h, at, :], ns.at[0], nr.at[b, h], e, other)

    def back_copy(d, h):
        src = stage_ref.at[h, block(d), :]
        dst = far_ref.at[h, block(d), :]
        return remote(src, dst, bs.at[h - 1], br.at[h - 1, d], e, 2 * peer_y(h) + core)

    def home_copy(d):
        src, dst = final_ref.at[block(d), :], home_ref.at[block(e), :]
        return remote(src, dst, hs.at[0], hr.at[0], partner(d), t)

    def all_home():
        src, dst = final_ref.at[capacity:, :], home_ref.at[capacity:, :]
        return remote(src, dst, hs.at[0], hr.at[0], partner(1), t)

    def pair_sum(d, h):
        return wide(part_ref[block(d), columns(2 * peer_y(h) + core)]) + wide(near_ref[h, block(d), :])

    def add_near(b):
        for h in range(1, n_y):
            near_copy(b, h).wait_recv()

        def one(d):
            for h in range(1, n_y):
                stage_ref[h, block(d), :] = bf(pair_sum(d, h))
                back_copy(d, h).start()

        span(b * half, (b + 1) * half, one)

    def add_far(d):
        total = pair_sum(d, 0)
        for h in range(1, n_y):
            back_copy(d, h).wait_recv()
            total = total + wide(far_ref[h, block(d), :])
        return bf(total)

    def go_home(d):
        final_ref[block(d), :] = add_far(d)
        home_copy(d).start()

    tile_count = model // wide_model
    part_rows = width // (2 * n_x)

    def source_of(h):
        return 2 * lax.rem(y - h + n_y, n_y) + core

    def part(index, place):
        return pl.ds(pl.multiple_of(index * width + place * part_rows, part_rows), part_rows)

    own_part = lax.rem(e, 2 * n_x)
    pair_part = lax.rem(own_part + n_x, 2 * n_x)

    def w_plane(h):
        ref = w_ref.at[part(t, own_part), :]
        return remote(ref, ref, wys.at[h - 1], wyr.at[h - 1], e, 2 * peer_y(h) + core)

    def w_pair(h):
        ref = w_ref.at[part(source_of(h), own_part), :]
        return remote(ref, ref, wgs.at[0], wzr.at[h - 1], partner(n_x), t)

    def w_line(h, place, k):
        ref = w_ref.at[part(source_of(h), place), :]
        return remote(ref, ref, wgs.at[0], wgr.at[0], partner(k), t)

    def w_rows(count):
        ref = w_ref.at[: (n_y - 1) * count * part_rows, :]
        return remote(ref, ref, wgs.at[0], wgr.at[0], partner(1), t)

    def w_core(h):
        ref = w_ref.at[shard(source_of(h)), :]
        return remote(ref, ref, wcs.at[h], wcr.at[h], e, other)

    def share_w():
        for h in range(1, n_y):
            w_plane(h).wait_recv()
            w_pair(h).start()
            span(1, n_x, lambda k: w_line(h, own_part, k).start())

    def share_pair_w():
        for h in range(1, n_y):
            w_pair(h).wait_recv()
            span(1, n_x, lambda k: w_line(h, pair_part, k).start())

    def mixed_copy(to):
        src = mixed_ref.at[pl.ds(pl.multiple_of(to * rows, rows), rows), :]
        return remote(src, mixed_all_ref.at[t], xs.at[0], xr.at[0], e, to)

    def all_mixed():
        ref = mixed_all_ref.at[1:]
        return remote(ref, ref, xs.at[0], xr.at[0], e, other)

    def tiles(count, body, hooks):
        for i in range(count):
            body(i)
            for hook in hooks.get(i, ()):
                hook()
        for i in sorted(hooks):
            for hook in hooks[i] if i >= count else ():
                hook()

    def units_at(i):
        return slice(i * wide_units, (i + 1) * wide_units)

    def activate(i, gate_val, up_val):
        hidden_ref[:, units_at(i)] = bf(gate_val * logistic(gate_val) * up_val)

    def widen_near(hooks):
        pltpu.make_async_copy(gate_hbm.at[0], gate_ref, gate_sem.at[0]).wait()
        pltpu.make_async_copy(up_hbm.at[0], up_ref, up_sem.at[0]).wait()

        def unit_tile(i):
            rows_in = piece_ref[:half_rows, :]
            activate(i, mm(rows_in, gate_ref[:, units_at(i)]), mm(rows_in, up_ref[:, units_at(i)]))

        tiles(units // wide_units, unit_tile, hooks)

    def widen_part(i, h):
        model_at = pl.ds(pl.multiple_of(peer_y(h) * 2 * share, 2 * share), 2 * share)
        rows_in = piece_ref[far_rows, model_at]
        return mm(rows_in, gate_ref[model_at, units_at(i)]), mm(rows_in, up_ref[model_at, units_at(i)])

    def widen_far_begin():
        for i in range(units // wide_units):
            gate_part_ref[:, units_at(i)], up_part_ref[:, units_at(i)] = widen_part(i, 0)

    def widen_far_end(hooks):
        def unit_tile(i):
            gate_val, up_val = gate_part_ref[:, units_at(i)], up_part_ref[:, units_at(i)]
            for h in range(1, n_y):
                more = widen_part(i, h)
                gate_val, up_val = gate_val + more[0], up_val + more[1]
            activate(i, gate_val, up_val)

        tiles(units // wide_units, unit_tile, hooks)

    def narrow(b, hooks):
        at = slice(b * half_rows, (b + 1) * half_rows)
        if b == 0:
            pltpu.make_async_copy(down_hbm.at[0], down_ref, down_sem.at[0]).wait()

        def tile(h, ours):
            index = 2 * peer_y(h) + (core if ours else 1 - core)
            part_ref[at, columns(index)] = bf(mm(hidden_ref[...], down_ref[:, columns(index)]))

        for h in range(n_y - 1, 0, -1):
            tile(h, False)
            near_copy(b, h).start()
        for hook in hooks:
            hook()
        for h in range(n_y - 1, 0, -1):
            tile(h, True)
        tile(0, False)
        tile(0, True)
        near_copy(b, 0).start()

    for copy in loads:
        copy.start()
    for i in range(units // wide_units):
        for copy in gate_copy(i):
            copy.start()
    for i in range(model // wide_model):
        down_copy(i).start()
    everyone_here = meet()

    order = flag(iota((tokens, tokens), 0) < iota((tokens, tokens), 1))
    expert_rows = max(16, experts)
    loads[0].wait()
    loads[1].wait()
    own_routes = routes_ref[...]
    names = iota((expert_rows, tokens), 0)
    named = [own_routes[k : k + 1, :] == names for k in range(own_routes.shape[0])]
    match = functools.reduce(jnp.logical_or, named)
    rank = mm(bf(flag(match)), bf(order))
    rank = jnp.where(match, rank, -1.0)
    level = iota((capacity, tokens), 0).astype(jnp.float32)
    for j in range(experts):
        place_ref[j * capacity : (j + 1) * capacity] = bf(flag(level == rank[j : j + 1, :]))
    loads[2].wait()
    step_rows = 32
    for i in range(tokens // step_rows):
        at = slice(i * step_rows, (i + 1) * step_rows)
        xw = wide(x_ref[at])
        scale = lax.rsqrt(jnp.mean(xw * xw, axis=-1, keepdims=True) + norm_eps)
        normed_ref[at] = bf(xw * scale * norm_gain_ref[...])
    here = jnp.concatenate([place_ref[block(partner(d)), :] for d in range(1, half)], axis=0)
    near_out_ref[capacity:half_rows] = bf(mm(here, normed_ref[:, plane]))
    there = jnp.concatenate([place_ref[block(partner(d)), :] for d in range(half, n_ep)], axis=0)
    far_out_ref[...] = bf(mm(there, normed_ref[:, columns(t)]))
    per = max(1, n_ep // 8)

    def unit(u, body):
        lo = max(1, min(n_ep, u * per))
        return lambda: span(lo, max(lo, min(n_ep, (u + 1) * per)), body)

    inner = lax.rem(lax.div(z + 1, 2), 2)

    def far_unit(k, body):
        first = [4 + 2 * inner, 5 + 2 * inner, 6 - 2 * inner, 7 - 2 * inner][k] * per
        return lambda: span(first, first + per, body)

    everyone_here()
    span(1, half, lambda d: near_ep(d).start())
    for k in range(4):
        far_unit(k, lambda d: far_ep(d).start())()
    for i in range(model // wide_model):
        at = slice(i * wide_model, (i + 1) * wide_model)
        piece_ref[:capacity, at] = bf(mm(place_ref[block(e), :], normed_ref[:, at]))

    loads[12].wait()
    for h in range(1, n_y):
        w_plane(h).start()
    w_core(0).start()
    for copy in loads[3:11]:
        copy.wait()
    heads, pairs = extra_in_ref.shape[0], chain_ref.shape[0]
    exact = extra_in_ref[...]
    extra_parts_ref[...] = jnp.zeros(extra_parts_ref.shape, jnp.float32)
    for i in range(3):
        piece = wide(bf(exact))
        extra_parts_ref[i * heads : (i + 1) * heads, :] = piece
        exact = exact - piece
    extra_parts = bf(extra_parts_ref[...])
    extra_rows = extra_parts_ref.shape[0]
    for p in range(pairs):
        head = lax.rem(iota((extra_rows, PAIR), 0), heads)
        wanted = head == 2 * p + lax.div(iota((extra_rows, PAIR), 1), HEAD_DIM)
        extra_ref[:, p * PAIR : (p + 1) * PAIR] = mm_tn(extra_parts, bf(flag(wanted)))
    steps = positions // (group * HEAD_DIM)
    events = {}

    def pump(g, point):
        for step in range(steps):
            due = events.get(4 * step + point)
            if due:

                @pl.when(g == step)
                def _(due=due):
                    for act in due:
                        act()

    scan_kernel(
        group,
        pump,
        r_ref,
        k_ref,
        v_ref,
        d_ref,
        a_ref,
        d_off_ref,
        a_off_ref,
        extra_ref,
        out_ref,
        reach_ref,
        every_ref.at[e],
        chain_ref,
    )
    for i in sorted(events):
        for act in events[i] if i >= 4 * steps else ():
            act()
    pass_ends(z)
    span(1, half, near_arrived)
    far_unit(0, far_arrived)()
    far_unit(1, far_arrived)()
    share_w()
    near_core(near_rows).wait_recv()
    relays = [lambda i=i: relay_ends(i) for i in range(1, n_z)]
    widen_near({2: [far_unit(2, far_arrived)], 3: [far_unit(0, pass_on)]})
    far_unit(1, pass_on)()
    narrow(0, [far_unit(3, far_arrived)])
    far_unit(2, pass_on)()
    add_near(0)
    for copy in loads[11:12] + loads[13:]:
        copy.wait()

    normed = normed_ref[...]
    group_logit = mm_nt(group_router_ref[...], normed)
    group_exp = jnp.exp(group_logit)
    group_prob = group_exp / jnp.sum(group_exp, axis=0, keepdims=True)
    expert_logit = mm_nt(expert_router_ref[...], normed)
    per_group = experts // groups
    first_of = iota((groups, tokens), 0) * per_group
    expert_names = iota((experts, tokens), 0)
    chosen, prob = [], []
    for k in range(2):
        route = own_routes[k : k + 1, :]
        chosen.append(
            jnp.sum(jnp.where(route == expert_names, expert_logit, 0.0), axis=0, keepdims=True)
        )
        inside = (route >= first_of) & (route < first_of + per_group)
        prob.append(jnp.sum(jnp.where(inside, group_prob, 0.0), axis=0, keepdims=True))
    weights = [prob[0] * logistic(chosen[0] - chosen[1]), prob[1] * logistic(chosen[1] - chosen[0])]
    for k in range(2):
        weight_ref[k] = jnp.transpose(jnp.broadcast_to(weights[k], (128, tokens)))
        for j in range(experts):
            at = slice(j * capacity, (j + 1) * capacity)
            picks_ref[k, at] = place_ref[at] * bf(flag(own_routes[k : k + 1, :] == j))
    far_core(far_rows).wait_recv()
    widen_far_begin()
    for relay in relays[:1]:
        relay()
    with jax.named_scope("pass3"):
        far_unit(3, pass_on)()
    near_copy(0, 0).wait_recv()
    gathered()
    last = z == n_z - 1
    passing = [lambda i=i: relay_ends(i, ~last) for i in range(2, min(3, n_z))]
    widen_far_end({1: passing})
    late = [lambda i=i: relay_ends(i, last if i < 3 else True) for i in range(2, n_z)]
    narrow(1, late + [share_pair_w])
    add_near(1)
    span(1, half, go_home)
    near_copy(1, 0).wait_recv()
    unit(4, go_home)()
    for u in range(5, 8):
        unit(u, go_home)()
    home_ref[block(e), :] = add_far(0)
    span(0, n_z, collect_ends)
    owners = [2 * peer_y(h) + c for h in range(1, n_y) for c in (core, 1 - core)] + [other, t]

    def joined(i):
        if i + 1 < n_tp:
            mixed_copy(owners[i]).start()

    join_kernel(
        "ep", every_ref, out_ref, reach_ref, gate_in_ref, gain_ref, mixed_ref, owners, joined
    )
    mixed_all_ref[t] = mixed_ref[pl.ds(pl.multiple_of(t * rows, rows), rows), :]
    w_rows(2 * n_x - 2).wait_recv()
    for h in range(1, n_y):
        w_core(h).start()
    all_mixed().wait_recv()
    for h in range(n_y):
        w_core(h).wait_recv()
    mixed = jnp.concatenate([mixed_all_ref[j] for j in range(n_tp)], axis=1)

    def project(i):
        at = pl.ds(pl.multiple_of(i * wide_model, wide_model), wide_model)
        mixer_ref[:, at] = bf(mm(mixed, w_ref[:, at]))

    for i in range(tile_count):
        project(i)

    near_src = near_out_ref.at[near_rows, :]
    remote(near_src, near_src, es.at[0], er.at[0], e, other).wait_send()
    remote(far_out_ref, far_out_ref, es.at[1], er.at[0], e, other).wait_send()
    near_core(near_rows).wait_send()
    far_core(far_rows).wait_send()
    remote(near_ref, near_ref, ns.at[0], nr.at[0, 0], e, other).wait_send()
    for h in range(1, n_y):
        ref = piece_ref.at[far_rows, columns(t)]
        remote(ref, ref, ys.at[h - 1], yr.at[h - 1, 0], e, other).wait_send()
        forward_copy(far_rows, h).wait_send()
        ref = stage_ref.at[h]
        remote(ref, ref, bs.at[h - 1], br.at[h - 1, 0], e, other).wait_send()
        w_plane(h).wait_send()
    for h in range(n_y):
        w_core(h).wait_send()
    w_rows(2 * n_x - 1).wait_send()
    all_mixed().wait_send()
    span(0, n_z, close_ends)
    all_home().wait_recv()
    back = home_ref[...]
    first, second = mm_tn(picks_ref[0], back), mm_tn(picks_ref[1], back)
    for i in range(share // 128):
        at = slice(i * 128, (i + 1) * 128)
        expert_ref[:, at] = bf(weight_ref[0] * first[:, at] + weight_ref[1] * second[:, at])
    all_home().wait_send()


def local(
    receptance,
    key_matrix,
    value_matrix,
    decay_data_term,
    correction_rate_data,
    output_gate_input,
    decay_channel_offset,
    correction_rate_offset,
    extra_head_log_decay,
    head_norm_gain,
    mixer_output_weight,
    expert_layer_input,
    feedforward_norm_gain,
    group_router_weight,
    expert_router_weight,
    routes,
    expert_gate_weight,
    expert_up_weight,
    expert_down_weight,
):
    positions, own_width = receptance.shape
    pairs = -(-own_width // PAIR)
    width = pairs * PAIR

    def filled(x, columns=width):
        return x if x.shape[-1] == columns else jnp.pad(x, ((0, 0), (0, columns - x.shape[-1])))

    blocks = positions // HEAD_DIM
    group = 4 if blocks % 4 == 0 else 1
    n_ep, n_tp = lax.axis_size("ep"), lax.axis_size("tp")
    n_y = n_tp // 2
    n_x = 1
    while 4 * n_x * n_x <= n_ep:
        n_x = 2 * n_x
    tokens, model = expert_layer_input.shape
    capacity, share = 4 * tokens // n_ep, model // n_tp
    slots = n_ep * capacity
    units = expert_gate_weight.shape[2]
    rows = positions // n_tp
    out_weight = jnp.pad(mixer_output_weight, ((0, width - own_width), (0, 0)))

    def held(*shape):
        return pltpu.VMEM(shape, jnp.bfloat16)

    def single(*shape):
        return pltpu.VMEM(shape, jnp.float32)

    def sems(*shape):
        return pltpu.SemaphoreType.DMA(shape)

    operands = (
        filled(receptance),
        filled(key_matrix),
        filled(value_matrix),
        filled(decay_data_term),
        filled(correction_rate_data),
        filled(output_gate_input),
        filled(decay_channel_offset[None]),
        filled(correction_rate_offset[None]),
        filled(extra_head_log_decay, 2 * pairs).T,
        filled(head_norm_gain[None]),
        out_weight,
        expert_layer_input,
        feedforward_norm_gain[None],
        group_router_weight.T,
        expert_router_weight.T,
        routes.T,
        expert_gate_weight,
        expert_up_weight,
        expert_down_weight,
    )
    in_vmem, in_hbm = pl.BlockSpec(memory_space=pltpu.VMEM), pl.BlockSpec(memory_space=pltpu.HBM)
    one, hops = sems(n_ep), sems(n_y - 1)
    mixer_out, expert_out = pl.pallas_call(
        functools.partial(whole_kernel, group),
        out_shape=(held(rows, model), held(tokens, share)),
        in_specs=[in_hbm] * 19,
        out_specs=[in_vmem] * 2,
        scratch_shapes=[held(positions, width)] * 6
        + [
            held(n_tp * width, model),
            held(tokens, model),
            single(1, width),
            single(1, width),
            single(2 * pairs, positions),
            single(1, width),
            single(1, model),
            held(*group_router_weight.shape[::-1]),
            held(*expert_router_weight.shape[::-1]),
            pltpu.VMEM(routes.shape[::-1], jnp.int32),
            single(16, positions),
            single(positions, width),
            held(tokens, model),
            held(slots, tokens),
            held(slots // 2, model // 2),
            held(slots // 2, share),
            held(2, slots, tokens),
            single(2, tokens, 128),
            held(slots, model),
            single(positions, width),
            held(positions, width),
            held(n_ep, pairs * 2 * HEAD_DIM, PAIR),
            single(pairs, 2 * PAIR, PAIR),
            held(positions, width),
            held(n_tp, rows, width),
            held(model, units),
            held(model, units),
            held(units, model),
            held(slots // 2, units),
            single(slots // 2, units),
            single(slots // 2, units),
            held(slots, model),
        ]
        + [held(n_y, slots, share)] * 3
        + [held(slots, share)] * 2
        + [sems(16)]
        + [sems(1)] * 3
        + [sems(2), one, sems(2), sems(2)]
        + [hops, sems(n_y - 1, n_ep // 2), hops, hops]
        + [sems(n_ep // n_x)] * 2
        + [sems(n_x - 1, n_ep // n_x)] * 2
        + [sems(1), sems(2, n_y)]
        + [hops, sems(n_y - 1, n_ep)]
        + [sems(1)] * 2
        + [hops, hops, sems(1), sems(1), hops, sems(n_y), sems(n_y), sems(1), sems(1)],
        compiler_params=pltpu.CompilerParams(
            collective_id=0, has_side_effects=True, vmem_limit_bytes=VMEM_LIMIT
        ),
    )(
        *(pltpu.with_memory_space_constraint(x, pltpu.HBM) for x in operands)
    )
    return mixer_out, expert_out


def solution(mesh):
    in_specs = (
        P("ep", "tp"),
        P("ep", "tp"),
        P("ep", "tp"),
        P("ep", "tp"),
        P("ep", "tp"),
        P("ep", "tp"),
        P("tp"),
        P("tp"),
        P("ep", "tp"),
        P("tp"),
        P("tp", None),
        P("ep", None),
        P(),
        P(),
        P(),
        P("ep", None),
        P("ep", None, "tp"),
        P("ep", None, "tp"),
        P("ep", "tp", None),
    )
    out_specs = (P(("ep", "tp"), None), P("ep", "tp"))
    return jax.shard_map(local, mesh=mesh, in_specs=in_specs, out_specs=out_specs, check_vma=False)
```

```python
import functools
import math

import jax
import jax.numpy as jnp
from jax import lax
from jax.experimental import pallas as pl
from jax.experimental.pallas import tpu as pltpu
from jax.sharding import PartitionSpec as P

HEAD_DIM = 64
PAIR = 2 * HEAD_DIM
VMEM_LIMIT = 48 << 20
HALF_EXP = math.exp(-0.5)
GROUPS = 4


key_eps = 1e-06
group_eps = 0.00064
norm_eps = 1e-06
highest = lax.Precision.HIGHEST


def bf(x):
    return x.astype(jnp.bfloat16)


def mm(x, y):
    return lax.dot_general(x, y, (((1,), (0,)), ((), ())), preferred_element_type=jnp.float32)


def mm_nt(x, y):
    return lax.dot_general(x, y, (((1,), (1,)), ((), ())), preferred_element_type=jnp.float32)


def mm_tn(x, y):
    return lax.dot_general(x, y, (((0,), (0,)), ((), ())), preferred_element_type=jnp.float32)


def halves(x):
    high = bf(x)
    return high, bf(x - high.astype(jnp.float32))


def sum_right(x, ones):
    high, low = halves(x)
    return mm(high, ones) + mm(low, ones)


def logistic(x):
    return 1.0 / (1.0 + jnp.exp(-x))


def flag(cond):
    return jnp.where(cond, 1.0, 0.0)


def iota(shape, dim):
    return lax.broadcasted_iota(jnp.int32, shape, dim)


def pair_blocks():
    return flag((iota((PAIR, PAIR), 0) < HEAD_DIM) == (iota((PAIR, PAIR), 1) < HEAD_DIM))


def scan_kernel(
    group,
    pump,
    r_ref,
    k_ref,
    v_ref,
    d_ref,
    a_ref,
    d_off_ref,
    a_off_ref,
    extra_ref,
    out_ref,
    reach_ref,
    ends_ref,
    chain_ref,
):
    positions, width = r_ref.shape
    pairs = width // PAIR
    C = HEAD_DIM
    rows_per = group * C
    own_block = pair_blocks()
    own_bf = bf(own_block)
    row, col = iota((C, PAIR), 0), iota((C, PAIR), 1) & (HEAD_DIM - 1)
    strict, upto = row > col, row >= col
    eye = flag(row == col)
    tri = bf(flag(iota((C, C), 0) >= iota((C, C), 1)))
    level_masks = []
    for s in range(6):
        inside = (
            ((row >> (s + 1)) == (col >> (s + 1)))
            & (((row >> s) & 1) == 1)
            & (((col >> s) & 1) == 0)
        )
        level_masks.append(bf(flag(inside)))

    def spread(x):
        return jnp.concatenate([x, x], axis=0) * own_bf

    square = (iota((PAIR, PAIR), 0) == iota((PAIR, PAIR), 1)).astype(jnp.float32)
    for p in range(pairs):
        chain_ref[p, :PAIR] = jnp.zeros((PAIR, PAIR), jnp.float32)
        chain_ref[p, PAIR:] = square

    def step(g, carry):
        base = pl.multiple_of(g * rows_per, rows_per)
        rows = pl.ds(base, rows_per)
        items = []
        for p in range(pairs):
            lanes = slice(p * PAIR, (p + 1) * PAIR)
            k = k_ref[rows, lanes].astype(jnp.float32)
            u = k * lax.rsqrt(sum_right(k * k, own_bf) + key_eps)
            rem = u * logistic(a_ref[rows, lanes].astype(jnp.float32) + a_off_ref[:, lanes])
            lg = extra_ref[rows, lanes] - HALF_EXP * logistic(
                d_ref[rows, lanes].astype(jnp.float32) + d_off_ref[:, lanes]
            )
            r = r_ref[rows, lanes].astype(jnp.float32)
            v = v_ref[rows, lanes]
            for c in range(group):
                cut = slice(c * C, (c + 1) * C)
                items.append((p, c, k[cut], u[cut], rem[cut], lg[cut], r[cut], v[cut]))
        stage = []
        for p, c, k, u, rem, lg, r, v in items:
            high, low = halves(lg)
            rest = bf(lg - high.astype(jnp.float32) - low.astype(jnp.float32))
            cumul = mm(tri, high) + mm(tri, low) + mm(tri, rest)
            stage.append(cumul)
        work = []
        for (p, c, k, u, rem, lg, r, v), cumul in zip(items, stage):
            mid = 0.5 * cumul[C - 1 : C]
            up_now, down = jnp.exp(cumul - mid), jnp.exp(mid - cumul)
            up_before = jnp.exp(cumul - lg - mid)
            half = jnp.exp(mid)
            cq, cu, dk, dr = r * up_now, u * up_before, k * down, rem * down
            left = bf(jnp.concatenate([cu, cq], axis=0))
            pair_r = mm_nt(left, spread(bf(dr)))
            pair_k = mm_nt(left, spread(bf(dk)))
            work.append((cq * half, bf(cu * half), bf(dk * half), bf(dr * half), half * half, pair_r, pair_k))
        pump(g, 0)
        solve = []
        for (p, c, k, u, rem, lg, r, v), (qe, ue, kt, rt, ed, pair_r, pair_k) in zip(items, work):
            rp = bf(jnp.where(strict, pair_r[:C], 0.0))
            rr = bf(jnp.where(upto, pair_r[C:], 0.0))
            kp = jnp.where(strict, pair_k[:C], 0.0)
            rk = jnp.where(upto, pair_k[C:], 0.0)
            kv = mm(bf(jnp.concatenate([kp, rk], axis=0)), spread(v))
            inv = eye - (rp * level_masks[0]).astype(jnp.float32)
            solve.append([rp, rr, kv, inv])
        for s in range(1, 6):
            mids = [bf(mm(bf(inv), spread(rp * level_masks[s]))) for rp, rr, kv, inv in solve]
            for item, y in zip(solve, mids):
                item[3] = item[3] - mm(y, spread(bf(item[3])))
            if s == 2:
                pump(g, 1)
        wvs = []
        for (rp, rr, kv, inv), w in zip(solve, work):
            wide = jnp.concatenate([spread(w[1]), spread(bf(kv[:C]))], axis=1)
            wvs.append(bf(mm(bf(inv), wide)))
        pump(g, 2)
        tails = []
        for (rp, rr, kv, inv), (qe, ue, kt, rt, ed, _, _), wv, item in zip(solve, work, wvs, items):
            wide = jnp.concatenate([spread(wv[:, :PAIR]), spread(wv[:, PAIR:])], axis=1)
            rw = mm(rr, wide)
            read = bf(qe - rw[:, :PAIR])
            local = kv[C:] - rw[:, PAIR:]
            v = item[7]
            x = jnp.concatenate(
                [jnp.concatenate([v, jnp.zeros_like(v)], axis=1),
                 jnp.concatenate([-wv[:, PAIR:], -wv[:, :PAIR]], axis=1)], axis=0)
            nb = mm_tn(x, jnp.concatenate([kt, rt], axis=0))
            tails.append((read, local, nb[:PAIR] * own_block, bf(nb[PAIR:] * own_block), ed))
        z = [chain_ref[p] for p in range(pairs)]
        for c in range(group):
            for p in range(pairs):
                read, local, add, neg, ed = tails[p * group + c]
                zb = bf(z[p])
                qz = mm_nt(read, zb)
                at = pl.ds(pl.multiple_of(base + c * C, C), C)
                lanes = slice(p * PAIR, (p + 1) * PAIR)
                out_ref[at, lanes] = local + qz[:, :PAIR]
                reach_ref[at, lanes] = bf(qz[:, PAIR:])
                moved = z[p] * ed + mm(zb, neg)
                z[p] = jnp.concatenate([moved[:PAIR] + add, moved[PAIR:]], axis=0)
        for p in range(pairs):
            chain_ref[p] = z[p]
        pump(g, 3)
        return carry

    lax.fori_loop(0, positions // rows_per, step, 0)
    for p in range(pairs):
        s, m = chain_ref[p, :PAIR], chain_ref[p, PAIR:]
        ends_ref[p * 2 * C : p * 2 * C + C] = bf(s[:C] + s[C:])
        ends_ref[p * 2 * C + C : (p + 1) * 2 * C] = bf(m[:C] + m[C:])


def join_kernel(axis, all_ref, out_ref, reach_ref, gate_ref, gain_ref, mixed_ref, planes, done):
    devices, place = lax.axis_size(axis), lax.axis_index(axis)
    width = out_ref.shape[1]
    pairs = width // PAIR
    C = HEAD_DIM
    own_block = pair_blocks()
    own_bf = bf(own_block)
    mean_bf = bf(own_block * (1.0 / HEAD_DIM))
    states = [jnp.zeros((C, PAIR), jnp.float32) for _ in range(pairs)]

    def hop(j, states):
        new = []
        for p in range(pairs):
            s = all_ref[j, p * 2 * C : p * 2 * C + C].astype(jnp.float32)
            m = all_ref[j, p * 2 * C + C : (p + 1) * 2 * C]
            m = jnp.concatenate([m, m], axis=0) * own_bf
            new.append(sum_right(states[p], m) + s)
        return tuple(new)

    states = lax.fori_loop(0, place, hop, tuple(states))
    rows = out_ref.shape[0] // len(planes)
    moves = []
    for p in range(pairs):
        s = bf(states[p])
        moves.append(jnp.concatenate([s, s], axis=0) * own_bf)
    for i, plane in enumerate(planes):
        at = pl.ds(pl.multiple_of(plane * rows, rows), rows)
        for p in range(pairs):
            lanes = slice(p * PAIR, (p + 1) * PAIR)
            head = out_ref[at, lanes] + mm_nt(reach_ref[at, lanes], moves[p])
            centred = head - sum_right(head, mean_bf)
            spread = sum_right(centred * centred, mean_bf)
            normed = centred * lax.rsqrt(spread + group_eps)
            gate = logistic(gate_ref[at, lanes].astype(jnp.float32))
            mixed_ref[at, lanes] = bf(normed * gain_ref[:, lanes] * gate)
        done(i)


def place_of():
    n_ep, n_tp = lax.axis_size("ep"), lax.axis_size("tp")
    e, t = lax.axis_index("ep"), lax.axis_index("tp")
    core = lax.rem(t, 2)
    return n_ep, n_tp, n_tp // 2, e, t, lax.div(t, 2), core


def remote(src, dst, send, recv, e, t):
    return pltpu.make_async_remote_copy(
        src_ref=src,
        dst_ref=dst,
        send_sem=send,
        recv_sem=recv,
        device_id=(e, t),
        device_id_type=pl.DeviceIdType.MESH,
    )


def meet():
    n_ep, n_tp, n_y, e, t, y, core = place_of()
    barrier = pltpu.get_barrier_semaphore()

    def greet(pe, pt):
        pl.semaphore_signal(
            barrier, inc=1, device_id=(pe, pt), device_id_type=pl.DeviceIdType.MESH
        )

    for d in range(1, n_ep):
        greet(lax.rem(e + d, n_ep), t)
    greet(e, 2 * y + 1 - core)
    for d in range(1, n_y):
        greet(e, 2 * lax.rem(y + d, n_y) + core)
        greet(e, 2 * lax.rem(y + d, n_y) + 1 - core)
    return lambda: pl.semaphore_wait(barrier, n_ep - 2 + 2 * n_y)


def span(first, last, body):
    def run(d, carry):
        body(d)
        return carry

    lax.fori_loop(first, last, run, 0)


def wide(x):
    return x.astype(jnp.float32)


def whole_kernel(
    group,
    r_hbm,
    k_hbm,
    v_hbm,
    d_hbm,
    a_hbm,
    gate_in_hbm,
    d_off_hbm,
    a_off_hbm,
    extra_hbm,
    gain_hbm,
    out_weight_hbm,
    x_hbm,
    norm_gain_hbm,
    group_router_hbm,
    expert_router_hbm,
    routes_hbm,
    gate_hbm,
    up_hbm,
    down_hbm,
    mixer_ref,
    expert_ref,
    r_ref,
    k_ref,
    v_ref,
    d_ref,
    a_ref,
    gate_in_ref,
    w_ref,
    x_ref,
    d_off_ref,
    a_off_ref,
    extra_in_ref,
    gain_ref,
    norm_gain_ref,
    group_router_ref,
    expert_router_ref,
    routes_ref,
    extra_parts_ref,
    extra_ref,
    normed_ref,
    place_ref,
    near_out_ref,
    far_out_ref,
    picks_ref,
    weight_ref,
    piece_ref,
    out_ref,
    reach_ref,
    every_ref,
    chain_ref,
    mixed_ref,
    mixed_all_ref,
    gate_ref,
    up_ref,
    down_ref,
    hidden_ref,
    gate_part_ref,
    up_part_ref,
    part_ref,
    near_ref,
    stage_ref,
    far_ref,
    final_ref,
    home_ref,
    in_sem,
    gate_sem,
    up_sem,
    down_sem,
    es,
    er,
    cs,
    cr,
    ys,
    yr,
    fs,
    fr,
    zs,
    zr,
    gs,
    gr,
    ns,
    nr,
    bs,
    br,
    hs,
    hr,
    wys,
    wyr,
    wgs,
    wgr,
    wzr,
    wcs,
    wcr,
    xs,
    xr,
):
    n_ep, n_tp, n_y, e, t, y, core = place_of()
    units = gate_ref.shape[1]
    model = x_ref.shape[1]
    tokens = x_ref.shape[0]
    share = model // n_tp
    slots = piece_ref.shape[0]
    capacity = slots // n_ep
    experts = expert_router_ref.shape[0]
    groups = group_router_ref.shape[0]
    positions, width = mixed_ref.shape
    rows = positions // n_tp
    other = 2 * y + 1 - core
    half = n_ep // 2
    half_rows = half * capacity
    wide_units, wide_model = min(256, units), min(512, model)

    def shard(index):
        return pl.ds(pl.multiple_of(index * width, width), width)

    x_rows = [slice(i * tokens // 4, (i + 1) * tokens // 4) for i in range(4)]
    inputs = [(routes_hbm, routes_ref), (norm_gain_hbm, norm_gain_ref)]
    inputs += [(x_hbm.at[at, :], x_ref.at[at, :]) for at in x_rows]
    inputs += [(extra_hbm, extra_in_ref), (d_off_hbm, d_off_ref), (a_off_hbm, a_off_ref)]
    inputs += [(k_hbm, k_ref), (a_hbm, a_ref), (d_hbm, d_ref), (r_hbm, r_ref), (v_hbm, v_ref)]
    inputs += [(gate_in_hbm, gate_in_ref), (out_weight_hbm, w_ref.at[shard(t), :]), (gain_hbm, gain_ref)]
    inputs += [(group_router_hbm, group_router_ref), (expert_router_hbm, expert_router_ref)]
    loads = [pltpu.make_async_copy(s, d, in_sem.at[i]) for i, (s, d) in enumerate(inputs)]

    def gate_copy(i):
        at = pl.ds(pl.multiple_of(i * wide_units, wide_units), wide_units)
        return (
            pltpu.make_async_copy(gate_hbm.at[0, :, at], gate_ref.at[:, at], gate_sem.at[0]),
            pltpu.make_async_copy(up_hbm.at[0, :, at], up_ref.at[:, at], up_sem.at[0]),
        )

    def down_copy(i):
        at = pl.ds(pl.multiple_of(i * wide_model, wide_model), wide_model)
        return pltpu.make_async_copy(down_hbm.at[0, :, at], down_ref.at[:, at], down_sem.at[0])

    def partner(d):
        bit, total = 1, 0
        while bit < n_ep:
            total = total + lax.rem(lax.div(e, bit) + lax.div(d, bit), 2) * bit
            bit = 2 * bit
        return total

    def columns(index):
        return pl.ds(pl.multiple_of(index * share, share), share)

    def block(d):
        return pl.ds(pl.multiple_of(d * capacity, capacity), capacity)

    def peer_y(h):
        return lax.rem(y + h, n_y)

    plane = pl.ds(pl.multiple_of(core * (model // 2), model // 2), model // 2)

    def near_ep(d):
        dst = piece_ref.at[block(d), plane]
        return remote(near_out_ref.at[block(d), :], dst, es.at[0], er.at[d], partner(d), t)

    def far_ep(d):
        src = far_out_ref.at[block(d - half), :]
        return remote(src, piece_ref.at[block(d), columns(t)], es.at[1], er.at[d], partner(d), t)

    near_rows, far_rows = slice(capacity, half_rows), slice(half_rows, slots)

    def near_core(at):
        ref = piece_ref.at[at, plane]
        return remote(ref, ref, cs.at[0], cr.at[0], e, other)

    def far_core(at):
        ref = piece_ref.at[at, columns(t)]
        return remote(ref, ref, cs.at[1], cr.at[1], e, other)

    def y_copy(d, h):
        ref = piece_ref.at[block(d), columns(t)]
        peer = 2 * peer_y(h) + core
        return remote(ref, ref, ys.at[h - 1], yr.at[h - 1, d - half], e, peer)

    def forward_copy(at, h):
        ref = piece_ref.at[at, columns(2 * lax.rem(y - h + n_y, n_y) + core)]
        return remote(ref, ref, fs.at[h - 1], fr.at[h - 1], e, other)

    def near_arrived(d):
        near_ep(d).wait_recv()
        near_core(block(d)).start()

    def far_arrived(d):
        far_ep(d).wait_recv()
        for h in range(1, n_y):
            y_copy(d, h).start()
        far_core(block(d)).start()

    def pass_on(d):
        for h in range(1, n_y):
            y_copy(d, h).wait_recv()
            forward_copy(block(d), h).start()

    def gathered():
        for h in range(1, n_y):
            forward_copy(far_rows, h).wait_recv()

    n_x = gs.shape[0] + 1
    n_z = n_ep // n_x
    z, x = lax.div(e, n_x), lax.rem(e, n_x)

    def up_copy(zz):
        ref = every_ref.at[zz * n_x + x]
        return remote(ref, ref, zs.at[zz], zr.at[zz], e + n_x, t)

    def side_copy(zz, h):
        ref = every_ref.at[zz * n_x + x]
        peer = z * n_x + lax.rem(x + h, n_x)
        return remote(ref, ref, gs.at[h - 1, zz], gr.at[h - 1, zz], peer, t)

    def pass_ends(zz):
        @pl.when(z + 1 < n_z)
        def _():
            up_copy(zz).start()

        for h in range(1, n_x):
            side_copy(zz, h).start()

    def relay_ends(i, wanted=True):
        @pl.when((z >= i) & wanted)
        def _():
            up_copy(z - i).wait_recv()
            pass_ends(z - i)

    def collect_ends(zz):
        @pl.when(z >= zz)
        def _():
            for h in range(1, n_x):
                side_copy(zz, h).wait_recv()

    def close_ends(zz):
        @pl.when(z >= zz)
        def _():
            @pl.when(z + 1 < n_z)
            def _():
                up_copy(zz).wait_send()

            for h in range(1, n_x):
                side_copy(zz, h).wait_send()

    def near_copy(b, h):
        at = pl.ds(b * half_rows, half_rows)
        src = part_ref.at[at, columns(2 * peer_y(h) + 1 - core)]
        return remote(src, near_ref.at[h, at, :], ns.at[0], nr.at[b, h], e, other)

    def back_copy(d, h):
        src = stage_ref.at[h, block(d), :]
        dst = far_ref.at[h, block(d), :]
        return remote(src, dst, bs.at[h - 1], br.at[h - 1, d], e, 2 * peer_y(h) + core)

    def home_copy(d):
        src, dst = final_ref.at[block(d), :], home_ref.at[block(e), :]
        return remote(src, dst, hs.at[0], hr.at[0], partner(d), t)

    def all_home():
        src, dst = final_ref.at[capacity:, :], home_ref.at[capacity:, :]
        return remote(src, dst, hs.at[0], hr.at[0], partner(1), t)

    def pair_sum(d, h):
        return wide(part_ref[block(d), columns(2 * peer_y(h) + core)]) + wide(near_ref[h, block(d), :])

    def add_near(b):
        for h in range(1, n_y):
            near_copy(b, h).wait_recv()

        def one(d):
            for h in range(1, n_y):
                stage_ref[h, block(d), :] = bf(pair_sum(d, h))
                back_copy(d, h).start()

        span(b * half, (b + 1) * half, one)

    def add_far(d):
        total = pair_sum(d, 0)
        for h in range(1, n_y):
            back_copy(d, h).wait_recv()
            total = total + wide(far_ref[h, block(d), :])
        return bf(total)

    def go_home(d):
        final_ref[block(d), :] = add_far(d)
        home_copy(d).start()

    tile_count = model // wide_model
    part_rows = width // (2 * n_x)

    def source_of(h):
        return 2 * lax.rem(y - h + n_y, n_y) + core

    def part(index, place):
        return pl.ds(pl.multiple_of(index * width + place * part_rows, part_rows), part_rows)

    own_part = lax.rem(e, 2 * n_x)
    pair_part = lax.rem(own_part + n_x, 2 * n_x)

    def w_plane(h):
        ref = w_ref.at[part(t, own_part), :]
        return remote(ref, ref, wys.at[h - 1], wyr.at[h - 1], e, 2 * peer_y(h) + core)

    def w_pair(h):
        ref = w_ref.at[part(source_of(h), own_part), :]
        return remote(ref, ref, wgs.at[0], wzr.at[h - 1], partner(n_x), t)

    def w_line(h, place, k):
        ref = w_ref.at[part(source_of(h), place), :]
        return remote(ref, ref, wgs.at[0], wgr.at[0], partner(k), t)

    def w_rows(count):
        ref = w_ref.at[: (n_y - 1) * count * part_rows, :]
        return remote(ref, ref, wgs.at[0], wgr.at[0], partner(1), t)

    def w_core(h):
        ref = w_ref.at[shard(source_of(h)), :]
        return remote(ref, ref, wcs.at[h], wcr.at[h], e, other)

    def w_core_part(h, place):
        ref = w_ref.at[part(source_of(h), place), :]
        return remote(ref, ref, wcs.at[h], wcr.at[h], e, other)

    def share_w():
        for h in range(1, n_y):
            w_plane(h).wait_recv()
            w_pair(h).start()
            span(1, n_x, lambda k: w_line(h, own_part, k).start())
            w_core_part(h, own_part).start()

    def share_pair_w(wanted):
        @pl.when(wanted)
        def _():
            for h in range(1, n_y):
                w_pair(h).wait_recv()
                span(1, n_x, lambda k: w_line(h, pair_part, k).start())
                w_core_part(h, pair_part).start()

    def share_line_w():
        w_rows(2 * n_x - 2).wait_recv()
        for h in range(1, n_y):
            for shift in (0, n_x):

                def one(k):
                    place = lax.rem(partner(k) + shift, 2 * n_x)
                    w_core_part(h, place).start()

                span(1, n_x, one)

    def mixed_copy(to):
        src = mixed_ref.at[pl.ds(pl.multiple_of(to * rows, rows), rows), :]
        return remote(src, mixed_all_ref.at[t], xs.at[0], xr.at[0], e, to)

    def all_mixed():
        ref = mixed_all_ref.at[1:]
        return remote(ref, ref, xs.at[0], xr.at[0], e, other)

    def tiles(count, body, hooks):
        for i in range(count):
            body(i)
            for hook in hooks.get(i, ()):
                hook()
        for i in sorted(hooks):
            for hook in hooks[i] if i >= count else ():
                hook()

    def units_at(i):
        return slice(i * wide_units, (i + 1) * wide_units)

    def activate(i, gate_val, up_val):
        hidden_ref[:, units_at(i)] = bf(gate_val * logistic(gate_val) * up_val)

    def widen_near(hooks):
        pltpu.make_async_copy(gate_hbm.at[0], gate_ref, gate_sem.at[0]).wait()
        pltpu.make_async_copy(up_hbm.at[0], up_ref, up_sem.at[0]).wait()

        def unit_tile(i):
            rows_in = piece_ref[:half_rows, :]
            activate(i, mm(rows_in, gate_ref[:, units_at(i)]), mm(rows_in, up_ref[:, units_at(i)]))

        tiles(units // wide_units, unit_tile, hooks)

    def widen_part(i, h):
        model_at = pl.ds(pl.multiple_of(peer_y(h) * 2 * share, 2 * share), 2 * share)
        rows_in = piece_ref[far_rows, model_at]
        return mm(rows_in, gate_ref[model_at, units_at(i)]), mm(rows_in, up_ref[model_at, units_at(i)])

    def widen_far_begin():
        for i in range(units // wide_units):
            gate_part_ref[:, units_at(i)], up_part_ref[:, units_at(i)] = widen_part(i, 0)

    def widen_far_end(hooks):
        def unit_tile(i):
            gate_val, up_val = gate_part_ref[:, units_at(i)], up_part_ref[:, units_at(i)]
            for h in range(1, n_y):
                more = widen_part(i, h)
                gate_val, up_val = gate_val + more[0], up_val + more[1]
            activate(i, gate_val, up_val)

        tiles(units // wide_units, unit_tile, hooks)

    def narrow(b, hooks):
        at = slice(b * half_rows, (b + 1) * half_rows)
        if b == 0:
            pltpu.make_async_copy(down_hbm.at[0], down_ref, down_sem.at[0]).wait()

        def tile(h, ours):
            index = 2 * peer_y(h) + (core if ours else 1 - core)
            part_ref[at, columns(index)] = bf(mm(hidden_ref[...], down_ref[:, columns(index)]))

        for h in range(n_y - 1, 0, -1):
            tile(h, False)
            near_copy(b, h).start()
        for hook in hooks:
            hook()
        for h in range(n_y - 1, 0, -1):
            tile(h, True)
        tile(0, False)
        tile(0, True)
        near_copy(b, 0).start()

    for copy in loads[:6]:
        copy.start()
    everyone_here = meet()

    order = flag(iota((tokens, tokens), 0) < iota((tokens, tokens), 1))
    expert_rows = max(16, experts)
    loads[0].wait()
    loads[1].wait()
    own_routes = routes_ref[...]
    names = iota((expert_rows, tokens), 0)
    named = [own_routes[k : k + 1, :] == names for k in range(own_routes.shape[0])]
    match = functools.reduce(jnp.logical_or, named)
    rank = mm(bf(flag(match)), bf(order))
    rank = jnp.where(match, rank, -1.0)
    level = iota((capacity, tokens), 0).astype(jnp.float32)
    for j in range(experts):
        place_ref[j * capacity : (j + 1) * capacity] = bf(flag(level == rank[j : j + 1, :]))
    for copy in loads[2:6]:
        copy.wait()
    for copy in loads[6:]:
        copy.start()
    for i in range(units // wide_units):
        for copy in gate_copy(i):
            copy.start()
    for i in range(model // wide_model):
        down_copy(i).start()
    step_rows = 32
    for i in range(tokens // step_rows):
        at = slice(i * step_rows, (i + 1) * step_rows)
        xw = wide(x_ref[at])
        scale = lax.rsqrt(jnp.mean(xw * xw, axis=-1, keepdims=True) + norm_eps)
        normed_ref[at] = bf(xw * scale * norm_gain_ref[...])
    here = jnp.concatenate([place_ref[block(partner(d)), :] for d in range(1, half)], axis=0)
    near_out_ref[capacity:half_rows] = bf(mm(here, normed_ref[:, plane]))
    there = jnp.concatenate([place_ref[block(partner(d)), :] for d in range(half, n_ep)], axis=0)
    far_out_ref[...] = bf(mm(there, normed_ref[:, columns(t)]))
    per = max(1, n_ep // 8)

    def unit(u, body):
        lo = max(1, min(n_ep, u * per))
        return lambda: span(lo, max(lo, min(n_ep, (u + 1) * per)), body)

    inner = lax.rem(lax.div(z + 1, 2), 2)

    def far_unit(k, body):
        first = [4 + 2 * inner, 5 + 2 * inner, 6 - 2 * inner, 7 - 2 * inner][k] * per
        return lambda: span(first, first + per, body)

    everyone_here()
    span(1, half, lambda d: near_ep(d).start())
    for k in range(4):
        far_unit(k, lambda d: far_ep(d).start())()
    for i in range(model // wide_model):
        at = slice(i * wide_model, (i + 1) * wide_model)
        piece_ref[:capacity, at] = bf(mm(place_ref[block(e), :], normed_ref[:, at]))

    loads[15].wait()
    for h in range(1, n_y):
        w_plane(h).start()
    w_core(0).start()
    for copy in loads[6:14]:
        copy.wait()
    heads, pairs = extra_in_ref.shape[0], chain_ref.shape[0]
    exact = extra_in_ref[...]
    extra_parts_ref[...] = jnp.zeros(extra_parts_ref.shape, jnp.float32)
    for i in range(3):
        piece = wide(bf(exact))
        extra_parts_ref[i * heads : (i + 1) * heads, :] = piece
        exact = exact - piece
    extra_parts = bf(extra_parts_ref[...])
    extra_rows = extra_parts_ref.shape[0]
    for p in range(pairs):
        head = lax.rem(iota((extra_rows, PAIR), 0), heads)
        wanted = head == 2 * p + lax.div(iota((extra_rows, PAIR), 1), HEAD_DIM)
        extra_ref[:, p * PAIR : (p + 1) * PAIR] = mm_tn(extra_parts, bf(flag(wanted)))
    steps = positions // (group * HEAD_DIM)
    events = {}

    def pump(g, point):
        for step in range(steps):
            due = events.get(4 * step + point)
            if due:

                @pl.when(g == step)
                def _(due=due):
                    for act in due:
                        act()

    scan_kernel(
        group,
        pump,
        r_ref,
        k_ref,
        v_ref,
        d_ref,
        a_ref,
        d_off_ref,
        a_off_ref,
        extra_ref,
        out_ref,
        reach_ref,
        every_ref.at[e],
        chain_ref,
    )
    for i in sorted(events):
        for act in events[i] if i >= 4 * steps else ():
            act()
    pass_ends(z)
    span(1, half, near_arrived)
    far_unit(0, far_arrived)()
    far_unit(1, far_arrived)()
    near_core(near_rows).wait_recv()
    relays = [lambda i=i: relay_ends(i) for i in range(1, n_z)]
    widen_near({0: [share_w], 2: [far_unit(2, far_arrived)], 3: [far_unit(0, pass_on)]})
    far_unit(1, pass_on)()
    narrow(0, [far_unit(3, far_arrived)])
    far_unit(2, pass_on)()
    add_near(0)
    for copy in loads[14:15] + loads[16:]:
        copy.wait()

    normed = normed_ref[...]
    group_logit = mm_nt(group_router_ref[...], normed)
    group_exp = jnp.exp(group_logit)
    group_prob = group_exp / jnp.sum(group_exp, axis=0, keepdims=True)
    expert_logit = mm_nt(expert_router_ref[...], normed)
    per_group = experts // groups
    first_of = iota((groups, tokens), 0) * per_group
    expert_names = iota((experts, tokens), 0)
    chosen, prob = [], []
    for k in range(2):
        route = own_routes[k : k + 1, :]
        chosen.append(
            jnp.sum(jnp.where(route == expert_names, expert_logit, 0.0), axis=0, keepdims=True)
        )
        inside = (route >= first_of) & (route < first_of + per_group)
        prob.append(jnp.sum(jnp.where(inside, group_prob, 0.0), axis=0, keepdims=True))
    weights = [prob[0] * logistic(chosen[0] - chosen[1]), prob[1] * logistic(chosen[1] - chosen[0])]
    for k in range(2):
        weight_ref[k] = jnp.transpose(jnp.broadcast_to(weights[k], (128, tokens)))
        for j in range(experts):
            at = slice(j * capacity, (j + 1) * capacity)
            picks_ref[k, at] = place_ref[at] * bf(flag(own_routes[k : k + 1, :] == j))
    last = z == n_z - 1
    far_core(far_rows).wait_recv()
    widen_far_begin()
    for relay in relays[:1]:
        relay()
    with jax.named_scope("pass3"):
        far_unit(3, pass_on)()
    near_copy(0, 0).wait_recv()
    gathered()
    passing = [lambda i=i: relay_ends(i, ~last) for i in range(2, min(3, n_z))]
    widen_far_end({1: passing})
    late = [lambda i=i: relay_ends(i, last if i < 3 else True) for i in range(2, n_z)]
    narrow(1, late[:1] + [lambda: share_pair_w(~last)])
    add_near(1)
    for relay in late[1:]:
        relay()
    share_pair_w(last)
    span(1, half, go_home)
    near_copy(1, 0).wait_recv()
    unit(4, go_home)()
    for u in range(5, 8):
        unit(u, go_home)()
    home_ref[block(e), :] = add_far(0)
    span(0, n_z, collect_ends)
    planes = [peer_y(h) for h in range(1, n_y)] + [y]

    def joined(i):
        if i + 1 < n_y:
            mixed_copy(2 * planes[i] + core).start()
        mixed_copy(2 * planes[i] + 1 - core).start()

    join_kernel(
        "ep", every_ref, out_ref, reach_ref, gate_in_ref, gain_ref, mixed_ref, planes, joined
    )
    mixed_all_ref[t] = mixed_ref[pl.ds(pl.multiple_of(t * rows, rows), rows), :]
    share_line_w()
    all_mixed().wait_recv()
    for h in range(n_y):
        w_core(h).wait_recv()
    mixed = jnp.concatenate([mixed_all_ref[j] for j in range(n_tp)], axis=1)

    def project(i):
        at = pl.ds(pl.multiple_of(i * wide_model, wide_model), wide_model)
        mixer_ref[:, at] = bf(mm(mixed, w_ref[:, at]))

    for i in range(tile_count):
        project(i)

    near_src = near_out_ref.at[near_rows, :]
    remote(near_src, near_src, es.at[0], er.at[0], e, other).wait_send()
    remote(far_out_ref, far_out_ref, es.at[1], er.at[0], e, other).wait_send()
    near_core(near_rows).wait_send()
    far_core(far_rows).wait_send()
    remote(near_ref, near_ref, ns.at[0], nr.at[0, 0], e, other).wait_send()
    for h in range(1, n_y):
        ref = piece_ref.at[far_rows, columns(t)]
        remote(ref, ref, ys.at[h - 1], yr.at[h - 1, 0], e, other).wait_send()
        forward_copy(far_rows, h).wait_send()
        ref = stage_ref.at[h]
        remote(ref, ref, bs.at[h - 1], br.at[h - 1, 0], e, other).wait_send()
        w_plane(h).wait_send()
    for h in range(n_y):
        w_core(h).wait_send()
    w_rows(2 * n_x - 1).wait_send()
    all_mixed().wait_send()
    span(0, n_z, close_ends)
    all_home().wait_recv()
    back = home_ref[...]
    first, second = mm_tn(picks_ref[0], back), mm_tn(picks_ref[1], back)
    for i in range(share // 128):
        at = slice(i * 128, (i + 1) * 128)
        expert_ref[:, at] = bf(weight_ref[0] * first[:, at] + weight_ref[1] * second[:, at])
    all_home().wait_send()


def leave_kernel(mixer_ref, expert_ref, mixer_hbm, expert_hbm, sem):
    parts = 4
    rows = mixer_ref.shape[0] // parts
    copies = []
    for i in range(parts):
        at = slice(i * rows, (i + 1) * rows)
        copies.append(pltpu.make_async_copy(mixer_ref.at[at, :], mixer_hbm.at[at, :], sem.at[i]))
    copies.append(pltpu.make_async_copy(expert_ref, expert_hbm, sem.at[parts]))
    for copy in copies:
        copy.start()
    for copy in copies:
        copy.wait()


def leave(mixer_out, expert_out):
    return pl.pallas_call(
        leave_kernel,
        out_shape=(
            jax.ShapeDtypeStruct(mixer_out.shape, mixer_out.dtype),
            jax.ShapeDtypeStruct(expert_out.shape, expert_out.dtype),
        ),
        in_specs=[pl.BlockSpec(memory_space=pltpu.VMEM)] * 2,
        out_specs=[pl.BlockSpec(memory_space=pltpu.HBM)] * 2,
        scratch_shapes=[pltpu.SemaphoreType.DMA((5,))],
        compiler_params=pltpu.CompilerParams(vmem_limit_bytes=1 << 20),
    )(
        pltpu.with_memory_space_constraint(mixer_out, pltpu.VMEM),
        pltpu.with_memory_space_constraint(expert_out, pltpu.VMEM),
    )


def local(
    receptance,
    key_matrix,
    value_matrix,
    decay_data_term,
    correction_rate_data,
    output_gate_input,
    decay_channel_offset,
    correction_rate_offset,
    extra_head_log_decay,
    head_norm_gain,
    mixer_output_weight,
    expert_layer_input,
    feedforward_norm_gain,
    group_router_weight,
    expert_router_weight,
    routes,
    expert_gate_weight,
    expert_up_weight,
    expert_down_weight,
):
    positions, own_width = receptance.shape
    pairs = -(-own_width // PAIR)
    width = pairs * PAIR

    def filled(x, columns=width):
        return x if x.shape[-1] == columns else jnp.pad(x, ((0, 0), (0, columns - x.shape[-1])))

    blocks = positions // HEAD_DIM
    group = 4 if blocks % 4 == 0 else 1
    n_ep, n_tp = lax.axis_size("ep"), lax.axis_size("tp")
    n_y = n_tp // 2
    n_x = 1
    while 4 * n_x * n_x <= n_ep:
        n_x = 2 * n_x
    tokens, model = expert_layer_input.shape
    capacity, share = 4 * tokens // n_ep, model // n_tp
    slots = n_ep * capacity
    units = expert_gate_weight.shape[2]
    rows = positions // n_tp
    out_weight = jnp.pad(mixer_output_weight, ((0, width - own_width), (0, 0)))

    def held(*shape):
        return pltpu.VMEM(shape, jnp.bfloat16)

    def single(*shape):
        return pltpu.VMEM(shape, jnp.float32)

    def sems(*shape):
        return pltpu.SemaphoreType.DMA(shape)

    operands = (
        filled(receptance),
        filled(key_matrix),
        filled(value_matrix),
        filled(decay_data_term),
        filled(correction_rate_data),
        filled(output_gate_input),
        filled(decay_channel_offset[None]),
        filled(correction_rate_offset[None]),
        filled(extra_head_log_decay, 2 * pairs).T,
        filled(head_norm_gain[None]),
        out_weight,
        expert_layer_input,
        feedforward_norm_gain[None],
        group_router_weight.T,
        expert_router_weight.T,
        routes.T,
        expert_gate_weight,
        expert_up_weight,
        expert_down_weight,
    )
    in_vmem, in_hbm = pl.BlockSpec(memory_space=pltpu.VMEM), pl.BlockSpec(memory_space=pltpu.HBM)
    one, hops = sems(n_ep), sems(n_y - 1)
    mixer_out, expert_out = pl.pallas_call(
        functools.partial(whole_kernel, group),
        out_shape=(held(rows, model), held(tokens, share)),
        in_specs=[in_hbm] * 19,
        out_specs=[in_vmem] * 2,
        scratch_shapes=[held(positions, width)] * 6
        + [
            held(n_tp * width, model),
            held(tokens, model),
            single(1, width),
            single(1, width),
            single(2 * pairs, positions),
            single(1, width),
            single(1, model),
            held(*group_router_weight.shape[::-1]),
            held(*expert_router_weight.shape[::-1]),
            pltpu.VMEM(routes.shape[::-1], jnp.int32),
            single(16, positions),
            single(positions, width),
            held(tokens, model),
            held(slots, tokens),
            held(slots // 2, model // 2),
            held(slots // 2, share),
            held(2, slots, tokens),
            single(2, tokens, 128),
            held(slots, model),
            single(positions, width),
            held(positions, width),
            held(n_ep, pairs * 2 * HEAD_DIM, PAIR),
            single(pairs, 2 * PAIR, PAIR),
            held(positions, width),
            held(n_tp, rows, width),
            held(model, units),
            held(model, units),
            held(units, model),
            held(slots // 2, units),
            single(slots // 2, units),
            single(slots // 2, units),
            held(slots, model),
        ]
        + [held(n_y, slots, share)] * 3
        + [held(slots, share)] * 2
        + [sems(19)]
        + [sems(1)] * 3
        + [sems(2), one, sems(2), sems(2)]
        + [hops, sems(n_y - 1, n_ep // 2), hops, hops]
        + [sems(n_ep // n_x)] * 2
        + [sems(n_x - 1, n_ep // n_x)] * 2
        + [sems(1), sems(2, n_y)]
        + [hops, sems(n_y - 1, n_ep)]
        + [sems(1)] * 2
        + [hops, hops, sems(1), sems(1), hops, sems(n_y), sems(n_y), sems(1), sems(1)],
        compiler_params=pltpu.CompilerParams(
            collective_id=0, has_side_effects=True, vmem_limit_bytes=VMEM_LIMIT
        ),
    )(
        *(pltpu.with_memory_space_constraint(x, pltpu.HBM) for x in operands)
    )
    return leave(mixer_out, expert_out)


def solution(mesh):
    in_specs = (
        P("ep", "tp"),
        P("ep", "tp"),
        P("ep", "tp"),
        P("ep", "tp"),
        P("ep", "tp"),
        P("ep", "tp"),
        P("tp"),
        P("tp"),
        P("ep", "tp"),
        P("tp"),
        P("tp", None),
        P("ep", None),
        P(),
        P(),
        P(),
        P("ep", None),
        P("ep", None, "tp"),
        P("ep", None, "tp"),
        P("ep", "tp", None),
    )
    out_specs = (P(("ep", "tp"), None), P("ep", "tp"))
    return jax.shard_map(local, mesh=mesh, in_specs=in_specs, out_specs=out_specs, check_vma=False)
```

```python
import functools
import math

import jax
import jax.numpy as jnp
from jax import lax
from jax.experimental import pallas as pl
from jax.experimental.pallas import tpu as pltpu
from jax.sharding import PartitionSpec as P

HEAD_DIM = 64
PAIR = 2 * HEAD_DIM
VMEM_LIMIT = 48 << 20
HALF_EXP = math.exp(-0.5)
GROUPS = 4


key_eps = 1e-06
group_eps = 0.00064
norm_eps = 1e-06
highest = lax.Precision.HIGHEST


def bf(x):
    return x.astype(jnp.bfloat16)


def mm(x, y):
    return lax.dot_general(x, y, (((1,), (0,)), ((), ())), preferred_element_type=jnp.float32)


def mm_nt(x, y):
    return lax.dot_general(x, y, (((1,), (1,)), ((), ())), preferred_element_type=jnp.float32)


def mm_tn(x, y):
    return lax.dot_general(x, y, (((0,), (0,)), ((), ())), preferred_element_type=jnp.float32)


def halves(x):
    high = bf(x)
    return high, bf(x - high.astype(jnp.float32))


def sum_right(x, ones):
    high, low = halves(x)
    return mm(high, ones) + mm(low, ones)


def logistic(x):
    return 1.0 / (1.0 + jnp.exp(-x))


def flag(cond):
    return jnp.where(cond, 1.0, 0.0)


def iota(shape, dim):
    return lax.broadcasted_iota(jnp.int32, shape, dim)


def pair_blocks():
    return flag((iota((PAIR, PAIR), 0) < HEAD_DIM) == (iota((PAIR, PAIR), 1) < HEAD_DIM))


def scan_kernel(
    group,
    pump,
    r_ref,
    k_ref,
    v_ref,
    d_ref,
    a_ref,
    d_off_ref,
    a_off_ref,
    extra_ref,
    out_ref,
    reach_ref,
    ends_ref,
    chain_ref,
):
    positions, width = r_ref.shape
    pairs = width // PAIR
    C = HEAD_DIM
    rows_per = group * C
    own_block = pair_blocks()
    own_bf = bf(own_block)
    row, col = iota((C, PAIR), 0), iota((C, PAIR), 1) & (HEAD_DIM - 1)
    strict, upto = row > col, row >= col
    eye = flag(row == col)
    tri = bf(flag(iota((C, C), 0) >= iota((C, C), 1)))
    level_masks = []
    for s in range(6):
        inside = (
            ((row >> (s + 1)) == (col >> (s + 1)))
            & (((row >> s) & 1) == 1)
            & (((col >> s) & 1) == 0)
        )
        level_masks.append(bf(flag(inside)))

    def spread(x):
        return jnp.concatenate([x, x], axis=0) * own_bf

    square = (iota((PAIR, PAIR), 0) == iota((PAIR, PAIR), 1)).astype(jnp.float32)
    for p in range(pairs):
        chain_ref[p, :PAIR] = jnp.zeros((PAIR, PAIR), jnp.float32)
        chain_ref[p, PAIR:] = square

    def step(g, carry):
        base = pl.multiple_of(g * rows_per, rows_per)
        rows = pl.ds(base, rows_per)
        items = []
        for p in range(pairs):
            lanes = slice(p * PAIR, (p + 1) * PAIR)
            k = k_ref[rows, lanes].astype(jnp.float32)
            u = k * lax.rsqrt(sum_right(k * k, own_bf) + key_eps)
            rem = u * logistic(a_ref[rows, lanes].astype(jnp.float32) + a_off_ref[:, lanes])
            lg = extra_ref[rows, lanes] - HALF_EXP * logistic(
                d_ref[rows, lanes].astype(jnp.float32) + d_off_ref[:, lanes]
            )
            r = r_ref[rows, lanes].astype(jnp.float32)
            v = v_ref[rows, lanes]
            for c in range(group):
                cut = slice(c * C, (c + 1) * C)
                items.append((p, c, k[cut], u[cut], rem[cut], lg[cut], r[cut], v[cut]))
        stage = []
        for p, c, k, u, rem, lg, r, v in items:
            high, low = halves(lg)
            rest = bf(lg - high.astype(jnp.float32) - low.astype(jnp.float32))
            cumul = mm(tri, high) + mm(tri, low) + mm(tri, rest)
            stage.append(cumul)
        work = []
        for (p, c, k, u, rem, lg, r, v), cumul in zip(items, stage):
            mid = 0.5 * cumul[C - 1 : C]
            up_now, down = jnp.exp(cumul - mid), jnp.exp(mid - cumul)
            up_before = jnp.exp(cumul - lg - mid)
            half = jnp.exp(mid)
            cq, cu, dk, dr = r * up_now, u * up_before, k * down, rem * down
            left = bf(jnp.concatenate([cu, cq], axis=0))
            pair_r = mm_nt(left, spread(bf(dr)))
            pair_k = mm_nt(left, spread(bf(dk)))
            work.append((cq * half, bf(cu * half), bf(dk * half), bf(dr * half), half * half, pair_r, pair_k))
        pump(g, 0)
        solve = []
        for (p, c, k, u, rem, lg, r, v), (qe, ue, kt, rt, ed, pair_r, pair_k) in zip(items, work):
            rp = bf(jnp.where(strict, pair_r[:C], 0.0))
            rr = bf(jnp.where(upto, pair_r[C:], 0.0))
            kp = jnp.where(strict, pair_k[:C], 0.0)
            rk = jnp.where(upto, pair_k[C:], 0.0)
            kv = mm(bf(jnp.concatenate([kp, rk], axis=0)), spread(v))
            inv = eye - (rp * level_masks[0]).astype(jnp.float32)
            solve.append([rp, rr, kv, inv])
        for s in range(1, 6):
            mids = [bf(mm(bf(inv), spread(rp * level_masks[s]))) for rp, rr, kv, inv in solve]
            for item, y in zip(solve, mids):
                item[3] = item[3] - mm(y, spread(bf(item[3])))
            if s == 2:
                pump(g, 1)
        wvs = []
        for (rp, rr, kv, inv), w in zip(solve, work):
            wide = jnp.concatenate([spread(w[1]), spread(bf(kv[:C]))], axis=1)
            wvs.append(bf(mm(bf(inv), wide)))
        pump(g, 2)
        tails = []
        for (rp, rr, kv, inv), (qe, ue, kt, rt, ed, _, _), wv, item in zip(solve, work, wvs, items):
            wide = jnp.concatenate([spread(wv[:, :PAIR]), spread(wv[:, PAIR:])], axis=1)
            rw = mm(rr, wide)
            read = bf(qe - rw[:, :PAIR])
            local = kv[C:] - rw[:, PAIR:]
            v = item[7]
            x = jnp.concatenate(
                [jnp.concatenate([v, jnp.zeros_like(v)], axis=1),
                 jnp.concatenate([-wv[:, PAIR:], -wv[:, :PAIR]], axis=1)], axis=0)
            nb = mm_tn(x, jnp.concatenate([kt, rt], axis=0))
            tails.append((read, local, nb[:PAIR] * own_block, bf(nb[PAIR:] * own_block), ed))
        z = [chain_ref[p] for p in range(pairs)]
        for c in range(group):
            for p in range(pairs):
                read, local, add, neg, ed = tails[p * group + c]
                zb = bf(z[p])
                qz = mm_nt(read, zb)
                at = pl.ds(pl.multiple_of(base + c * C, C), C)
                lanes = slice(p * PAIR, (p + 1) * PAIR)
                out_ref[at, lanes] = local + qz[:, :PAIR]
                reach_ref[at, lanes] = bf(qz[:, PAIR:])
                moved = z[p] * ed + mm(zb, neg)
                z[p] = jnp.concatenate([moved[:PAIR] + add, moved[PAIR:]], axis=0)
        for p in range(pairs):
            chain_ref[p] = z[p]
        pump(g, 3)
        return carry

    lax.fori_loop(0, positions // rows_per, step, 0)
    for p in range(pairs):
        s, m = chain_ref[p, :PAIR], chain_ref[p, PAIR:]
        ends_ref[p * 2 * C : p * 2 * C + C] = bf(s[:C] + s[C:])
        ends_ref[p * 2 * C + C : (p + 1) * 2 * C] = bf(m[:C] + m[C:])


def join_kernel(axis, all_ref, out_ref, reach_ref, gate_ref, gain_ref, mixed_ref, planes, done):
    devices, place = lax.axis_size(axis), lax.axis_index(axis)
    width = out_ref.shape[1]
    pairs = width // PAIR
    C = HEAD_DIM
    own_block = pair_blocks()
    own_bf = bf(own_block)
    mean_bf = bf(own_block * (1.0 / HEAD_DIM))
    states = [jnp.zeros((C, PAIR), jnp.float32) for _ in range(pairs)]

    def hop(j, states):
        new = []
        for p in range(pairs):
            s = all_ref[j, p * 2 * C : p * 2 * C + C].astype(jnp.float32)
            m = all_ref[j, p * 2 * C + C : (p + 1) * 2 * C]
            m = jnp.concatenate([m, m], axis=0) * own_bf
            new.append(sum_right(states[p], m) + s)
        return tuple(new)

    states = lax.fori_loop(0, place, hop, tuple(states))
    rows = out_ref.shape[0] // len(planes)
    moves = []
    for p in range(pairs):
        s = bf(states[p])
        moves.append(jnp.concatenate([s, s], axis=0) * own_bf)
    for i, plane in enumerate(planes):
        at = pl.ds(pl.multiple_of(plane * rows, rows), rows)
        for p in range(pairs):
            lanes = slice(p * PAIR, (p + 1) * PAIR)
            head = out_ref[at, lanes] + mm_nt(reach_ref[at, lanes], moves[p])
            centred = head - sum_right(head, mean_bf)
            spread = sum_right(centred * centred, mean_bf)
            normed = centred * lax.rsqrt(spread + group_eps)
            gate = logistic(gate_ref[at, lanes].astype(jnp.float32))
            mixed_ref[at, lanes] = bf(normed * gain_ref[:, lanes] * gate)
        done(i)


def place_of():
    n_ep, n_tp = lax.axis_size("ep"), lax.axis_size("tp")
    e, t = lax.axis_index("ep"), lax.axis_index("tp")
    core = lax.rem(t, 2)
    return n_ep, n_tp, n_tp // 2, e, t, lax.div(t, 2), core


def remote(src, dst, send, recv, e, t):
    return pltpu.make_async_remote_copy(
        src_ref=src,
        dst_ref=dst,
        send_sem=send,
        recv_sem=recv,
        device_id=(e, t),
        device_id_type=pl.DeviceIdType.MESH,
    )


def meet():
    n_ep, n_tp, n_y, e, t, y, core = place_of()
    barrier = pltpu.get_barrier_semaphore()

    def greet(pe, pt):
        pl.semaphore_signal(
            barrier, inc=1, device_id=(pe, pt), device_id_type=pl.DeviceIdType.MESH
        )

    for d in range(1, n_ep):
        greet(lax.rem(e + d, n_ep), t)
    greet(e, 2 * y + 1 - core)
    for d in range(1, n_y):
        greet(e, 2 * lax.rem(y + d, n_y) + core)
        greet(e, 2 * lax.rem(y + d, n_y) + 1 - core)
    return lambda: pl.semaphore_wait(barrier, n_ep - 2 + 2 * n_y)


def span(first, last, body):
    def run(d, carry):
        body(d)
        return carry

    lax.fori_loop(first, last, run, 0)


def wide(x):
    return x.astype(jnp.float32)


def whole_kernel(
    group,
    r_hbm,
    k_hbm,
    v_hbm,
    d_hbm,
    a_hbm,
    gate_in_hbm,
    d_off_hbm,
    a_off_hbm,
    extra_hbm,
    gain_hbm,
    out_weight_hbm,
    x_hbm,
    norm_gain_hbm,
    group_router_hbm,
    expert_router_hbm,
    routes_hbm,
    gate_hbm,
    up_hbm,
    down_hbm,
    mixer_ref,
    expert_ref,
    r_ref,
    k_ref,
    v_ref,
    d_ref,
    a_ref,
    gate_in_ref,
    w_ref,
    x_ref,
    d_off_ref,
    a_off_ref,
    extra_in_ref,
    gain_ref,
    norm_gain_ref,
    group_router_ref,
    expert_router_ref,
    routes_ref,
    extra_parts_ref,
    extra_ref,
    normed_ref,
    place_ref,
    near_out_ref,
    far_out_ref,
    picks_ref,
    weight_ref,
    piece_ref,
    out_ref,
    reach_ref,
    every_ref,
    chain_ref,
    mixed_ref,
    mixed_all_ref,
    product_ref,
    gate_ref,
    up_ref,
    down_ref,
    hidden_ref,
    gate_part_ref,
    up_part_ref,
    part_ref,
    near_ref,
    stage_ref,
    far_ref,
    final_ref,
    home_ref,
    in_sem,
    gate_sem,
    up_sem,
    down_sem,
    es,
    er,
    cs,
    cr,
    ys,
    yr,
    fs,
    fr,
    zs,
    zr,
    gs,
    gr,
    ns,
    nr,
    bs,
    br,
    hs,
    hr,
    wys,
    wyr,
    wgs,
    wgr,
    wzr,
    wcs,
    wcr,
    xs,
    xr,
):
    n_ep, n_tp, n_y, e, t, y, core = place_of()
    units = gate_ref.shape[1]
    model = x_ref.shape[1]
    tokens = x_ref.shape[0]
    share = model // n_tp
    slots = piece_ref.shape[0]
    capacity = slots // n_ep
    experts = expert_router_ref.shape[0]
    groups = group_router_ref.shape[0]
    positions, width = mixed_ref.shape
    rows = positions // n_tp
    other = 2 * y + 1 - core
    half = n_ep // 2
    half_rows = half * capacity
    wide_units, wide_model = min(256, units), min(512, model)

    def shard(index):
        return pl.ds(pl.multiple_of(index * width, width), width)

    x_rows = [slice(i * tokens // 4, (i + 1) * tokens // 4) for i in range(4)]
    inputs = [(routes_hbm, routes_ref), (norm_gain_hbm, norm_gain_ref)]
    inputs += [(x_hbm.at[at, :], x_ref.at[at, :]) for at in x_rows]
    inputs += [(extra_hbm, extra_in_ref), (d_off_hbm, d_off_ref), (a_off_hbm, a_off_ref)]
    inputs += [(k_hbm, k_ref), (a_hbm, a_ref), (d_hbm, d_ref), (r_hbm, r_ref), (v_hbm, v_ref)]
    inputs += [(gate_in_hbm, gate_in_ref), (out_weight_hbm, w_ref.at[shard(t), :]), (gain_hbm, gain_ref)]
    inputs += [(group_router_hbm, group_router_ref), (expert_router_hbm, expert_router_ref)]
    loads = [pltpu.make_async_copy(s, d, in_sem.at[i]) for i, (s, d) in enumerate(inputs)]

    def gate_copy(i):
        at = pl.ds(pl.multiple_of(i * wide_units, wide_units), wide_units)
        return (
            pltpu.make_async_copy(gate_hbm.at[0, :, at], gate_ref.at[:, at], gate_sem.at[0]),
            pltpu.make_async_copy(up_hbm.at[0, :, at], up_ref.at[:, at], up_sem.at[0]),
        )

    def down_copy(i):
        at = pl.ds(pl.multiple_of(i * wide_model, wide_model), wide_model)
        return pltpu.make_async_copy(down_hbm.at[0, :, at], down_ref.at[:, at], down_sem.at[0])

    def partner(d):
        bit, total = 1, 0
        while bit < n_ep:
            total = total + lax.rem(lax.div(e, bit) + lax.div(d, bit), 2) * bit
            bit = 2 * bit
        return total

    def columns(index):
        return pl.ds(pl.multiple_of(index * share, share), share)

    def block(d):
        return pl.ds(pl.multiple_of(d * capacity, capacity), capacity)

    def peer_y(h):
        return lax.rem(y + h, n_y)

    plane = pl.ds(pl.multiple_of(core * (model // 2), model // 2), model // 2)

    def near_ep(d):
        dst = piece_ref.at[block(d), plane]
        return remote(near_out_ref.at[block(d), :], dst, es.at[0], er.at[d], partner(d), t)

    def far_ep(d):
        src = far_out_ref.at[block(d - half), :]
        return remote(src, piece_ref.at[block(d), columns(t)], es.at[1], er.at[d], partner(d), t)

    near_rows, far_rows = slice(capacity, half_rows), slice(half_rows, slots)

    def near_core(at):
        ref = piece_ref.at[at, plane]
        return remote(ref, ref, cs.at[0], cr.at[0], e, other)

    def far_core(at):
        ref = piece_ref.at[at, columns(t)]
        return remote(ref, ref, cs.at[1], cr.at[1], e, other)

    def y_copy(d, h):
        ref = piece_ref.at[block(d), columns(t)]
        peer = 2 * peer_y(h) + core
        return remote(ref, ref, ys.at[h - 1], yr.at[h - 1, d - half], e, peer)

    def forward_copy(at, h):
        ref = piece_ref.at[at, columns(2 * lax.rem(y - h + n_y, n_y) + core)]
        return remote(ref, ref, fs.at[h - 1], fr.at[h - 1], e, other)

    def near_arrived(d):
        near_ep(d).wait_recv()
        near_core(block(d)).start()

    def far_arrived(d):
        far_ep(d).wait_recv()
        for h in range(1, n_y):
            y_copy(d, h).start()
        far_core(block(d)).start()

    def pass_on(d):
        for h in range(1, n_y):
            y_copy(d, h).wait_recv()
            forward_copy(block(d), h).start()

    def gathered():
        for h in range(1, n_y):
            forward_copy(far_rows, h).wait_recv()

    n_x = gs.shape[0] + 1
    n_z = n_ep // n_x
    z, x = lax.div(e, n_x), lax.rem(e, n_x)

    def up_copy(zz):
        ref = every_ref.at[zz * n_x + x]
        return remote(ref, ref, zs.at[zz], zr.at[zz], e + n_x, t)

    def side_copy(zz, h):
        ref = every_ref.at[zz * n_x + x]
        peer = z * n_x + lax.rem(x + h, n_x)
        return remote(ref, ref, gs.at[h - 1, zz], gr.at[h - 1, zz], peer, t)

    def pass_ends(zz):
        @pl.when(z + 1 < n_z)
        def _():
            up_copy(zz).start()

        for h in range(1, n_x):
            side_copy(zz, h).start()

    def relay_ends(i, wanted=True):
        @pl.when((z >= i) & wanted)
        def _():
            up_copy(z - i).wait_recv()
            pass_ends(z - i)

    def collect_ends(zz):
        @pl.when(z >= zz)
        def _():
            for h in range(1, n_x):
                side_copy(zz, h).wait_recv()

    def close_ends(zz):
        @pl.when(z >= zz)
        def _():
            @pl.when(z + 1 < n_z)
            def _():
                up_copy(zz).wait_send()

            for h in range(1, n_x):
                side_copy(zz, h).wait_send()

    def near_copy(b, h):
        at = pl.ds(b * half_rows, half_rows)
        src = part_ref.at[at, columns(2 * peer_y(h) + 1 - core)]
        return remote(src, near_ref.at[h, at, :], ns.at[0], nr.at[b, h], e, other)

    half_block = capacity // 2

    def sub(i):
        return pl.ds(pl.multiple_of(i * half_block, half_block), half_block)

    def back_copy(i, h):
        src = stage_ref.at[h, sub(i), :]
        dst = far_ref.at[h, sub(i), :]
        return remote(src, dst, bs.at[h - 1], br.at[h - 1, i], e, 2 * peer_y(h) + core)

    def home_copy(i):
        d, s = lax.div(i, 2), lax.rem(i, 2)
        src, dst = final_ref.at[sub(i), :], home_ref.at[sub(2 * e + s), :]
        return remote(src, dst, hs.at[0], hr.at[0], partner(d), t)

    def all_home():
        src, dst = final_ref.at[capacity:, :], home_ref.at[capacity:, :]
        return remote(src, dst, hs.at[0], hr.at[0], partner(1), t)

    def pair_sum(i, h):
        return wide(part_ref[sub(i), columns(2 * peer_y(h) + core)]) + wide(near_ref[h, sub(i), :])

    def add_near(b):
        for h in range(1, n_y):
            near_copy(b, h).wait_recv()

        def one(i):
            for h in range(1, n_y):
                stage_ref[h, sub(i), :] = bf(pair_sum(i, h))
                back_copy(i, h).start()

        span(2 * b * half, 2 * (b + 1) * half, one)

    def add_far(i):
        total = pair_sum(i, 0)
        for h in range(1, n_y):
            back_copy(i, h).wait_recv()
            total = total + wide(far_ref[h, sub(i), :])
        return bf(total)

    def go_home(d):
        def one(i):
            final_ref[sub(i), :] = add_far(i)
            home_copy(i).start()

        span(2 * d, 2 * d + 2, one)

    tile_count = model // wide_model
    part_rows = width // (2 * n_x)

    def source_of(h):
        return 2 * lax.rem(y - h + n_y, n_y) + core

    def part(index, place):
        return pl.ds(pl.multiple_of(index * width + place * part_rows, part_rows), part_rows)

    own_part = lax.rem(e, 2 * n_x)
    pair_part = lax.rem(own_part + n_x, 2 * n_x)

    def w_plane(h):
        ref = w_ref.at[part(t, own_part), :]
        return remote(ref, ref, wys.at[h - 1], wyr.at[h - 1], e, 2 * peer_y(h) + core)

    def w_pair(h):
        ref = w_ref.at[part(source_of(h), own_part), :]
        return remote(ref, ref, wgs.at[0], wzr.at[h - 1], partner(n_x), t)

    def w_line(h, place, k):
        ref = w_ref.at[part(source_of(h), place), :]
        return remote(ref, ref, wgs.at[0], wgr.at[0], partner(k), t)

    def w_rows(count):
        ref = w_ref.at[: (n_y - 1) * count * part_rows, :]
        return remote(ref, ref, wgs.at[0], wgr.at[0], partner(1), t)

    def w_core(h):
        ref = w_ref.at[shard(source_of(h)), :]
        return remote(ref, ref, wcs.at[h], wcr.at[h], e, other)

    def w_core_part(h, place):
        ref = w_ref.at[part(source_of(h), place), :]
        return remote(ref, ref, wcs.at[h], wcr.at[h], e, other)

    def share_w():
        for h in range(1, n_y):
            w_plane(h).wait_recv()
            w_pair(h).start()
            span(1, n_x, lambda k: w_line(h, own_part, k).start())
            w_core_part(h, own_part).start()

    def share_pair_w(wanted):
        @pl.when(wanted)
        def _():
            for h in range(1, n_y):
                w_pair(h).wait_recv()
                span(1, n_x, lambda k: w_line(h, pair_part, k).start())
                w_core_part(h, pair_part).start()

    def share_line_w():
        w_rows(2 * n_x - 2).wait_recv()
        for h in range(1, n_y):
            for shift in (0, n_x):

                def one(k):
                    place = lax.rem(partner(k) + shift, 2 * n_x)
                    w_core_part(h, place).start()

                span(1, n_x, one)

    def mixed_copy(to):
        src = mixed_ref.at[pl.ds(pl.multiple_of(to * rows, rows), rows), :]
        return remote(src, mixed_all_ref.at[t], xs.at[0], xr.at[0], e, to)

    def mixed_core():
        src = mixed_ref.at[pl.ds(pl.multiple_of(other * rows, rows), rows), :]
        return remote(src, mixed_all_ref.at[t], xs.at[1], xr.at[1], e, other)

    def mixed_planes():
        ref = mixed_all_ref.at[: n_tp - 2]
        return remote(ref, ref, xs.at[0], xr.at[0], e, other)

    def plane_product(plane, at):
        held_rows = pl.ds(pl.multiple_of(plane * 2 * width, 2 * width), 2 * width)
        left = jnp.concatenate([mixed_all_ref[2 * plane], mixed_all_ref[2 * plane + 1]], axis=1)
        return mm(left, w_ref[held_rows, at])

    def tiles(count, body, hooks):
        for i in range(count):
            body(i)
            for hook in hooks.get(i, ()):
                hook()
        for i in sorted(hooks):
            for hook in hooks[i] if i >= count else ():
                hook()

    def units_at(i):
        return slice(i * wide_units, (i + 1) * wide_units)

    def activate(i, gate_val, up_val):
        hidden_ref[:, units_at(i)] = bf(gate_val * logistic(gate_val) * up_val)

    def widen_near(hooks):
        pltpu.make_async_copy(gate_hbm.at[0], gate_ref, gate_sem.at[0]).wait()
        pltpu.make_async_copy(up_hbm.at[0], up_ref, up_sem.at[0]).wait()

        def unit_tile(i):
            rows_in = piece_ref[:half_rows, :]
            activate(i, mm(rows_in, gate_ref[:, units_at(i)]), mm(rows_in, up_ref[:, units_at(i)]))

        tiles(units // wide_units, unit_tile, hooks)

    def widen_part(i, h):
        model_at = pl.ds(pl.multiple_of(peer_y(h) * 2 * share, 2 * share), 2 * share)
        rows_in = piece_ref[far_rows, model_at]
        return mm(rows_in, gate_ref[model_at, units_at(i)]), mm(rows_in, up_ref[model_at, units_at(i)])

    def widen_far_begin():
        for i in range(units // wide_units):
            gate_part_ref[:, units_at(i)], up_part_ref[:, units_at(i)] = widen_part(i, 0)

    def widen_far_end(hooks):
        def unit_tile(i):
            gate_val, up_val = gate_part_ref[:, units_at(i)], up_part_ref[:, units_at(i)]
            for h in range(1, n_y):
                more = widen_part(i, h)
                gate_val, up_val = gate_val + more[0], up_val + more[1]
            activate(i, gate_val, up_val)

        tiles(units // wide_units, unit_tile, hooks)

    def narrow(b, hooks):
        at = slice(b * half_rows, (b + 1) * half_rows)
        if b == 0:
            pltpu.make_async_copy(down_hbm.at[0], down_ref, down_sem.at[0]).wait()

        def tile(h, ours):
            index = 2 * peer_y(h) + (core if ours else 1 - core)
            part_ref[at, columns(index)] = bf(mm(hidden_ref[...], down_ref[:, columns(index)]))

        for h in range(n_y - 1, 0, -1):
            tile(h, False)
            near_copy(b, h).start()
        for hook in hooks:
            hook()
        for h in range(n_y - 1, 0, -1):
            tile(h, True)
        tile(0, False)
        tile(0, True)
        near_copy(b, 0).start()

    for copy in loads[:6]:
        copy.start()
    everyone_here = meet()

    order = flag(iota((tokens, tokens), 0) < iota((tokens, tokens), 1))
    expert_rows = max(16, experts)
    loads[0].wait()
    loads[1].wait()
    own_routes = routes_ref[...]
    names = iota((expert_rows, tokens), 0)
    named = [own_routes[k : k + 1, :] == names for k in range(own_routes.shape[0])]
    match = functools.reduce(jnp.logical_or, named)
    rank = mm(bf(flag(match)), bf(order))
    rank = jnp.where(match, rank, -1.0)
    level = iota((capacity, tokens), 0).astype(jnp.float32)
    for j in range(experts):
        place_ref[j * capacity : (j + 1) * capacity] = bf(flag(level == rank[j : j + 1, :]))
    for copy in loads[2:6]:
        copy.wait()
    for copy in loads[6:]:
        copy.start()
    for i in range(units // wide_units):
        for copy in gate_copy(i):
            copy.start()
    for i in range(model // wide_model):
        down_copy(i).start()
    step_rows = 32
    for i in range(tokens // step_rows):
        at = slice(i * step_rows, (i + 1) * step_rows)
        xw = wide(x_ref[at])
        scale = lax.rsqrt(jnp.mean(xw * xw, axis=-1, keepdims=True) + norm_eps)
        normed_ref[at] = bf(xw * scale * norm_gain_ref[...])
    here = jnp.concatenate([place_ref[block(partner(d)), :] for d in range(1, half)], axis=0)
    near_out_ref[capacity:half_rows] = bf(mm(here, normed_ref[:, plane]))
    there = jnp.concatenate([place_ref[block(partner(d)), :] for d in range(half, n_ep)], axis=0)
    far_out_ref[...] = bf(mm(there, normed_ref[:, columns(t)]))
    per = max(1, n_ep // 8)

    def unit(u, body):
        lo = max(1, min(n_ep, u * per))
        return lambda: span(lo, max(lo, min(n_ep, (u + 1) * per)), body)

    inner = lax.rem(lax.div(z + 1, 2), 2)

    def far_unit(k, body):
        first = [4 + 2 * inner, 5 + 2 * inner, 6 - 2 * inner, 7 - 2 * inner][k] * per
        return lambda: span(first, first + per, body)

    everyone_here()
    span(1, half, lambda d: near_ep(d).start())
    for k in range(4):
        far_unit(k, lambda d: far_ep(d).start())()
    for i in range(model // wide_model):
        at = slice(i * wide_model, (i + 1) * wide_model)
        piece_ref[:capacity, at] = bf(mm(place_ref[block(e), :], normed_ref[:, at]))

    loads[15].wait()
    for h in range(1, n_y):
        w_plane(h).start()
    w_core(0).start()
    for copy in loads[6:14]:
        copy.wait()
    heads, pairs = extra_in_ref.shape[0], chain_ref.shape[0]
    exact = extra_in_ref[...]
    extra_parts_ref[...] = jnp.zeros(extra_parts_ref.shape, jnp.float32)
    for i in range(3):
        piece = wide(bf(exact))
        extra_parts_ref[i * heads : (i + 1) * heads, :] = piece
        exact = exact - piece
    extra_parts = bf(extra_parts_ref[...])
    extra_rows = extra_parts_ref.shape[0]
    for p in range(pairs):
        head = lax.rem(iota((extra_rows, PAIR), 0), heads)
        wanted = head == 2 * p + lax.div(iota((extra_rows, PAIR), 1), HEAD_DIM)
        extra_ref[:, p * PAIR : (p + 1) * PAIR] = mm_tn(extra_parts, bf(flag(wanted)))
    steps = positions // (group * HEAD_DIM)
    events = {}

    def pump(g, point):
        for step in range(steps):
            due = events.get(4 * step + point)
            if due:

                @pl.when(g == step)
                def _(due=due):
                    for act in due:
                        act()

    scan_kernel(
        group,
        pump,
        r_ref,
        k_ref,
        v_ref,
        d_ref,
        a_ref,
        d_off_ref,
        a_off_ref,
        extra_ref,
        out_ref,
        reach_ref,
        every_ref.at[e],
        chain_ref,
    )
    for i in sorted(events):
        for act in events[i] if i >= 4 * steps else ():
            act()
    pass_ends(z)
    span(1, half, near_arrived)
    far_unit(0, far_arrived)()
    far_unit(1, far_arrived)()
    near_core(near_rows).wait_recv()
    relays = [lambda i=i: relay_ends(i) for i in range(1, n_z)]
    widen_near({0: [share_w], 2: [far_unit(2, far_arrived)], 3: [far_unit(0, pass_on)]})
    far_unit(1, pass_on)()
    narrow(0, [far_unit(3, far_arrived)])
    far_unit(2, pass_on)()
    add_near(0)
    for copy in loads[14:15] + loads[16:]:
        copy.wait()

    normed = normed_ref[...]
    group_logit = mm_nt(group_router_ref[...], normed)
    group_exp = jnp.exp(group_logit)
    group_prob = group_exp / jnp.sum(group_exp, axis=0, keepdims=True)
    expert_logit = mm_nt(expert_router_ref[...], normed)
    per_group = experts // groups
    first_of = iota((groups, tokens), 0) * per_group
    expert_names = iota((experts, tokens), 0)
    chosen, prob = [], []
    for k in range(2):
        route = own_routes[k : k + 1, :]
        chosen.append(
            jnp.sum(jnp.where(route == expert_names, expert_logit, 0.0), axis=0, keepdims=True)
        )
        inside = (route >= first_of) & (route < first_of + per_group)
        prob.append(jnp.sum(jnp.where(inside, group_prob, 0.0), axis=0, keepdims=True))
    weights = [prob[0] * logistic(chosen[0] - chosen[1]), prob[1] * logistic(chosen[1] - chosen[0])]
    for k in range(2):
        weight_ref[k] = jnp.transpose(jnp.broadcast_to(weights[k], (128, tokens)))
        for j in range(experts):
            at = slice(j * capacity, (j + 1) * capacity)
            picks_ref[k, at] = place_ref[at] * bf(flag(own_routes[k : k + 1, :] == j))
    last = z == n_z - 1
    far_core(far_rows).wait_recv()
    widen_far_begin()
    for relay in relays[:1]:
        relay()
    with jax.named_scope("pass3"):
        far_unit(3, pass_on)()
    near_copy(0, 0).wait_recv()
    gathered()
    passing = [lambda i=i: relay_ends(i, ~last) for i in range(2, min(3, n_z))]
    widen_far_end({1: passing})
    late = [lambda i=i: relay_ends(i, last if i < 3 else True) for i in range(2, n_z)]
    narrow(1, late[:1] + [lambda: share_pair_w(~last)])
    add_near(1)
    for relay in late[1:]:
        relay()
    share_pair_w(last)
    span(1, half, go_home)
    near_copy(1, 0).wait_recv()
    unit(4, go_home)()
    for u in range(5, 8):
        unit(u, go_home)()
    for i in range(2):
        home_ref[sub(2 * e + i), :] = add_far(i)
    span(0, n_z, collect_ends)
    planes = [peer_y(h) for h in range(1, n_y)] + [y]

    def joined(i):
        if i + 1 < n_y:
            mixed_copy(2 * planes[i] + core).start()
            mixed_copy(2 * planes[i] + 1 - core).start()
        else:
            mixed_core().start()

    join_kernel(
        "ep", every_ref, out_ref, reach_ref, gate_in_ref, gain_ref, mixed_ref, planes, joined
    )
    mixed_all_ref[t] = mixed_ref[pl.ds(pl.multiple_of(t * rows, rows), rows), :]
    tile_slices = [slice(i * wide_model, (i + 1) * wide_model) for i in range(tile_count)]
    w_core(0).wait_recv()
    mixed_core().wait_recv()
    for at in tile_slices:
        product_ref[:, at] = plane_product(y, at)
    share_line_w()
    mixed_planes().wait_recv()
    for h in range(1, n_y):
        w_core(h).wait_recv()
    for at in tile_slices:
        total = product_ref[:, at]
        for h in range(1, n_y):
            total = total + plane_product(peer_y(h), at)
        mixer_ref[:, at] = bf(total)

    near_src = near_out_ref.at[near_rows, :]
    remote(near_src, near_src, es.at[0], er.at[0], e, other).wait_send()
    remote(far_out_ref, far_out_ref, es.at[1], er.at[0], e, other).wait_send()
    near_core(near_rows).wait_send()
    far_core(far_rows).wait_send()
    remote(near_ref, near_ref, ns.at[0], nr.at[0, 0], e, other).wait_send()
    for h in range(1, n_y):
        ref = piece_ref.at[far_rows, columns(t)]
        remote(ref, ref, ys.at[h - 1], yr.at[h - 1, 0], e, other).wait_send()
        forward_copy(far_rows, h).wait_send()
        ref = stage_ref.at[h]
        remote(ref, ref, bs.at[h - 1], br.at[h - 1, 0], e, other).wait_send()
        w_plane(h).wait_send()
    for h in range(n_y):
        w_core(h).wait_send()
    w_rows(2 * n_x - 1).wait_send()
    mixed_planes().wait_send()
    mixed_core().wait_send()
    span(0, n_z, close_ends)
    all_home().wait_recv()
    back = home_ref[...]
    first, second = mm_tn(picks_ref[0], back), mm_tn(picks_ref[1], back)
    for i in range(share // 128):
        at = slice(i * 128, (i + 1) * 128)
        expert_ref[:, at] = bf(weight_ref[0] * first[:, at] + weight_ref[1] * second[:, at])
    all_home().wait_send()


def leave_kernel(mixer_ref, expert_ref, mixer_hbm, expert_hbm, sem):
    parts = 4
    rows = mixer_ref.shape[0] // parts
    copies = []
    for i in range(parts):
        at = slice(i * rows, (i + 1) * rows)
        copies.append(pltpu.make_async_copy(mixer_ref.at[at, :], mixer_hbm.at[at, :], sem.at[i]))
    copies.append(pltpu.make_async_copy(expert_ref, expert_hbm, sem.at[parts]))
    for copy in copies:
        copy.start()
    for copy in copies:
        copy.wait()


def leave(mixer_out, expert_out):
    return pl.pallas_call(
        leave_kernel,
        out_shape=(
            jax.ShapeDtypeStruct(mixer_out.shape, mixer_out.dtype),
            jax.ShapeDtypeStruct(expert_out.shape, expert_out.dtype),
        ),
        in_specs=[pl.BlockSpec(memory_space=pltpu.VMEM)] * 2,
        out_specs=[pl.BlockSpec(memory_space=pltpu.HBM)] * 2,
        scratch_shapes=[pltpu.SemaphoreType.DMA((5,))],
        compiler_params=pltpu.CompilerParams(vmem_limit_bytes=1 << 20),
    )(
        pltpu.with_memory_space_constraint(mixer_out, pltpu.VMEM),
        pltpu.with_memory_space_constraint(expert_out, pltpu.VMEM),
    )


def local(
    receptance,
    key_matrix,
    value_matrix,
    decay_data_term,
    correction_rate_data,
    output_gate_input,
    decay_channel_offset,
    correction_rate_offset,
    extra_head_log_decay,
    head_norm_gain,
    mixer_output_weight,
    expert_layer_input,
    feedforward_norm_gain,
    group_router_weight,
    expert_router_weight,
    routes,
    expert_gate_weight,
    expert_up_weight,
    expert_down_weight,
):
    positions, own_width = receptance.shape
    pairs = -(-own_width // PAIR)
    width = pairs * PAIR

    def filled(x, columns=width):
        return x if x.shape[-1] == columns else jnp.pad(x, ((0, 0), (0, columns - x.shape[-1])))

    blocks = positions // HEAD_DIM
    group = 4 if blocks % 4 == 0 else 1
    n_ep, n_tp = lax.axis_size("ep"), lax.axis_size("tp")
    n_y = n_tp // 2
    n_x = 1
    while 4 * n_x * n_x <= n_ep:
        n_x = 2 * n_x
    tokens, model = expert_layer_input.shape
    capacity, share = 4 * tokens // n_ep, model // n_tp
    slots = n_ep * capacity
    units = expert_gate_weight.shape[2]
    rows = positions // n_tp
    out_weight = jnp.pad(mixer_output_weight, ((0, width - own_width), (0, 0)))

    def held(*shape):
        return pltpu.VMEM(shape, jnp.bfloat16)

    def single(*shape):
        return pltpu.VMEM(shape, jnp.float32)

    def sems(*shape):
        return pltpu.SemaphoreType.DMA(shape)

    operands = (
        filled(receptance),
        filled(key_matrix),
        filled(value_matrix),
        filled(decay_data_term),
        filled(correction_rate_data),
        filled(output_gate_input),
        filled(decay_channel_offset[None]),
        filled(correction_rate_offset[None]),
        filled(extra_head_log_decay, 2 * pairs).T,
        filled(head_norm_gain[None]),
        out_weight,
        expert_layer_input,
        feedforward_norm_gain[None],
        group_router_weight.T,
        expert_router_weight.T,
        routes.T,
        expert_gate_weight,
        expert_up_weight,
        expert_down_weight,
    )
    in_vmem, in_hbm = pl.BlockSpec(memory_space=pltpu.VMEM), pl.BlockSpec(memory_space=pltpu.HBM)
    one, hops = sems(n_ep), sems(n_y - 1)
    mixer_out, expert_out = pl.pallas_call(
        functools.partial(whole_kernel, group),
        out_shape=(held(rows, model), held(tokens, share)),
        in_specs=[in_hbm] * 19,
        out_specs=[in_vmem] * 2,
        scratch_shapes=[held(positions, width)] * 6
        + [
            held(n_tp * width, model),
            held(tokens, model),
            single(1, width),
            single(1, width),
            single(2 * pairs, positions),
            single(1, width),
            single(1, model),
            held(*group_router_weight.shape[::-1]),
            held(*expert_router_weight.shape[::-1]),
            pltpu.VMEM(routes.shape[::-1], jnp.int32),
            single(16, positions),
            single(positions, width),
            held(tokens, model),
            held(slots, tokens),
            held(slots // 2, model // 2),
            held(slots // 2, share),
            held(2, slots, tokens),
            single(2, tokens, 128),
            held(slots, model),
            single(positions, width),
            held(positions, width),
            held(n_ep, pairs * 2 * HEAD_DIM, PAIR),
            single(pairs, 2 * PAIR, PAIR),
            held(positions, width),
            held(n_tp, rows, width),
            single(rows, model),
            held(model, units),
            held(model, units),
            held(units, model),
            held(slots // 2, units),
            single(slots // 2, units),
            single(slots // 2, units),
            held(slots, model),
        ]
        + [held(n_y, slots, share)] * 3
        + [held(slots, share)] * 2
        + [sems(19)]
        + [sems(1)] * 3
        + [sems(2), one, sems(2), sems(2)]
        + [hops, sems(n_y - 1, n_ep // 2), hops, hops]
        + [sems(n_ep // n_x)] * 2
        + [sems(n_x - 1, n_ep // n_x)] * 2
        + [sems(1), sems(2, n_y)]
        + [hops, sems(n_y - 1, 2 * n_ep)]
        + [sems(1)] * 2
        + [hops, hops, sems(1), sems(1), hops, sems(n_y), sems(n_y), sems(2), sems(2)],
        compiler_params=pltpu.CompilerParams(
            collective_id=0, has_side_effects=True, vmem_limit_bytes=VMEM_LIMIT
        ),
    )(
        *(pltpu.with_memory_space_constraint(x, pltpu.HBM) for x in operands)
    )
    return leave(mixer_out, expert_out)


def solution(mesh):
    in_specs = (
        P("ep", "tp"),
        P("ep", "tp"),
        P("ep", "tp"),
        P("ep", "tp"),
        P("ep", "tp"),
        P("ep", "tp"),
        P("tp"),
        P("tp"),
        P("ep", "tp"),
        P("tp"),
        P("tp", None),
        P("ep", None),
        P(),
        P(),
        P(),
        P("ep", None),
        P("ep", None, "tp"),
        P("ep", None, "tp"),
        P("ep", "tp", None),
    )
    out_specs = (P(("ep", "tp"), None), P("ep", "tp"))
    return jax.shard_map(local, mesh=mesh, in_specs=in_specs, out_specs=out_specs, check_vma=False)
```

```python
import functools
import math

import jax
import jax.numpy as jnp
from jax import lax
from jax.experimental import pallas as pl
from jax.experimental.pallas import tpu as pltpu
from jax.sharding import PartitionSpec as P

HEAD_DIM = 64
PAIR = 2 * HEAD_DIM
VMEM_LIMIT = 48 << 20
HALF_EXP = math.exp(-0.5)
GROUPS = 4


key_eps = 1e-06
group_eps = 0.00064
norm_eps = 1e-06
highest = lax.Precision.HIGHEST


def bf(x):
    return x.astype(jnp.bfloat16)


def mm(x, y):
    return lax.dot_general(x, y, (((1,), (0,)), ((), ())), preferred_element_type=jnp.float32)


def mm_nt(x, y):
    return lax.dot_general(x, y, (((1,), (1,)), ((), ())), preferred_element_type=jnp.float32)


def mm_tn(x, y):
    return lax.dot_general(x, y, (((0,), (0,)), ((), ())), preferred_element_type=jnp.float32)


def halves(x):
    high = bf(x)
    return high, bf(x - high.astype(jnp.float32))


def sum_right(x, ones):
    high, low = halves(x)
    return mm(high, ones) + mm(low, ones)


def logistic(x):
    return 1.0 / (1.0 + jnp.exp(-x))


def flag(cond):
    return jnp.where(cond, 1.0, 0.0)


def iota(shape, dim):
    return lax.broadcasted_iota(jnp.int32, shape, dim)


def pair_blocks():
    return flag((iota((PAIR, PAIR), 0) < HEAD_DIM) == (iota((PAIR, PAIR), 1) < HEAD_DIM))


def scan_kernel(
    group,
    pump,
    r_ref,
    k_ref,
    v_ref,
    d_ref,
    a_ref,
    d_off_ref,
    a_off_ref,
    extra_ref,
    out_ref,
    reach_ref,
    ends_ref,
    chain_ref,
):
    positions, width = r_ref.shape
    pairs = width // PAIR
    C = HEAD_DIM
    rows_per = group * C
    own_block = pair_blocks()
    own_bf = bf(own_block)
    row, col = iota((C, PAIR), 0), iota((C, PAIR), 1) & (HEAD_DIM - 1)
    strict, upto = row > col, row >= col
    eye = flag(row == col)
    tri = bf(flag(iota((C, C), 0) >= iota((C, C), 1)))
    level_masks = []
    for s in range(6):
        inside = (
            ((row >> (s + 1)) == (col >> (s + 1)))
            & (((row >> s) & 1) == 1)
            & (((col >> s) & 1) == 0)
        )
        level_masks.append(bf(flag(inside)))

    def spread(x):
        return jnp.concatenate([x, x], axis=0) * own_bf

    square = (iota((PAIR, PAIR), 0) == iota((PAIR, PAIR), 1)).astype(jnp.float32)
    for p in range(pairs):
        chain_ref[p, :PAIR] = jnp.zeros((PAIR, PAIR), jnp.float32)
        chain_ref[p, PAIR:] = square

    def step(g, carry):
        base = pl.multiple_of(g * rows_per, rows_per)
        rows = pl.ds(base, rows_per)
        items = []
        for p in range(pairs):
            lanes = slice(p * PAIR, (p + 1) * PAIR)
            k = k_ref[rows, lanes].astype(jnp.float32)
            u = k * lax.rsqrt(sum_right(k * k, own_bf) + key_eps)
            rem = u * logistic(a_ref[rows, lanes].astype(jnp.float32) + a_off_ref[:, lanes])
            lg = extra_ref[rows, lanes] - HALF_EXP * logistic(
                d_ref[rows, lanes].astype(jnp.float32) + d_off_ref[:, lanes]
            )
            r = r_ref[rows, lanes].astype(jnp.float32)
            v = v_ref[rows, lanes]
            for c in range(group):
                cut = slice(c * C, (c + 1) * C)
                items.append((p, c, k[cut], u[cut], rem[cut], lg[cut], r[cut], v[cut]))
        stage = []
        for p, c, k, u, rem, lg, r, v in items:
            high, low = halves(lg)
            rest = bf(lg - high.astype(jnp.float32) - low.astype(jnp.float32))
            cumul = mm(tri, high) + mm(tri, low) + mm(tri, rest)
            stage.append(cumul)
        work = []
        for (p, c, k, u, rem, lg, r, v), cumul in zip(items, stage):
            mid = 0.5 * cumul[C - 1 : C]
            up_now, down = jnp.exp(cumul - mid), jnp.exp(mid - cumul)
            up_before = jnp.exp(cumul - lg - mid)
            half = jnp.exp(mid)
            cq, cu, dk, dr = r * up_now, u * up_before, k * down, rem * down
            left = bf(jnp.concatenate([cu, cq], axis=0))
            pair_r = mm_nt(left, spread(bf(dr)))
            pair_k = mm_nt(left, spread(bf(dk)))
            work.append((cq * half, bf(cu * half), bf(dk * half), bf(dr * half), half * half, pair_r, pair_k))
        pump(g, 0)
        solve = []
        for (p, c, k, u, rem, lg, r, v), (qe, ue, kt, rt, ed, pair_r, pair_k) in zip(items, work):
            rp = bf(jnp.where(strict, pair_r[:C], 0.0))
            rr = bf(jnp.where(upto, pair_r[C:], 0.0))
            kp = jnp.where(strict, pair_k[:C], 0.0)
            rk = jnp.where(upto, pair_k[C:], 0.0)
            kv = mm(bf(jnp.concatenate([kp, rk], axis=0)), spread(v))
            inv = eye - (rp * level_masks[0]).astype(jnp.float32)
            solve.append([rp, rr, kv, inv])
        for s in range(1, 6):
            mids = [bf(mm(bf(inv), spread(rp * level_masks[s]))) for rp, rr, kv, inv in solve]
            for item, y in zip(solve, mids):
                item[3] = item[3] - mm(y, spread(bf(item[3])))
            if s == 2:
                pump(g, 1)
        wvs = []
        for (rp, rr, kv, inv), w in zip(solve, work):
            wide = jnp.concatenate([spread(w[1]), spread(bf(kv[:C]))], axis=1)
            wvs.append(bf(mm(bf(inv), wide)))
        pump(g, 2)
        tails = []
        for (rp, rr, kv, inv), (qe, ue, kt, rt, ed, _, _), wv, item in zip(solve, work, wvs, items):
            wide = jnp.concatenate([spread(wv[:, :PAIR]), spread(wv[:, PAIR:])], axis=1)
            rw = mm(rr, wide)
            read = bf(qe - rw[:, :PAIR])
            local = kv[C:] - rw[:, PAIR:]
            v = item[7]
            x = jnp.concatenate(
                [jnp.concatenate([v, jnp.zeros_like(v)], axis=1),
                 jnp.concatenate([-wv[:, PAIR:], -wv[:, :PAIR]], axis=1)], axis=0)
            nb = mm_tn(x, jnp.concatenate([kt, rt], axis=0))
            tails.append((read, local, nb[:PAIR] * own_block, bf(nb[PAIR:] * own_block), ed))
        z = [chain_ref[p] for p in range(pairs)]
        for c in range(group):
            for p in range(pairs):
                read, local, add, neg, ed = tails[p * group + c]
                zb = bf(z[p])
                qz = mm_nt(read, zb)
                at = pl.ds(pl.multiple_of(base + c * C, C), C)
                lanes = slice(p * PAIR, (p + 1) * PAIR)
                out_ref[at, lanes] = local + qz[:, :PAIR]
                reach_ref[at, lanes] = bf(qz[:, PAIR:])
                moved = z[p] * ed + mm(zb, neg)
                z[p] = jnp.concatenate([moved[:PAIR] + add, moved[PAIR:]], axis=0)
        for p in range(pairs):
            chain_ref[p] = z[p]
        pump(g, 3)
        return carry

    lax.fori_loop(0, positions // rows_per, step, 0)
    for p in range(pairs):
        s, m = chain_ref[p, :PAIR], chain_ref[p, PAIR:]
        ends_ref[p * 2 * C : p * 2 * C + C] = bf(s[:C] + s[C:])
        ends_ref[p * 2 * C + C : (p + 1) * 2 * C] = bf(m[:C] + m[C:])


def join_kernel(axis, all_ref, out_ref, reach_ref, gate_ref, gain_ref, mixed_ref, planes, done):
    devices, place = lax.axis_size(axis), lax.axis_index(axis)
    width = out_ref.shape[1]
    pairs = width // PAIR
    C = HEAD_DIM
    own_block = pair_blocks()
    own_bf = bf(own_block)
    mean_bf = bf(own_block * (1.0 / HEAD_DIM))
    states = [jnp.zeros((C, PAIR), jnp.float32) for _ in range(pairs)]

    def hop(j, states):
        new = []
        for p in range(pairs):
            s = all_ref[j, p * 2 * C : p * 2 * C + C].astype(jnp.float32)
            m = all_ref[j, p * 2 * C + C : (p + 1) * 2 * C]
            m = jnp.concatenate([m, m], axis=0) * own_bf
            new.append(sum_right(states[p], m) + s)
        return tuple(new)

    states = lax.fori_loop(0, place, hop, tuple(states))
    rows = out_ref.shape[0] // len(planes)
    moves = []
    for p in range(pairs):
        s = bf(states[p])
        moves.append(jnp.concatenate([s, s], axis=0) * own_bf)
    for i, plane in enumerate(planes):
        at = pl.ds(pl.multiple_of(plane * rows, rows), rows)
        for p in range(pairs):
            lanes = slice(p * PAIR, (p + 1) * PAIR)
            head = out_ref[at, lanes] + mm_nt(reach_ref[at, lanes], moves[p])
            centred = head - sum_right(head, mean_bf)
            spread = sum_right(centred * centred, mean_bf)
            normed = centred * lax.rsqrt(spread + group_eps)
            gate = logistic(gate_ref[at, lanes].astype(jnp.float32))
            mixed_ref[at, lanes] = bf(normed * gain_ref[:, lanes] * gate)
        done(i)


def place_of():
    n_ep, n_tp = lax.axis_size("ep"), lax.axis_size("tp")
    e, t = lax.axis_index("ep"), lax.axis_index("tp")
    core = lax.rem(t, 2)
    return n_ep, n_tp, n_tp // 2, e, t, lax.div(t, 2), core


def remote(src, dst, send, recv, e, t):
    return pltpu.make_async_remote_copy(
        src_ref=src,
        dst_ref=dst,
        send_sem=send,
        recv_sem=recv,
        device_id=(e, t),
        device_id_type=pl.DeviceIdType.MESH,
    )


def meet():
    n_ep, n_tp, n_y, e, t, y, core = place_of()
    barrier = pltpu.get_barrier_semaphore()

    def greet(pe, pt):
        pl.semaphore_signal(
            barrier, inc=1, device_id=(pe, pt), device_id_type=pl.DeviceIdType.MESH
        )

    for d in range(1, n_ep):
        greet(lax.rem(e + d, n_ep), t)
    greet(e, 2 * y + 1 - core)
    for d in range(1, n_y):
        greet(e, 2 * lax.rem(y + d, n_y) + core)
        greet(e, 2 * lax.rem(y + d, n_y) + 1 - core)
    return lambda: pl.semaphore_wait(barrier, n_ep - 2 + 2 * n_y)


def span(first, last, body):
    def run(d, carry):
        body(d)
        return carry

    lax.fori_loop(first, last, run, 0)


def wide(x):
    return x.astype(jnp.float32)


def whole_kernel(
    group,
    r_hbm,
    k_hbm,
    v_hbm,
    d_hbm,
    a_hbm,
    gate_in_hbm,
    d_off_hbm,
    a_off_hbm,
    extra_hbm,
    gain_hbm,
    out_weight_hbm,
    x_hbm,
    norm_gain_hbm,
    group_router_hbm,
    expert_router_hbm,
    routes_hbm,
    gate_hbm,
    up_hbm,
    down_hbm,
    mixer_ref,
    expert_ref,
    r_ref,
    k_ref,
    v_ref,
    d_ref,
    a_ref,
    gate_in_ref,
    w_ref,
    x_ref,
    d_off_ref,
    a_off_ref,
    extra_in_ref,
    gain_ref,
    norm_gain_ref,
    group_router_ref,
    expert_router_ref,
    routes_ref,
    extra_parts_ref,
    extra_ref,
    normed_ref,
    place_ref,
    near_out_ref,
    far_out_ref,
    picks_ref,
    weight_ref,
    piece_ref,
    out_ref,
    reach_ref,
    every_ref,
    chain_ref,
    mixed_ref,
    mixed_all_ref,
    product_ref,
    gate_ref,
    up_ref,
    down_ref,
    hidden_ref,
    gate_part_ref,
    up_part_ref,
    part_ref,
    near_ref,
    stage_ref,
    far_ref,
    final_ref,
    home_ref,
    in_sem,
    gate_sem,
    up_sem,
    down_sem,
    es,
    er,
    cs,
    cr,
    ys,
    yr,
    fs,
    fr,
    zs,
    zr,
    gs,
    gr,
    ns,
    nr,
    bs,
    br,
    hs,
    hr,
    wys,
    wyr,
    wgs,
    wgr,
    wzr,
    wcs,
    wcr,
    xs,
    xr,
):
    n_ep, n_tp, n_y, e, t, y, core = place_of()
    units = gate_ref.shape[1]
    model = x_ref.shape[1]
    tokens = x_ref.shape[0]
    share = model // n_tp
    slots = piece_ref.shape[0]
    capacity = slots // n_ep
    experts = expert_router_ref.shape[0]
    groups = group_router_ref.shape[0]
    positions, width = mixed_ref.shape
    rows = positions // n_tp
    other = 2 * y + 1 - core
    half = n_ep // 2
    half_rows = half * capacity
    wide_units, wide_model = min(256, units), min(512, model)

    def shard(index):
        return pl.ds(pl.multiple_of(index * width, width), width)

    x_rows = [slice(i * tokens // 4, (i + 1) * tokens // 4) for i in range(4)]
    inputs = [(routes_hbm, routes_ref), (norm_gain_hbm, norm_gain_ref)]
    inputs += [(x_hbm.at[at, :], x_ref.at[at, :]) for at in x_rows]
    inputs += [(extra_hbm, extra_in_ref), (d_off_hbm, d_off_ref), (a_off_hbm, a_off_ref)]
    inputs += [(k_hbm, k_ref), (a_hbm, a_ref), (d_hbm, d_ref), (r_hbm, r_ref), (v_hbm, v_ref)]
    inputs += [(gate_in_hbm, gate_in_ref), (out_weight_hbm, w_ref.at[shard(t), :]), (gain_hbm, gain_ref)]
    inputs += [(group_router_hbm, group_router_ref), (expert_router_hbm, expert_router_ref)]
    loads = [pltpu.make_async_copy(s, d, in_sem.at[i]) for i, (s, d) in enumerate(inputs)]

    def gate_copy(i):
        at = pl.ds(pl.multiple_of(i * wide_units, wide_units), wide_units)
        return (
            pltpu.make_async_copy(gate_hbm.at[0, :, at], gate_ref.at[:, at], gate_sem.at[0]),
            pltpu.make_async_copy(up_hbm.at[0, :, at], up_ref.at[:, at], up_sem.at[0]),
        )

    def down_copy(i):
        at = pl.ds(pl.multiple_of(i * wide_model, wide_model), wide_model)
        return pltpu.make_async_copy(down_hbm.at[0, :, at], down_ref.at[:, at], down_sem.at[0])

    def partner(d):
        bit, total = 1, 0
        while bit < n_ep:
            total = total + lax.rem(lax.div(e, bit) + lax.div(d, bit), 2) * bit
            bit = 2 * bit
        return total

    def columns(index):
        return pl.ds(pl.multiple_of(index * share, share), share)

    def block(d):
        return pl.ds(pl.multiple_of(d * capacity, capacity), capacity)

    def peer_y(h):
        return lax.rem(y + h, n_y)

    plane = pl.ds(pl.multiple_of(core * (model // 2), model // 2), model // 2)

    def near_ep(d):
        dst = piece_ref.at[block(d), plane]
        return remote(near_out_ref.at[block(d), :], dst, es.at[0], er.at[d], partner(d), t)

    def far_ep(d):
        src = far_out_ref.at[block(d - half), :]
        return remote(src, piece_ref.at[block(d), columns(t)], es.at[1], er.at[d], partner(d), t)

    near_rows, far_rows = slice(capacity, half_rows), slice(half_rows, slots)

    def near_core(at):
        ref = piece_ref.at[at, plane]
        return remote(ref, ref, cs.at[0], cr.at[0], e, other)

    def far_core(at):
        ref = piece_ref.at[at, columns(t)]
        return remote(ref, ref, cs.at[1], cr.at[1], e, other)

    def y_copy(d, h):
        ref = piece_ref.at[block(d), columns(t)]
        peer = 2 * peer_y(h) + core
        return remote(ref, ref, ys.at[h - 1], yr.at[h - 1, d - half], e, peer)

    def forward_copy(at, h):
        ref = piece_ref.at[at, columns(2 * lax.rem(y - h + n_y, n_y) + core)]
        return remote(ref, ref, fs.at[h - 1], fr.at[h - 1], e, other)

    def near_arrived(d):
        near_ep(d).wait_recv()
        near_core(block(d)).start()

    def far_arrived(d):
        far_ep(d).wait_recv()
        for h in range(1, n_y):
            y_copy(d, h).start()
        far_core(block(d)).start()

    def pass_on(d):
        for h in range(1, n_y):
            y_copy(d, h).wait_recv()
            forward_copy(block(d), h).start()

    def gathered():
        for h in range(1, n_y):
            forward_copy(far_rows, h).wait_recv()

    n_x = gs.shape[0] + 1
    n_z = n_ep // n_x
    z, x = lax.div(e, n_x), lax.rem(e, n_x)

    def up_copy(zz):
        ref = every_ref.at[zz * n_x + x]
        return remote(ref, ref, zs.at[zz], zr.at[zz], e + n_x, t)

    def side_copy(zz, h):
        ref = every_ref.at[zz * n_x + x]
        peer = z * n_x + lax.rem(x + h, n_x)
        return remote(ref, ref, gs.at[h - 1, zz], gr.at[h - 1, zz], peer, t)

    def pass_ends(zz):
        @pl.when(z + 1 < n_z)
        def _():
            up_copy(zz).start()

        for h in range(1, n_x):
            side_copy(zz, h).start()

    def relay_ends(i, wanted=True):
        @pl.when((z >= i) & wanted)
        def _():
            up_copy(z - i).wait_recv()
            pass_ends(z - i)

    def collect_ends(zz):
        @pl.when(z >= zz)
        def _():
            for h in range(1, n_x):
                side_copy(zz, h).wait_recv()

    def close_ends(zz):
        @pl.when(z >= zz)
        def _():
            @pl.when(z + 1 < n_z)
            def _():
                up_copy(zz).wait_send()

            for h in range(1, n_x):
                side_copy(zz, h).wait_send()

    def near_copy(b, h):
        at = pl.ds(b * half_rows, half_rows)
        src = part_ref.at[at, columns(2 * peer_y(h) + 1 - core)]
        return remote(src, near_ref.at[h, at, :], ns.at[0], nr.at[b, h], e, other)

    half_block = capacity // 2

    def sub(i):
        return pl.ds(pl.multiple_of(i * half_block, half_block), half_block)

    def back_copy(i, h):
        src = stage_ref.at[h, sub(i), :]
        dst = far_ref.at[h, sub(i), :]
        return remote(src, dst, bs.at[h - 1], br.at[h - 1, i], e, 2 * peer_y(h) + core)

    def home_copy(i):
        d, s = lax.div(i, 2), lax.rem(i, 2)
        src, dst = final_ref.at[sub(i), :], home_ref.at[sub(2 * e + s), :]
        return remote(src, dst, hs.at[0], hr.at[0], partner(d), t)

    def all_home():
        src, dst = final_ref.at[capacity:, :], home_ref.at[capacity:, :]
        return remote(src, dst, hs.at[0], hr.at[0], partner(1), t)

    def pair_sum(i, h):
        return wide(part_ref[sub(i), columns(2 * peer_y(h) + core)]) + wide(near_ref[h, sub(i), :])

    def add_near(b):
        for h in range(1, n_y):
            near_copy(b, h).wait_recv()

        def one(i):
            for h in range(1, n_y):
                stage_ref[h, sub(i), :] = bf(pair_sum(i, h))
                back_copy(i, h).start()

        span(2 * b * half, 2 * (b + 1) * half, one)

    def add_far(i):
        total = pair_sum(i, 0)
        for h in range(1, n_y):
            back_copy(i, h).wait_recv()
            total = total + wide(far_ref[h, sub(i), :])
        return bf(total)

    def go_home(d):
        def one(i):
            final_ref[sub(i), :] = add_far(i)
            home_copy(i).start()

        span(2 * d, 2 * d + 2, one)

    tile_count = model // wide_model
    part_rows = width // (2 * n_x)

    def source_of(h):
        return 2 * lax.rem(y - h + n_y, n_y) + core

    def part(index, place):
        return pl.ds(pl.multiple_of(index * width + place * part_rows, part_rows), part_rows)

    own_part = lax.rem(e, 2 * n_x)
    pair_part = lax.rem(own_part + n_x, 2 * n_x)

    def w_plane(h):
        ref = w_ref.at[part(t, own_part), :]
        return remote(ref, ref, wys.at[h - 1], wyr.at[h - 1], e, 2 * peer_y(h) + core)

    def w_pair(h):
        ref = w_ref.at[part(source_of(h), own_part), :]
        return remote(ref, ref, wgs.at[0], wzr.at[h - 1], partner(n_x), t)

    def w_line(h, place, k):
        ref = w_ref.at[part(source_of(h), place), :]
        return remote(ref, ref, wgs.at[0], wgr.at[0], partner(k), t)

    def w_rows(count):
        ref = w_ref.at[: (n_y - 1) * count * part_rows, :]
        return remote(ref, ref, wgs.at[0], wgr.at[0], partner(1), t)

    def w_core(h):
        ref = w_ref.at[shard(source_of(h)), :]
        return remote(ref, ref, wcs.at[h], wcr.at[h], e, other)

    def w_core_part(h, place):
        ref = w_ref.at[part(source_of(h), place), :]
        return remote(ref, ref, wcs.at[h], wcr.at[h], e, other)

    def share_w():
        for h in range(1, n_y):
            w_plane(h).wait_recv()
            w_pair(h).start()
            span(1, n_x, lambda k: w_line(h, own_part, k).start())
            w_core_part(h, own_part).start()

    def share_pair_w(wanted):
        @pl.when(wanted)
        def _():
            for h in range(1, n_y):
                w_pair(h).wait_recv()
                span(1, n_x, lambda k: w_line(h, pair_part, k).start())
                w_core_part(h, pair_part).start()

    def share_line_w():
        w_rows(2 * n_x - 2).wait_recv()
        for h in range(1, n_y):
            for shift in (0, n_x):

                def one(k):
                    place = lax.rem(partner(k) + shift, 2 * n_x)
                    w_core_part(h, place).start()

                span(1, n_x, one)

    def mixed_copy(to):
        src = mixed_ref.at[pl.ds(pl.multiple_of(to * rows, rows), rows), :]
        return remote(src, mixed_all_ref.at[t], xs.at[0], xr.at[0], e, to)

    def mixed_core():
        src = mixed_ref.at[pl.ds(pl.multiple_of(other * rows, rows), rows), :]
        return remote(src, mixed_all_ref.at[t], xs.at[1], xr.at[1], e, other)

    def mixed_planes():
        ref = mixed_all_ref.at[: n_tp - 2]
        return remote(ref, ref, xs.at[0], xr.at[0], e, other)

    def plane_product(plane, at):
        held_rows = pl.ds(pl.multiple_of(plane * 2 * width, 2 * width), 2 * width)
        left = jnp.concatenate([mixed_all_ref[2 * plane], mixed_all_ref[2 * plane + 1]], axis=1)
        return mm(left, w_ref[held_rows, at])

    def tiles(count, body, hooks):
        for i in range(count):
            body(i)
            for hook in hooks.get(i, ()):
                hook()
        for i in sorted(hooks):
            for hook in hooks[i] if i >= count else ():
                hook()

    def units_at(i):
        return slice(i * wide_units, (i + 1) * wide_units)

    def activate(i, gate_val, up_val):
        hidden_ref[:, units_at(i)] = bf(gate_val * logistic(gate_val) * up_val)

    def widen_near(hooks):
        pltpu.make_async_copy(gate_hbm.at[0], gate_ref, gate_sem.at[0]).wait()
        pltpu.make_async_copy(up_hbm.at[0], up_ref, up_sem.at[0]).wait()

        def unit_tile(i):
            rows_in = piece_ref[:half_rows, :]
            activate(i, mm(rows_in, gate_ref[:, units_at(i)]), mm(rows_in, up_ref[:, units_at(i)]))

        tiles(units // wide_units, unit_tile, hooks)

    def widen_part(i, h):
        model_at = pl.ds(pl.multiple_of(peer_y(h) * 2 * share, 2 * share), 2 * share)
        rows_in = piece_ref[far_rows, model_at]
        return mm(rows_in, gate_ref[model_at, units_at(i)]), mm(rows_in, up_ref[model_at, units_at(i)])

    def widen_far_begin():
        for i in range(units // wide_units):
            gate_part_ref[:, units_at(i)], up_part_ref[:, units_at(i)] = widen_part(i, 0)

    def widen_far_end(hooks):
        def unit_tile(i):
            gate_val, up_val = gate_part_ref[:, units_at(i)], up_part_ref[:, units_at(i)]
            for h in range(1, n_y):
                more = widen_part(i, h)
                gate_val, up_val = gate_val + more[0], up_val + more[1]
            activate(i, gate_val, up_val)

        tiles(units // wide_units, unit_tile, hooks)

    def narrow(b, hooks):
        at = slice(b * half_rows, (b + 1) * half_rows)
        if b == 0:
            pltpu.make_async_copy(down_hbm.at[0], down_ref, down_sem.at[0]).wait()

        def tile(h, ours):
            index = 2 * peer_y(h) + (core if ours else 1 - core)
            part_ref[at, columns(index)] = bf(mm(hidden_ref[...], down_ref[:, columns(index)]))

        for h in range(n_y - 1, 0, -1):
            tile(h, False)
            near_copy(b, h).start()
        for hook in hooks:
            hook()
        for h in range(n_y - 1, 0, -1):
            tile(h, True)
        tile(0, False)
        tile(0, True)
        near_copy(b, 0).start()

    for copy in loads[:6]:
        copy.start()
    everyone_here = meet()

    order = flag(iota((tokens, tokens), 0) < iota((tokens, tokens), 1))
    expert_rows = max(16, experts)
    loads[0].wait()
    loads[1].wait()
    own_routes = routes_ref[...]
    names = iota((expert_rows, tokens), 0)
    named = [own_routes[k : k + 1, :] == names for k in range(own_routes.shape[0])]
    match = functools.reduce(jnp.logical_or, named)
    rank = mm(bf(flag(match)), bf(order))
    rank = jnp.where(match, rank, -1.0)
    level = iota((capacity, tokens), 0).astype(jnp.float32)
    for j in range(experts):
        place_ref[j * capacity : (j + 1) * capacity] = bf(flag(level == rank[j : j + 1, :]))
    for copy in loads[2:6]:
        copy.wait()
    for copy in loads[6:]:
        copy.start()
    for i in range(units // wide_units):
        for copy in gate_copy(i):
            copy.start()
    for i in range(model // wide_model):
        down_copy(i).start()
    step_rows = 32
    for i in range(tokens // step_rows):
        at = slice(i * step_rows, (i + 1) * step_rows)
        xw = wide(x_ref[at])
        scale = lax.rsqrt(jnp.mean(xw * xw, axis=-1, keepdims=True) + norm_eps)
        normed_ref[at] = bf(xw * scale * norm_gain_ref[...])
    here = jnp.concatenate([place_ref[block(partner(d)), :] for d in range(1, half)], axis=0)
    near_out_ref[capacity:half_rows] = bf(mm(here, normed_ref[:, plane]))
    there = jnp.concatenate([place_ref[block(partner(d)), :] for d in range(half, n_ep)], axis=0)
    far_out_ref[...] = bf(mm(there, normed_ref[:, columns(t)]))
    per = max(1, n_ep // 8)

    def unit(u, body):
        lo = max(1, min(n_ep, u * per))
        return lambda: span(lo, max(lo, min(n_ep, (u + 1) * per)), body)

    inner = lax.rem(lax.div(z + 1, 2), 2)

    def far_unit(k, body):
        first = [4 + 2 * inner, 5 + 2 * inner, 6 - 2 * inner, 7 - 2 * inner][k] * per
        return lambda: span(first, first + per, body)

    everyone_here()
    span(1, half, lambda d: near_ep(d).start())
    for k in range(4):
        far_unit(k, lambda d: far_ep(d).start())()
    for i in range(model // wide_model):
        at = slice(i * wide_model, (i + 1) * wide_model)
        piece_ref[:capacity, at] = bf(mm(place_ref[block(e), :], normed_ref[:, at]))

    loads[15].wait()
    for h in range(1, n_y):
        w_plane(h).start()
    w_core(0).start()
    for copy in loads[6:14]:
        copy.wait()
    heads, pairs = extra_in_ref.shape[0], chain_ref.shape[0]
    exact = extra_in_ref[...]
    extra_parts_ref[...] = jnp.zeros(extra_parts_ref.shape, jnp.float32)
    for i in range(3):
        piece = wide(bf(exact))
        extra_parts_ref[i * heads : (i + 1) * heads, :] = piece
        exact = exact - piece
    extra_parts = bf(extra_parts_ref[...])
    extra_rows = extra_parts_ref.shape[0]
    for p in range(pairs):
        head = lax.rem(iota((extra_rows, PAIR), 0), heads)
        wanted = head == 2 * p + lax.div(iota((extra_rows, PAIR), 1), HEAD_DIM)
        extra_ref[:, p * PAIR : (p + 1) * PAIR] = mm_tn(extra_parts, bf(flag(wanted)))
    steps = positions // (group * HEAD_DIM)
    events = {}

    def pump(g, point):
        for step in range(steps):
            due = events.get(4 * step + point)
            if due:

                @pl.when(g == step)
                def _(due=due):
                    for act in due:
                        act()

    scan_kernel(
        group,
        pump,
        r_ref,
        k_ref,
        v_ref,
        d_ref,
        a_ref,
        d_off_ref,
        a_off_ref,
        extra_ref,
        out_ref,
        reach_ref,
        every_ref.at[e],
        chain_ref,
    )
    for i in sorted(events):
        for act in events[i] if i >= 4 * steps else ():
            act()
    pass_ends(z)
    span(1, half, near_arrived)
    far_unit(0, far_arrived)()
    far_unit(1, far_arrived)()
    near_core(near_rows).wait_recv()
    relays = [lambda i=i: relay_ends(i) for i in range(1, n_z)]
    widen_near({0: [share_w], 2: [far_unit(2, far_arrived)], 3: [far_unit(0, pass_on)]})
    far_unit(1, pass_on)()
    narrow(0, [far_unit(3, far_arrived)])
    far_unit(2, pass_on)()
    add_near(0)
    for copy in loads[14:15] + loads[16:]:
        copy.wait()

    normed = normed_ref[...]
    group_logit = mm_nt(group_router_ref[...], normed)
    group_exp = jnp.exp(group_logit)
    group_prob = group_exp / jnp.sum(group_exp, axis=0, keepdims=True)
    expert_logit = mm_nt(expert_router_ref[...], normed)
    per_group = experts // groups
    first_of = iota((groups, tokens), 0) * per_group
    expert_names = iota((experts, tokens), 0)
    chosen, prob = [], []
    for k in range(2):
        route = own_routes[k : k + 1, :]
        chosen.append(
            jnp.sum(jnp.where(route == expert_names, expert_logit, 0.0), axis=0, keepdims=True)
        )
        inside = (route >= first_of) & (route < first_of + per_group)
        prob.append(jnp.sum(jnp.where(inside, group_prob, 0.0), axis=0, keepdims=True))
    weights = [prob[0] * logistic(chosen[0] - chosen[1]), prob[1] * logistic(chosen[1] - chosen[0])]
    for k in range(2):
        weight_ref[k] = jnp.transpose(jnp.broadcast_to(weights[k], (128, tokens)))
        for j in range(experts):
            at = slice(j * capacity, (j + 1) * capacity)
            picks_ref[k, at] = place_ref[at] * bf(flag(own_routes[k : k + 1, :] == j))
    last = z == n_z - 1
    far_core(far_rows).wait_recv()
    widen_far_begin()
    for relay in relays[:1]:
        relay()
    with jax.named_scope("pass3"):
        far_unit(3, pass_on)()
    near_copy(0, 0).wait_recv()
    gathered()
    passing = [lambda i=i: relay_ends(i, ~last) for i in range(2, min(3, n_z))]
    widen_far_end({1: passing})
    late = [lambda i=i: relay_ends(i, last if i < 3 else True) for i in range(2, n_z)]
    narrow(1, late[:1] + [lambda: share_pair_w(~last)])
    add_near(1)
    for relay in late[1:]:
        relay()
    share_pair_w(last)

    def near_home(wanted):
        @pl.when(wanted)
        def _():
            span(1, half, go_home)

    near_home(~last)
    near_copy(1, 0).wait_recv()
    unit(4, go_home)()
    for u in range(5, 8):
        unit(u, go_home)()
    near_home(last)
    for i in range(2):
        home_ref[sub(2 * e + i), :] = add_far(i)
    span(0, n_z, collect_ends)
    planes = [peer_y(h) for h in range(1, n_y)] + [y]

    def joined(i):
        if i + 1 < n_y:
            mixed_copy(2 * planes[i] + core).start()
            mixed_copy(2 * planes[i] + 1 - core).start()
        else:
            mixed_core().start()

    join_kernel(
        "ep", every_ref, out_ref, reach_ref, gate_in_ref, gain_ref, mixed_ref, planes, joined
    )
    mixed_all_ref[t] = mixed_ref[pl.ds(pl.multiple_of(t * rows, rows), rows), :]
    tile_slices = [slice(i * wide_model, (i + 1) * wide_model) for i in range(tile_count)]
    w_core(0).wait_recv()
    mixed_core().wait_recv()
    for at in tile_slices:
        product_ref[:, at] = plane_product(y, at)
    share_line_w()
    mixed_planes().wait_recv()
    for h in range(1, n_y):
        w_core(h).wait_recv()
    for at in tile_slices:
        total = product_ref[:, at]
        for h in range(1, n_y):
            total = total + plane_product(peer_y(h), at)
        mixer_ref[:, at] = bf(total)

    near_src = near_out_ref.at[near_rows, :]
    remote(near_src, near_src, es.at[0], er.at[0], e, other).wait_send()
    remote(far_out_ref, far_out_ref, es.at[1], er.at[0], e, other).wait_send()
    near_core(near_rows).wait_send()
    far_core(far_rows).wait_send()
    remote(near_ref, near_ref, ns.at[0], nr.at[0, 0], e, other).wait_send()
    for h in range(1, n_y):
        ref = piece_ref.at[far_rows, columns(t)]
        remote(ref, ref, ys.at[h - 1], yr.at[h - 1, 0], e, other).wait_send()
        forward_copy(far_rows, h).wait_send()
        ref = stage_ref.at[h]
        remote(ref, ref, bs.at[h - 1], br.at[h - 1, 0], e, other).wait_send()
        w_plane(h).wait_send()
    for h in range(n_y):
        w_core(h).wait_send()
    w_rows(2 * n_x - 1).wait_send()
    mixed_planes().wait_send()
    mixed_core().wait_send()
    span(0, n_z, close_ends)
    all_home().wait_recv()
    back = home_ref[...]
    first, second = mm_tn(picks_ref[0], back), mm_tn(picks_ref[1], back)
    for i in range(share // 128):
        at = slice(i * 128, (i + 1) * 128)
        expert_ref[:, at] = bf(weight_ref[0] * first[:, at] + weight_ref[1] * second[:, at])
    all_home().wait_send()


def leave_kernel(mixer_ref, expert_ref, mixer_hbm, expert_hbm, sem):
    parts = 4
    rows = mixer_ref.shape[0] // parts
    copies = []
    for i in range(parts):
        at = slice(i * rows, (i + 1) * rows)
        copies.append(pltpu.make_async_copy(mixer_ref.at[at, :], mixer_hbm.at[at, :], sem.at[i]))
    copies.append(pltpu.make_async_copy(expert_ref, expert_hbm, sem.at[parts]))
    for copy in copies:
        copy.start()
    for copy in copies:
        copy.wait()


def leave(mixer_out, expert_out):
    return pl.pallas_call(
        leave_kernel,
        out_shape=(
            jax.ShapeDtypeStruct(mixer_out.shape, mixer_out.dtype),
            jax.ShapeDtypeStruct(expert_out.shape, expert_out.dtype),
        ),
        in_specs=[pl.BlockSpec(memory_space=pltpu.VMEM)] * 2,
        out_specs=[pl.BlockSpec(memory_space=pltpu.HBM)] * 2,
        scratch_shapes=[pltpu.SemaphoreType.DMA((5,))],
        compiler_params=pltpu.CompilerParams(vmem_limit_bytes=1 << 20),
    )(
        pltpu.with_memory_space_constraint(mixer_out, pltpu.VMEM),
        pltpu.with_memory_space_constraint(expert_out, pltpu.VMEM),
    )


def local(
    receptance,
    key_matrix,
    value_matrix,
    decay_data_term,
    correction_rate_data,
    output_gate_input,
    decay_channel_offset,
    correction_rate_offset,
    extra_head_log_decay,
    head_norm_gain,
    mixer_output_weight,
    expert_layer_input,
    feedforward_norm_gain,
    group_router_weight,
    expert_router_weight,
    routes,
    expert_gate_weight,
    expert_up_weight,
    expert_down_weight,
):
    positions, own_width = receptance.shape
    pairs = -(-own_width // PAIR)
    width = pairs * PAIR

    def filled(x, columns=width):
        return x if x.shape[-1] == columns else jnp.pad(x, ((0, 0), (0, columns - x.shape[-1])))

    blocks = positions // HEAD_DIM
    group = 4 if blocks % 4 == 0 else 1
    n_ep, n_tp = lax.axis_size("ep"), lax.axis_size("tp")
    n_y = n_tp // 2
    n_x = 1
    while 4 * n_x * n_x <= n_ep:
        n_x = 2 * n_x
    tokens, model = expert_layer_input.shape
    capacity, share = 4 * tokens // n_ep, model // n_tp
    slots = n_ep * capacity
    units = expert_gate_weight.shape[2]
    rows = positions // n_tp
    out_weight = jnp.pad(mixer_output_weight, ((0, width - own_width), (0, 0)))

    def held(*shape):
        return pltpu.VMEM(shape, jnp.bfloat16)

    def single(*shape):
        return pltpu.VMEM(shape, jnp.float32)

    def sems(*shape):
        return pltpu.SemaphoreType.DMA(shape)

    operands = (
        filled(receptance),
        filled(key_matrix),
        filled(value_matrix),
        filled(decay_data_term),
        filled(correction_rate_data),
        filled(output_gate_input),
        filled(decay_channel_offset[None]),
        filled(correction_rate_offset[None]),
        filled(extra_head_log_decay, 2 * pairs).T,
        filled(head_norm_gain[None]),
        out_weight,
        expert_layer_input,
        feedforward_norm_gain[None],
        group_router_weight.T,
        expert_router_weight.T,
        routes.T,
        expert_gate_weight,
        expert_up_weight,
        expert_down_weight,
    )
    in_vmem, in_hbm = pl.BlockSpec(memory_space=pltpu.VMEM), pl.BlockSpec(memory_space=pltpu.HBM)
    one, hops = sems(n_ep), sems(n_y - 1)
    mixer_out, expert_out = pl.pallas_call(
        functools.partial(whole_kernel, group),
        out_shape=(held(rows, model), held(tokens, share)),
        in_specs=[in_hbm] * 19,
        out_specs=[in_vmem] * 2,
        scratch_shapes=[held(positions, width)] * 6
        + [
            held(n_tp * width, model),
            held(tokens, model),
            single(1, width),
            single(1, width),
            single(2 * pairs, positions),
            single(1, width),
            single(1, model),
            held(*group_router_weight.shape[::-1]),
            held(*expert_router_weight.shape[::-1]),
            pltpu.VMEM(routes.shape[::-1], jnp.int32),
            single(16, positions),
            single(positions, width),
            held(tokens, model),
            held(slots, tokens),
            held(slots // 2, model // 2),
            held(slots // 2, share),
            held(2, slots, tokens),
            single(2, tokens, 128),
            held(slots, model),
            single(positions, width),
            held(positions, width),
            held(n_ep, pairs * 2 * HEAD_DIM, PAIR),
            single(pairs, 2 * PAIR, PAIR),
            held(positions, width),
            held(n_tp, rows, width),
            single(rows, model),
            held(model, units),
            held(model, units),
            held(units, model),
            held(slots // 2, units),
            single(slots // 2, units),
            single(slots // 2, units),
            held(slots, model),
        ]
        + [held(n_y, slots, share)] * 3
        + [held(slots, share)] * 2
        + [sems(19)]
        + [sems(1)] * 3
        + [sems(2), one, sems(2), sems(2)]
        + [hops, sems(n_y - 1, n_ep // 2), hops, hops]
        + [sems(n_ep // n_x)] * 2
        + [sems(n_x - 1, n_ep // n_x)] * 2
        + [sems(1), sems(2, n_y)]
        + [hops, sems(n_y - 1, 2 * n_ep)]
        + [sems(1)] * 2
        + [hops, hops, sems(1), sems(1), hops, sems(n_y), sems(n_y), sems(2), sems(2)],
        compiler_params=pltpu.CompilerParams(
            collective_id=0, has_side_effects=True, vmem_limit_bytes=VMEM_LIMIT
        ),
    )(
        *(pltpu.with_memory_space_constraint(x, pltpu.HBM) for x in operands)
    )
    return leave(mixer_out, expert_out)


def solution(mesh):
    in_specs = (
        P("ep", "tp"),
        P("ep", "tp"),
        P("ep", "tp"),
        P("ep", "tp"),
        P("ep", "tp"),
        P("ep", "tp"),
        P("tp"),
        P("tp"),
        P("ep", "tp"),
        P("tp"),
        P("tp", None),
        P("ep", None),
        P(),
        P(),
        P(),
        P("ep", None),
        P("ep", None, "tp"),
        P("ep", None, "tp"),
        P("ep", "tp", None),
    )
    out_specs = (P(("ep", "tp"), None), P("ep", "tp"))
    return jax.shard_map(local, mesh=mesh, in_specs=in_specs, out_specs=out_specs, check_vma=False)
```
